32 devices in a mesh: sp: 8 (over z, x), tp: 4 (over y, core).
Axes of the slice: x: 2, y: 2, z: 4, core: 2. Of those that a mesh axis runs over, the one named last changes fastest.
Arguments:
- tokens: bfloat16 [8192, 2048], P('sp', 'tp'), may hold values from -6 to 6
- norm_gain: float32 [2048], replicated, may hold values from 0.1 to 1.9
- att_query: bfloat16 [2048, 1024], P(None, 'tp'), may hold values from -1 to 1, as said below
- att_key: bfloat16 [2048, 512], P(None, 'tp'), may hold values from -16 to 16, as said below
- att_value: bfloat16 [2048, 512], P(None, 'tp'), may hold values from -0.125 to 0.125
- ret_query: bfloat16 [2048, 512], P(None, 'tp'), may hold values from -0.125 to 0.125
- ret_key: bfloat16 [2048, 512], P(None, 'tp'), may hold values from -0.125 to 0.125
- ret_value: bfloat16 [2048, 1024], P(None, 'tp'), may hold values from -0.125 to 0.125
- ret_gate: bfloat16 [2048, 1024], P(None, 'tp'), may hold values from -0.125 to 0.125
- att_sink: float32 [16], P('tp'), may hold values from 4 to 7
- decay_log: float32 [8, 8192], P('tp', 'sp'), may hold values from -2 to 0, as said below
- init_state: float32 [2, 8, 64, 128], P(None, 'tp'), may hold values from -24 to 24
- out_att: bfloat16 [1024, 2048], P('tp'), may hold values from -0.125 to 0.125
- out_ret: bfloat16 [1024, 2048], P('tp'), may hold values from -0.125 to 0.125
Outputs:
- mixed: bfloat16 [8192, 2048], P('sp', 'tp')
The draws below stay inside these ranges and needn't reach their ends.
Inputs may be any that keep to these rules, and one draw needn't show every extreme that they name: `att_query`: entries of order D ** -0.5. `att_key`: entries of order D ** -0.5 or larger. `decay_log`: log decays, negative.
All inputs are finite; a program needn't handle non-finite values.
Results may differ from the reference program's by a relative error of at most 0.02.
Values may be sent and summed in bfloat16 or wider, within the bound.
A program may use at most 64 MiB of HBM per device.

```python
import math
import jax
import jax.numpy as jnp
from jax import lax

D = 2048
ATT_HEADS = 16
KV_HEADS = 8
HD = 64
RET_HEADS = 8
RK = 64
RV = 128
WINDOW = 128
RET_BLOCK = 128
TOK_DEV = 1024
SEQUENCE_LENGTH = 8192
N_TP = 4


def draw_tokens(key, part):
    base_rows = jnp.clip(jax.random.normal(key, (SEQUENCE_LENGTH, D), jnp.float32), -6.0, 6.0)
    return base_rows.astype(jnp.bfloat16)


def attention_weights(key):
    query_w = jnp.clip(jax.random.normal(jax.random.fold_in(key, 11), (D, ATT_HEADS * HD), jnp.float32), -4.0, 4.0) * D ** (-0.5)
    key_w = jnp.clip(jax.random.normal(jax.random.fold_in(key, 12), (D, KV_HEADS * HD), jnp.float32), -4.0, 4.0) * D ** (-0.5)
    return (query_w, key_w)


def draw_att_query(key, part):
    return attention_weights(key)[0].astype(jnp.bfloat16)


def draw_att_key(key, part):
    return attention_weights(key)[1].astype(jnp.bfloat16)


def draw_decay_log(key, part):
    child_random_keys = jax.random.split(key, 7)
    slow_heads = jax.random.uniform(child_random_keys[0], (RET_HEADS,)) < 0.5
    slow_rate = 0.15 * math.log(10.0) / SEQUENCE_LENGTH * jax.random.uniform(child_random_keys[1], (RET_HEADS,), minval=0.5, maxval=1.5)
    fast_rate = jax.random.uniform(child_random_keys[2], (RET_HEADS,), minval=1.0 / 100.0, maxval=1.0 / 30.0)
    baseline_rate = jnp.where(slow_heads, slow_rate, fast_rate)
    device_pace = jnp.exp(jax.random.uniform(child_random_keys[3], (SEQUENCE_LENGTH // TOK_DEV,), minval=math.log(0.5), maxval=math.log(2.0)))
    full_speed = jnp.repeat(device_pace, TOK_DEV, total_repeat_length=SEQUENCE_LENGTH)
    jaggedness = jax.random.uniform(child_random_keys[4], (RET_HEADS, SEQUENCE_LENGTH), minval=0.5, maxval=1.5)
    spike_positions = jax.random.randint(child_random_keys[5], (3,), 0, SEQUENCE_LENGTH)
    spike_depth = jax.random.uniform(child_random_keys[6], (3,), minval=0.55, maxval=0.85)
    spike_count = jnp.zeros((SEQUENCE_LENGTH,), jnp.float32).at[spike_positions].add(jnp.log(spike_depth))
    return -baseline_rate[:, None] * full_speed[None, :] * jaggedness + spike_count[None, :]


def block_scale(rng, dims, pieces, smallest, largest):
    def one(position, shards_of):
        heights = jax.random.uniform(jax.random.fold_in(jax.random.fold_in(rng, 6), position), (shards_of,), jnp.float32, smallest / len(pieces), largest / len(pieces))
        return jnp.repeat(jnp.exp(heights), dims[position] // shards_of).reshape((-1,) + (1,) * (len(dims) - position - 1))

    loudness = one(*pieces[0])
    for cut in pieces[1:]:
        loudness = loudness * one(*cut)
    return loudness


def scatter_about(own_key, extent, scale, limit, cuts=(), held_as=jnp.bfloat16):
    result = jax.random.normal(own_key, extent, jnp.float32) * scale
    if len(cuts) > 0:
        result = block_scale(own_key, extent, cuts, -0.22, 0.18) * result
    return jnp.clip(result, min=-limit, max=limit).astype(held_as)


def setup_inputs(seed: int = 0) -> dict:
    seeds = jax.random.split(jax.random.key(seed), 15)
    tokens = draw_tokens(jax.random.fold_in(seeds[14], 71), 0)
    norm_gain = jnp.clip(1.0 + 0.18 * jax.random.normal(seeds[1], (D,), jnp.float32), 0.1, 1.9)
    att_query = draw_att_query(jax.random.fold_in(seeds[14], 71), 0)
    att_key = draw_att_key(jax.random.fold_in(seeds[14], 71), 0)
    att_value = scatter_about(seeds[4], (D, KV_HEADS * HD), D ** -0.5, 0.125, ((1, 4),))
    ret_query = scatter_about(seeds[5], (D, RET_HEADS * RK), D ** -0.5, 0.125, ((1, 4),))
    ret_key = scatter_about(seeds[6], (D, RET_HEADS * RK), D ** -0.5, 0.125, ((1, 4),))
    ret_value = scatter_about(seeds[7], (D, RET_HEADS * RV), D ** -0.5, 0.125, ((1, 4),))
    ret_gate = scatter_about(seeds[8], (D, RET_HEADS * RV), D ** -0.5, 0.125, ((1, 4),))
    att_sink = jnp.clip(4.0 + 3.0 * jax.random.uniform(seeds[9], (ATT_HEADS,), jnp.float32) ** block_scale(seeds[9], (ATT_HEADS,), ((0, 4),), -0.2, 0.2), 4.0, 7.0)
    decay_log = draw_decay_log(jax.random.fold_in(seeds[14], 71), 0)
    init_state = scatter_about(seeds[11], (2, RET_HEADS, RK, RV), 4.0, 24.0, ((1, 4),), jnp.float32)
    out_att = scatter_about(seeds[12], (ATT_HEADS * HD, D), (ATT_HEADS * HD + RET_HEADS * RV) ** -0.5, 0.125, ((0, 4),))
    out_ret = scatter_about(seeds[13], (RET_HEADS * RV, D), (ATT_HEADS * HD + RET_HEADS * RV) ** -0.5, 0.125, ((0, 4),))
    return dict(tokens=tokens, norm_gain=norm_gain, att_query=att_query, att_key=att_key, att_value=att_value, ret_query=ret_query, ret_key=ret_key, ret_value=ret_value, ret_gate=ret_gate, att_sink=att_sink, decay_log=decay_log, init_state=init_state, out_att=out_att, out_ret=out_ret)


NORM_EPS = 1e-06
ROPE_BASE = 10000.0
HIGHEST = lax.Precision.HIGHEST

def rotated(values, positions):
    half_dim = values.shape[-1] // 2
    inverse = ROPE_BASE ** (-2.0 * jnp.arange(half_dim, dtype=jnp.float32) / values.shape[-1])
    angles = positions.astype(jnp.float32)[:, None] * inverse[None, :]
    cosine = jnp.cos(angles)[:, None, :]
    sine = jnp.sin(angles)[:, None, :]
    first_half = values[..., :half_dim]
    second_half = values[..., half_dim:]
    return jnp.concatenate([first_half * cosine - second_half * sine, first_half * sine + second_half * cosine], axis=-1)

def attend_all(queries, key_proj, value_proj, att_sink):
    seq_len = queries.shape[0]
    block_rows = 512
    groups = ATT_HEADS // KV_HEADS
    span_rows = block_rows + 2 * WINDOW
    padded_keys = jnp.pad(key_proj, ((WINDOW, WINDOW), (0, 0)))
    padded_vals = jnp.pad(value_proj, ((WINDOW, WINDOW), (0, 0)))
    sink_col = att_sink.astype(jnp.float32).reshape(KV_HEADS, groups, 1, 1)

    def one_block(block_index):
        first_row = block_index * block_rows
        query_block = lax.dynamic_slice_in_dim(queries, first_row, block_rows, 0).reshape(block_rows, KV_HEADS, groups, HD)
        key_block = lax.dynamic_slice_in_dim(padded_keys, first_row, span_rows, 0).reshape(span_rows, KV_HEADS, HD)
        value_block = lax.dynamic_slice_in_dim(padded_vals, first_row, span_rows, 0).reshape(span_rows, KV_HEADS, HD)
        scores = jnp.einsum('qkgd,skd->kgqs', query_block.astype(jnp.float32), key_block.astype(jnp.float32)) * HD ** (-0.5)
        query_pos = first_row + jnp.arange(block_rows, dtype=jnp.int32)
        key_pos = first_row - WINDOW + jnp.arange(span_rows, dtype=jnp.int32)
        allowed = (jnp.abs(query_pos[:, None] - key_pos[None, :]) <= WINDOW) & (key_pos >= 0)[None, :] & (key_pos < seq_len)[None, :]
        scores = jnp.where(allowed, scores, -jnp.inf)
        row_top = jnp.maximum(lax.optimization_barrier(jnp.max(scores, axis=-1, keepdims=True)), sink_col)
        raised = jnp.exp(scores - row_top)
        denominator = lax.optimization_barrier(jnp.sum(raised, axis=-1, keepdims=True)) + jnp.exp(sink_col - row_top)
        weights_bf = (raised / denominator).astype(jnp.bfloat16)
        block_out = jnp.einsum('kgqs,skd->qkgd', weights_bf.astype(jnp.float32), value_block.astype(jnp.float32))
        return block_out.reshape(block_rows, ATT_HEADS * HD).astype(jnp.bfloat16)
    blocks = lax.map(one_block, jnp.arange(seq_len // block_rows, dtype=jnp.int32))
    return blocks.reshape(seq_len, ATT_HEADS * HD)

def advance(state_now, item_pair):
    factor_now, term_now = item_pair
    return (factor_now[:, None, None] * state_now + term_now, state_now)

def retain_all(query_rot, key_rot, value_f, decay_log, init_state):
    seq_len = query_rot.shape[0]
    block_count = seq_len // RET_BLOCK

    def heads_first(values, width):
        return jnp.transpose(values.reshape(block_count, RET_BLOCK, RET_HEADS, width), (2, 0, 1, 3))
    query_h = heads_first(query_rot, RK)
    key_h = heads_first(key_rot, RK)
    value_h = heads_first(value_f, RV)
    block_logs = decay_log.reshape(RET_HEADS, block_count, RET_BLOCK)
    cumul = jnp.cumsum(block_logs, axis=-1)
    block_log = cumul[..., -1]
    inner_w = jnp.einsum('hbnk,hbmk->hbnm', query_h, key_h, precision=HIGHEST) * jnp.exp(-jnp.abs(cumul[..., :, None] - cumul[..., None, :]))
    local_out = jnp.einsum('hbnm,hbmv->hbnv', inner_w, value_h, precision=HIGHEST)
    fwd_terms = jnp.einsum('hbmk,hbmv->bhkv', key_h * jnp.exp(block_log[..., None] - cumul)[..., None], value_h, precision=HIGHEST)
    bwd_terms = jnp.einsum('hbmk,hbmv->bhkv', key_h * jnp.exp(cumul)[..., None], value_h, precision=HIGHEST)
    factors = jnp.exp(block_log).T
    _, fwd_in = lax.scan(advance, init_state[0], (factors, fwd_terms))
    _, bwd_in = lax.scan(advance, init_state[1], (factors, bwd_terms), reverse=True)
    cross_out = jnp.exp(cumul)[..., None] * jnp.einsum('hbnk,bhkv->hbnv', query_h, fwd_in, precision=HIGHEST)
    cross_out = cross_out + jnp.exp(block_log[..., None] - cumul)[..., None] * jnp.einsum('hbnk,bhkv->hbnv', query_h, bwd_in, precision=HIGHEST)
    combined = local_out + cross_out
    centered = combined - lax.optimization_barrier(jnp.mean(combined, axis=-1, keepdims=True))
    normed = centered * lax.rsqrt(lax.optimization_barrier(jnp.mean(centered * centered, axis=-1, keepdims=True)) + NORM_EPS)
    return jnp.transpose(normed, (1, 2, 0, 3)).reshape(seq_len, RET_HEADS * RV)

def reference(tokens, norm_gain, att_query, att_key, att_value, ret_query, ret_key, ret_value, ret_gate, att_sink, decay_log, init_state, out_att, out_ret):
    seq_len = tokens.shape[0]
    tokens_f = tokens.astype(jnp.float32)
    inv_rms = lax.rsqrt(lax.optimization_barrier(jnp.mean(tokens_f * tokens_f, axis=-1, keepdims=True)) + NORM_EPS)
    normed = (tokens_f * norm_gain.astype(jnp.float32)[None, :]).astype(jnp.bfloat16)

    def project(weight):
        return (jnp.dot(normed, weight, preferred_element_type=jnp.float32) * inv_rms).astype(jnp.bfloat16)
    attended = attend_all(project(att_query), project(att_key), project(att_value), att_sink)
    positions = jnp.arange(seq_len, dtype=jnp.int32)
    query_rot = rotated(project(ret_query).astype(jnp.float32).reshape(seq_len, RET_HEADS, RK), positions)
    key_rot = rotated(project(ret_key).astype(jnp.float32).reshape(seq_len, RET_HEADS, RK), positions) * RK ** (-0.5)
    value_f = project(ret_value).astype(jnp.float32).reshape(seq_len, RET_HEADS, RV)
    retained = retain_all(query_rot, key_rot, value_f, decay_log, init_state)
    gate_f = project(ret_gate).astype(jnp.float32)
    ret_out = (jax.nn.silu(gate_f) * retained).astype(jnp.bfloat16)
    att_width = ATT_HEADS * HD // N_TP
    ret_width = RET_HEADS * RV // N_TP
    summed = jnp.zeros((seq_len, D), jnp.float32)
    for group_index in range(N_TP):
        att_lo = group_index * att_width
        ret_lo = group_index * ret_width
        partial_sum = jnp.dot(attended[:, att_lo:att_lo + att_width], out_att[att_lo:att_lo + att_width], preferred_element_type=jnp.float32)
        partial_sum = partial_sum + jnp.dot(ret_out[:, ret_lo:ret_lo + ret_width], out_ret[ret_lo:ret_lo + ret_width], preferred_element_type=jnp.float32)
        rounded = lax.optimization_barrier(partial_sum.astype(jnp.bfloat16))
        summed = summed + rounded.astype(jnp.float32)
    return summed.astype(jnp.bfloat16)
```

```python
import contextlib
import functools

import jax
import jax.numpy as jnp
import numpy as np
from jax import lax
from jax.experimental import pallas as pl
from jax.experimental.pallas import tpu as pltpu
from jax.sharding import PartitionSpec as P

HD = 64
RK = 64
RV = 128
WINDOW = 128
CHUNK = 256
MIX = 128
NORM_EPS = 1e-06
ROPE_BASE = 10000.0
F32 = jnp.float32
BF16 = jnp.bfloat16
MESH = pl.DeviceIdType.MESH


def scope(name):
    return contextlib.nullcontext()


def rope_tables(count, step, heads):
    half = RK // 2
    inverse = ROPE_BASE ** (-2.0 * np.arange(half, dtype=np.float64) / RK)
    angles = (np.arange(count, dtype=np.float64) * step)[:, None] * inverse[None, :]
    wide = np.tile(np.concatenate([angles, angles], axis=1), (1, heads))
    return np.cos(wide).astype(np.float32), np.sin(wide).astype(np.float32)


def remote(src, dst, send, recv, **where):
    return pltpu.make_async_remote_copy(
        src_ref=src, dst_ref=dst, send_sem=send, recv_sem=recv,
        device_id=where, device_id_type=MESH,
    )


def rows_of(index, size):
    return pl.ds(pl.multiple_of(index * size, size), size)


def mm(a, b):
    return jnp.dot(a, b, preferred_element_type=F32)


def mm_t(a, b):
    return lax.dot_general(a, b, (((1,), (1,)), ((), ())), preferred_element_type=F32)


def tm_m(a, b):
    return lax.dot_general(a, b, (((0,), (0,)), ((), ())), preferred_element_type=F32)


class Spread:
    def __init__(self, place, buf, size, send, recv, src=None):
        self.place, self.buf, self.size, self.send, self.recv, self.src = place, buf, size, send, recv, src

    def own(self, c, k):
        tp, partner, across, _ = self.place
        rows = rows_of(c, self.size)
        src = self.buf.at[tp, rows, :] if self.src is None else self.src.at[rows, :]
        return remote(src, self.buf.at[tp, rows, :], self.send.at[k, c], self.recv.at[tp, c],
                      tp=partner if k == 0 else across(k))

    def got(self, c, slot, k=0):
        rows = rows_of(c, self.size)
        block = self.buf.at[slot, rows, :]
        return remote(block, block, self.send.at[k, c], self.recv.at[slot, c], tp=self.place[1])

    def start(self, c):
        n_chips = self.place[3]
        for k in list(range(1, n_chips)) + [0]:
            self.own(c, k).start()

    def relay(self, c):
        _, _, across, n_chips = self.place
        for k in range(1, n_chips):
            slot = across(k)
            self.got(c, slot).wait_recv()
            self.got(c, slot, n_chips - 1 + k).start()

    def settle(self, c):
        _, partner, across, n_chips = self.place
        self.got(c, partner).wait_recv()
        for k in range(1, n_chips):
            slot = across(k)
            self.got(c, slot + 1 - 2 * lax.rem(slot, 2)).wait_recv()

    def drain(self, c):
        _, _, across, n_chips = self.place
        for k in range(n_chips):
            self.own(c, k).wait_send()
        for k in range(1, n_chips):
            self.got(c, across(k), n_chips - 1 + k).wait_send()


def kernel(cfg, *refs):
    n_buf, n_small = len(cfg["buffers"]), 8
    (tokens, w_q, w_k, w_v, w_rq, w_rk, w_rv, w_rg, init, o_att, o_ret) = refs[:11]
    small_hbm = refs[11:11 + n_small - 1]
    out = refs[10 + n_small]
    rest = refs[11 + n_small:]
    w_bufs = rest[:n_buf]
    small = rest[n_buf:n_buf + n_small - 1]
    gain, sink, decay, outer_cos, outer_sin, inner_cos, inner_sin = small
    (wg, gath, xbuf, qs, kbuf, vbuf, matt, mret, qfb, rloc, gs, fterm, bterm, blog, both_in,
     tot_f, tot_b, tots, logs, states, obuf,
     ready, w_sem, wo_sem, tok_sem, small_sem, out_sem,
     tok_send, tok_recv, att_send, att_recv, ret_send, ret_recv,
     pw_send, pw_recv, w1_send, w2_send, w_recv,
     halo_send, halo_recv, tot_send, tot_recv, log_send, log_recv) = rest[n_buf + n_small - 1:]
    n_tp, n_sp, n_chips, chunks = cfg["n_tp"], cfg["n_sp"], cfg["n_chips"], cfg["chunks"]
    chan, heads, ret, kv = cfg["chan"], cfg["heads"], cfg["ret"], cfg["kv"]
    rows = chunks * CHUNK
    width = n_tp * chan
    groups = heads // kv
    seq_len = rows * n_sp
    att_w, ret_w = heads * HD, ret * RV
    piece = (att_w + ret_w) // n_sp
    per = CHUNK // MIX
    mixes = rows // MIX
    sp = lax.axis_index("sp")
    tp = lax.axis_index("tp")
    core = lax.rem(tp, 2)
    chip = lax.div(tp, 2)
    partner = chip * 2 + 1 - core

    def across(k):
        return lax.rem(chip + k, n_chips) * 2 + core

    place = (tp, partner, across, n_chips)
    tok = Spread(place, gath, CHUNK, tok_send, tok_recv, src=tokens)
    atd = Spread(place, matt, MIX, att_send, att_recv)
    rtd = Spread(place, mret, MIX, ret_send, ret_recv)

    barrier = pltpu.get_barrier_semaphore()
    for k in range(1, n_tp):
        pl.semaphore_signal(barrier, inc=1, device_id={"tp": lax.rem(tp + k, n_tp)}, device_id_type=MESH)

    @pl.when(sp == 0)
    def _():
        for k in range(1, n_sp):
            pl.semaphore_signal(barrier, inc=1, device_id={"sp": k}, device_id_type=MESH)

    token_copy = pltpu.make_async_copy(tokens, gath.at[tp], tok_sem)
    token_copy.start()
    local = [pltpu.make_async_copy(a, b, small_sem.at[i]) for i, (a, b) in enumerate(zip(small_hbm, small))]
    local.append(pltpu.make_async_copy(init, states, small_sem.at[n_small - 1]))
    weights = (w_q, w_k, w_v, w_rq, w_rk, w_rv, w_rg)
    for i, (w_ref, (b, off, cols)) in enumerate(zip(weights, cfg["places"])):
        dst = w_bufs[b].at[:, pl.ds(off, cols)] if cfg["joined"] else w_bufs[b]
        local.append(pltpu.make_async_copy(w_ref, dst, w_sem.at[i]))
    halves = ((o_att, 0, att_w), (o_ret, att_w, ret_w))

    def columns(t):
        return pl.ds(pl.multiple_of(t * chan, chan), chan)

    for i, (src, first, count) in enumerate(halves):
        local.append(pltpu.make_async_copy(
            src.at[:, columns(tp)], wg.at[tp, pl.ds(first, count), :], wo_sem.at[i]))
    for copy in local:
        copy.start()

    with scope("barrier"):
        @pl.when(sp == 0)
        def _():
            pl.semaphore_wait(barrier, n_tp - 1)

        @pl.when(sp > 0)
        def _():
            pl.semaphore_wait(barrier, n_tp)
            pl.semaphore_signal(ready, inc=1, device_id={"sp": 0}, device_id_type=MESH)

    others = [lax.rem(chip + k, n_chips) * 2 + p for k in range(1, n_chips) for p in range(2)]

    def w_copy(t, e, send, **where):
        block = wg.at[t, rows_of(e, piece), :]
        return remote(block, block, send, w_recv.at[t, e], **where)

    def w_first(src, first):
        for t in others:
            remote(src.at[rows_of(sp - first // piece, piece), columns(t)], wg.at[tp, rows_of(sp, piece), :],
                   w1_send.at[t], w_recv.at[tp, sp], tp=t).start()

    @pl.when(sp * piece < att_w)
    def _():
        w_first(o_att, 0)

    @pl.when(sp * piece >= att_w)
    def _():
        w_first(o_ret, att_w)

    def first_sends(c, carry):
        tok.start(c)
        return carry

    lax.fori_loop(0, chunks, first_sends, 0)

    def w_partner(i):
        src, first, count = halves[i]
        return remote(src.at[:, columns(partner)], wg.at[tp, pl.ds(first, count), :],
                      pw_send.at[i], pw_recv.at[i], tp=partner)

    for i in range(2):
        w_partner(i).start()

    with scope("lwait"):
        for copy in local:
            copy.wait()
        token_copy.wait()

    for h in range(ret):
        total = jnp.sum(decay[h:h + 1, :], axis=1, keepdims=True)
        logs[sp, h] = jnp.broadcast_to(total, (8, 128))

    @pl.when(sp == 0)
    def _():
        kbuf[0:WINDOW, :] = jnp.zeros((WINDOW, kbuf.shape[1]), BF16)
        vbuf[0:WINDOW, :] = jnp.zeros((WINDOW, vbuf.shape[1]), BF16)

    @pl.when(sp == n_sp - 1)
    def _():
        kbuf[rows + WINDOW:, :] = jnp.zeros((WINDOW, kbuf.shape[1]), BF16)
        vbuf[rows + WINDOW:, :] = jnp.zeros((WINDOW, vbuf.shape[1]), BF16)

    with scope("ready"):
        @pl.when(sp == 0)
        def _():
            pl.semaphore_wait(ready, n_sp - 1)
            for k in range(1, n_sp):
                pl.semaphore_signal(ready, inc=1, device_id={"sp": k}, device_id_type=MESH)

        @pl.when(sp > 0)
        def _():
            pl.semaphore_wait(ready, 1)

    def log_copy(k):
        return remote(logs.at[sp], logs.at[sp], log_send.at[k], log_recv.at[sp], sp=lax.rem(sp + k, n_sp))

    def log_arrival(k):
        other = lax.rem(sp + k, n_sp)
        return remote(logs.at[other], logs.at[other], log_send.at[k], log_recv.at[other], sp=other)

    for k in range(1, n_sp):
        log_copy(k).start()

    with scope("wfwd"):
        for t in others:
            w_copy(t, sp, w2_send.at[t, 0], sp=sp).wait_recv()

        def w_pass(k, carry):
            for t in others:
                w_copy(t, sp, w2_send.at[t, k], sp=lax.rem(sp + k, n_sp)).start()
            return carry

        lax.fori_loop(1, n_sp, w_pass, 0)

    row_i = lax.broadcasted_iota(jnp.int32, (CHUNK, CHUNK), 0)
    col_i = lax.broadcasted_iota(jnp.int32, (CHUNK, CHUNK), 1)
    rw = ret * RK
    p_row = lax.broadcasted_iota(jnp.int32, (rw, rw), 0)
    p_col = lax.broadcasted_iota(jnp.int32, (rw, rw), 1)
    first_half = lax.rem(p_col, RK) < RK // 2
    swap = jnp.where(
        first_half & (p_row == p_col + RK // 2), -1.0,
        jnp.where(jnp.logical_not(first_half) & (p_row == p_col - RK // 2), 1.0, 0.0),
    ).astype(BF16)

    def attend(i):
        here = rows_of(i, MIX)
        span = pl.ds(pl.multiple_of(i * MIX, MIX), MIX + 2 * WINDOW)
        shape = (MIX, MIX + 2 * WINDOW)
        q_i = lax.broadcasted_iota(jnp.int32, shape, 0)
        k_i = lax.broadcasted_iota(jnp.int32, shape, 1)
        key_pos = k_i + (sp * rows + i * MIX - WINDOW)
        allowed = (k_i >= q_i) & (k_i <= q_i + 2 * WINDOW) & (key_pos >= 0) & (key_pos < seq_len)
        allowed = jnp.concatenate([allowed.astype(F32)] * groups, axis=0) > 0.5
        done = []
        for g in range(kv):
            query = jnp.concatenate(
                [qs[here, (g * groups + j) * HD:(g * groups + j + 1) * HD] for j in range(groups)], axis=0)
            key = kbuf[span, g * HD:(g + 1) * HD]
            value = vbuf[span, g * HD:(g + 1) * HD]
            scores = jnp.where(allowed, mm_t(query, key), -jnp.inf)
            sink_col = jnp.concatenate(
                [jnp.broadcast_to(sink[0:1, g * groups + j:g * groups + j + 1], (MIX, 1))
                 for j in range(groups)], axis=0)
            top = jnp.maximum(jnp.max(scores, axis=1, keepdims=True), sink_col)
            raised = jnp.exp(scores - top)
            denominator = jnp.sum(raised, axis=1, keepdims=True) + jnp.exp(sink_col - top)
            result = mm(raised.astype(BF16), value) / denominator
            for j in range(groups):
                done.append(result[j * MIX:(j + 1) * MIX])
        matt[tp, here, :] = jnp.concatenate(done, axis=1).astype(BF16)
        atd.start(i)

    left, right = sp - 1, sp + 1

    def halo(side, i, where):
        buf = (kbuf, vbuf)[i]
        src, dst = ((rows, 0), (WINDOW, rows + WINDOW))[side]
        return remote(buf.at[pl.ds(src, WINDOW), :], buf.at[pl.ds(dst, WINDOW), :],
                      halo_send.at[side, i], halo_recv.at[side, i], sp=where)

    def chunk(c, last):
        here = rows_of(c, CHUNK)
        with scope("x1"):
            tok.relay(c)
        with scope("x2"):
            tok.settle(c)
        ctx = scope("phaseA")
        ctx.__enter__()
        squares = jnp.zeros((CHUNK, 1), F32)
        for s in range(n_tp):
            part = gath[s, here, :].astype(F32)
            squares = squares + jnp.sum(part * part, axis=1, keepdims=True)
            xbuf[:, s * chan:(s + 1) * chan] = (part * gain[0:1, s * chan:(s + 1) * chan]).astype(BF16)
        inv_rms = lax.rsqrt(squares / width + NORM_EPS)
        found = {}

        def product(first):
            for b, off, cols, names in cfg["dots"]:
                if (names[0][0] in ("rq", "rk", "rv")) != first:
                    continue
                block = (mm(xbuf[...], w_bufs[b][:, off:off + cols]) * inv_rms).astype(BF16)
                at = 0
                for name, count in names:
                    found[name] = block[:, at:at + count]
                    at += count

        product(True)
        spot = sp * chunks + c
        oc, os_ = outer_cos[pl.ds(spot, 1), :], outer_sin[pl.ds(spot, 1), :]
        ic, is_ = inner_cos[...], inner_sin[...]
        cosine = oc * ic - os_ * is_
        sine = os_ * ic + oc * is_
        query_rot = found["rq"].astype(F32) * cosine + mm(found["rq"], swap) * sine
        key_rot = (found["rk"].astype(F32) * cosine + mm(found["rk"], swap) * sine) * RK ** -0.5
        kept = []
        for h in range(ret):
            log_row = decay[h:h + 1, here]
            wide = jnp.broadcast_to(log_row, (CHUNK, CHUNK))
            log_col = jnp.sum(jnp.where(row_i == col_i, wide, 0.0), axis=1, keepdims=True)
            cum_col = jnp.sum(jnp.where(col_i <= row_i, wide, 0.0), axis=1, keepdims=True)
            total = jnp.sum(log_row, axis=1, keepdims=True)
            key = key_rot[:, h * RK:(h + 1) * RK]
            value = found["rv"][:, h * RV:(h + 1) * RV]
            up = jnp.exp(cum_col)
            down = jnp.exp(jnp.minimum(total - cum_col, 0.0))
            both = jnp.concatenate([key * down, key * up], axis=1).astype(BF16)
            terms = tm_m(both, value)
            fterm[h, c] = terms[:RK]
            bterm[h, c] = terms[RK:]
            blog[h, c] = jnp.broadcast_to(total, (8, 128))
            kept.append((log_col, cum_col, up, down, key, value))
        ctx.__exit__(None, None, None)
        if last:
            with scope("totals"):
                send_totals()
        ctx = scope("phaseB")
        ctx.__enter__()
        product(False)
        qs[here, :] = found["q"] * jnp.asarray(HD ** -0.5, BF16)
        shifted = pl.ds(pl.multiple_of(c * CHUNK + WINDOW, 128), CHUNK)
        kbuf[shifted, :] = found["k"]
        vbuf[shifted, :] = found["v"]
        gs[here, :] = found["g"]
        for h in range(ret):
            log_col, cum_col, up, down, key, value = kept[h]
            cum_row = jnp.sum(jnp.where(row_i <= col_i, log_col, 0.0), axis=0, keepdims=True)
            query = query_rot[:, h * RK:(h + 1) * RK]
            inner = mm_t(query.astype(BF16), key.astype(BF16)) * jnp.exp(-jnp.abs(cum_col - cum_row))
            rloc[h, here, :] = mm(inner.astype(BF16), value)
            qfb[h, here, :] = jnp.concatenate([query * up, query * down], axis=1).astype(BF16)
        ctx.__exit__(None, None, None)

    def send_totals():
        for h in range(ret):
            state = jnp.zeros((RK, RV), F32)
            back = jnp.zeros((RK, RV), F32)
            for c in range(chunks):
                state = jnp.exp(blog[h, c, 0:1, :]) * state + fterm[h, c]
                back = jnp.exp(blog[h, chunks - 1 - c, 0:1, :]) * back + bterm[h, chunks - 1 - c]
            tot_f[h] = state.astype(BF16)
            tot_b[h] = back.astype(BF16)

        def send_f(d, carry):
            remote(tot_f, tots.at[sp], tot_send.at[d], tot_recv.at[sp], sp=d).start()
            return carry

        def send_b(d, carry):
            remote(tot_b, tots.at[sp], tot_send.at[d], tot_recv.at[sp], sp=d).start()
            return carry

        lax.fori_loop(sp + 1, n_sp, send_f, 0)
        lax.fori_loop(0, sp, send_b, 0)

    def chunk_body(c, carry):
        @pl.when(c >= 2)
        def _():
            with scope("slot"):
                for j in range(per):
                    attend(per * (c - 2) + 1 + j)

        chunk(c, False)

        @pl.when((c == 0) & (sp > 0))
        def _():
            for i in range(2):
                halo(1, i, left).start()

        return carry

    lax.fori_loop(0, chunks - 1, chunk_body, 0)
    early = per * (chunks - 2)
    with scope("slot"):
        for j in range(per):
            attend(early - per + 1 + j)
    chunk(chunks - 1, True)

    @pl.when(sp < n_sp - 1)
    def _():
        for i in range(2):
            halo(0, i, right).start()

    def late(j, carry):
        with scope("late"):
            attend(j + 1)
        with scope("lrelay"):
            atd.relay(j - early + 1)
        return carry

    lax.fori_loop(early, mixes - 2, late, 0)

    @pl.when(sp < n_sp - 1)
    def _():
        for i in range(2):
            halo(1, i, right).wait_recv()

    late(mixes - 2, 0)

    @pl.when(sp > 0)
    def _():
        for i in range(2):
            halo(0, i, left).wait_recv()

    with scope("late"):
        attend(0)
    atd.relay(mixes - early)

    def total_arrival(e):
        return remote(tots.at[e], tots.at[e], tot_send.at[e], tot_recv.at[e], sp=e)

    with scope("states"):
        for k in range(1, n_sp):
            log_arrival(k).wait_recv()

        def from_low(e, carry):
            total_arrival(e).wait_recv()
            for h in range(ret):
                states[0, h] = jnp.exp(logs[e, h, 0:1, :]) * states[0, h] + tots[e, h].astype(F32)
            return carry

        def from_high(i, carry):
            e = n_sp - 1 - i
            total_arrival(e).wait_recv()
            for h in range(ret):
                states[1, h] = jnp.exp(logs[e, h, 0:1, :]) * states[1, h] + tots[e, h].astype(F32)
            return carry

        lax.fori_loop(0, sp, from_low, 0)
        lax.fori_loop(0, n_sp - 1 - sp, from_high, 0)

        for h in range(ret):
            state = states[0, h]
            back = states[1, h]
            for c in range(chunks):
                both_in[h, c, 0:RK] = state.astype(BF16)
                state = jnp.exp(blog[h, c, 0:1, :]) * state + fterm[h, c]
                r = chunks - 1 - c
                both_in[h, r, RK:2 * RK] = back.astype(BF16)
                back = jnp.exp(blog[h, r, 0:1, :]) * back + bterm[h, r]

    def retain(c):
        here = rows_of(c, MIX)
        at = lax.div(c, per)
        pieces = []
        for h in range(ret):
            combined = rloc[h, here, :] + mm(qfb[h, here, :], both_in[h, at])
            centered = combined - jnp.mean(combined, axis=1, keepdims=True)
            normed = centered * lax.rsqrt(jnp.mean(centered * centered, axis=1, keepdims=True) + NORM_EPS)
            gate = gs[here, h * RV:(h + 1) * RV].astype(F32)
            pieces.append((gate / (1.0 + jnp.exp(-gate)) * normed).astype(BF16))
        mret[tp, here, :] = jnp.concatenate(pieces, axis=1) if ret > 1 else pieces[0]
        rtd.start(c)

    def ret_body(c, carry):
        with scope("retain"):
            retain(c)
        return carry

    lax.fori_loop(0, mixes, ret_body, 0)

    def att_rest(j, carry):
        atd.relay(lax.rem(j - early + 1, mixes))
        return carry

    with scope("attrest"):
        lax.fori_loop(mixes, mixes + early, att_rest, 0)

    with scope("wsettle"):
        for i in range(2):
            w_partner(i).wait_recv()

        def w_settle(k, carry):
            for t in others:
                w_copy(t, lax.rem(sp + k, n_sp), w2_send.at[t, k], sp=sp).wait_recv()
            return carry

        lax.fori_loop(1, n_sp, w_settle, 0)

    def out_copy(c):
        return pltpu.make_async_copy(obuf.at[rows_of(c, MIX), :], out.at[rows_of(c, MIX), :], out_sem.at[c])

    def mix(c):
        here = rows_of(c, MIX)
        with scope("msettle"):
            atd.settle(c)
            rtd.settle(c)
        with scope("mix"):
            total = jnp.zeros((MIX, chan), F32)
            for t in range(n_tp):
                total = total + mm(matt[t, here, :], wg[t, 0:att_w, :])
                total = total + mm(mret[t, here, :], wg[t, att_w:att_w + ret_w, :])
            obuf[here, :] = total.astype(BF16)
            out_copy(c).start()

    def mix_body(c, carry):
        @pl.when(c < mixes)
        def _():
            with scope("rrelay"):
                rtd.relay(c)

        @pl.when(c > 0)
        def _():
            mix(c - 1)

        return carry

    lax.fori_loop(0, mixes + 1, mix_body, 0)

    with scope("drain"):
        def drain_chunks(c, carry):
            tok.drain(c)
            return carry

        def drain_mixes(c, carry):
            atd.drain(c)
            rtd.drain(c)
            out_copy(c).wait()
            return carry

        def drain_w(k, carry):
            for t in others:
                w_copy(t, sp, w2_send.at[t, k], sp=sp).wait_send()
            return carry

        lax.fori_loop(0, chunks, drain_chunks, 0)
        lax.fori_loop(0, mixes, drain_mixes, 0)
        lax.fori_loop(1, n_sp, drain_w, 0)
        for i in range(2):
            w_partner(i).wait_send()
        for t in others:
            w_copy(tp, sp, w1_send.at[t], tp=t).wait_send()

        @pl.when(sp > 0)
        def _():
            for i in range(2):
                halo(1, i, left).wait_send()

        @pl.when(sp < n_sp - 1)
        def _():
            for i in range(2):
                halo(0, i, right).wait_send()

        for k in range(1, n_sp):
            log_copy(k).wait_send()

        def sent_total(d, carry):
            total_arrival(d).wait_send()
            return carry

        lax.fori_loop(sp + 1, n_sp, sent_total, 0)
        lax.fori_loop(0, sp, sent_total, 0)


def body(n_sp, n_tp, tokens, norm_gain, w_q, w_k, w_v, w_rq, w_rk, w_rv, w_rg, att_sink,
         decay_log, init_state, out_att, out_ret):
    rows, chan = tokens.shape
    width = n_tp * chan
    ret = decay_log.shape[0]
    heads = att_sink.shape[0]
    kv_cols = w_k.shape[1]
    kv = kv_cols // HD
    chunks = rows // CHUNK
    n_chips = n_tp // 2
    weights = (w_q, w_k, w_v, w_rq, w_rk, w_rv, w_rg)
    names = ("q", "k", "v", "rq", "rk", "rv", "g")
    cols = [w.shape[1] for w in weights]
    joined = all(count % 128 == 0 for count in cols)
    places, dots = [], []
    if joined:
        buffers = [sum(cols)]
        at = 0
        for count in cols:
            places.append((0, at, count))
            at += count
        for group in ((3, 4), (5,), (1, 2), (0,), (6,)):
            dots.append((0, places[group[0]][1], sum(cols[i] for i in group),
                         tuple((names[i], cols[i]) for i in group)))
    else:
        buffers = cols
        for i, count in enumerate(cols):
            places.append((i, 0, count))
            dots.append((i, 0, count, ((names[i], count),)))
    cfg = dict(n_sp=n_sp, n_tp=n_tp, n_chips=n_chips, chunks=chunks, chan=chan, heads=heads,
               ret=ret, kv=kv, buffers=buffers, places=places, dots=dots, joined=joined)
    tables = rope_tables(n_sp * chunks, CHUNK, ret) + rope_tables(CHUNK, 1, ret)
    small = [norm_gain.reshape(1, width), att_sink.reshape(1, heads), decay_log]
    small += [jnp.asarray(t) for t in tables]
    anyw = pl.BlockSpec(memory_space=pl.ANY)
    dma = pltpu.SemaphoreType.DMA
    att_w, ret_w = heads * HD, ret * RV
    mixes = rows // MIX
    scratch = [pltpu.VMEM((width, count), BF16) for count in buffers] + [
        pltpu.VMEM(a.shape, F32) for a in small] + [
        pltpu.VMEM((n_tp, att_w + ret_w, chan), BF16),
        pltpu.VMEM((n_tp, rows, chan), BF16),
        pltpu.VMEM((CHUNK, width), BF16),
        pltpu.VMEM((rows, att_w), BF16),
        pltpu.VMEM((rows + 2 * WINDOW, kv_cols), BF16),
        pltpu.VMEM((rows + 2 * WINDOW, kv_cols), BF16),
        pltpu.VMEM((n_tp, rows, att_w), BF16),
        pltpu.VMEM((n_tp, rows, ret_w), BF16),
        pltpu.VMEM((ret, rows, 2 * RK), BF16),
        pltpu.VMEM((ret, rows, RV), F32),
        pltpu.VMEM((rows, ret_w), BF16),
        pltpu.VMEM((ret, chunks, RK, RV), F32),
        pltpu.VMEM((ret, chunks, RK, RV), F32),
        pltpu.VMEM((ret, chunks, 8, 128), F32),
        pltpu.VMEM((ret, chunks, 2 * RK, RV), BF16),
        pltpu.VMEM((ret, RK, RV), BF16),
        pltpu.VMEM((ret, RK, RV), BF16),
        pltpu.VMEM((n_sp, ret, RK, RV), BF16),
        pltpu.VMEM((n_sp, ret, 8, 128), F32),
        pltpu.VMEM((2, ret, RK, RV), F32),
        pltpu.VMEM((rows, chan), BF16),
        pltpu.SemaphoreType.REGULAR,
        dma((7,)), dma((2,)), dma, dma((8,)), dma((mixes,)),
        dma((2 * n_chips, chunks)), dma((n_tp, chunks)),
        dma((2 * n_chips, mixes)), dma((n_tp, mixes)),
        dma((2 * n_chips, mixes)), dma((n_tp, mixes)),
        dma((2,)), dma((2,)), dma((n_tp,)), dma((n_tp, n_sp)), dma((n_tp, n_sp)),
        dma((2, 2)), dma((2, 2)),
        dma((n_sp,)), dma((n_sp,)),
        dma((n_sp,)), dma((n_sp,)),
    ]
    return pl.pallas_call(
        functools.partial(kernel, cfg),
        out_shape=jax.ShapeDtypeStruct((rows, chan), BF16),
        in_specs=[anyw] * (11 + len(small)),
        out_specs=anyw,
        scratch_shapes=scratch,
        compiler_params=pltpu.CompilerParams(
            collective_id=0, has_side_effects=True, vmem_limit_bytes=60 * 1024 * 1024),
    )(tokens, *weights, init_state, out_att, out_ret, *small)


def solution(mesh):
    n_sp, n_tp = mesh.shape["sp"], mesh.shape["tp"]
    in_specs = (
        P("sp", "tp"),
        P(),
        P(None, "tp"),
        P(None, "tp"),
        P(None, "tp"),
        P(None, "tp"),
        P(None, "tp"),
        P(None, "tp"),
        P(None, "tp"),
        P("tp"),
        P("tp", "sp"),
        P(None, "tp", None, None),
        P("tp", None),
        P("tp", None),
    )
    return jax.shard_map(functools.partial(body, n_sp, n_tp), mesh=mesh, in_specs=in_specs,
                         out_specs=P("sp", "tp"), check_vma=False)
```

```python
import contextlib
import functools

import jax
import jax.numpy as jnp
import numpy as np
from jax import lax
from jax.experimental import pallas as pl
from jax.experimental.pallas import tpu as pltpu
from jax.sharding import PartitionSpec as P

HD = 64
RK = 64
RV = 128
WINDOW = 128
CHUNK = 256
MIX = 128
NORM_EPS = 1e-06
ROPE_BASE = 10000.0
F32 = jnp.float32
BF16 = jnp.bfloat16
MESH = pl.DeviceIdType.MESH


def scope(name):
    return contextlib.nullcontext()


def rope_tables(count, step, heads):
    half = RK // 2
    inverse = ROPE_BASE ** (-2.0 * np.arange(half, dtype=np.float64) / RK)
    angles = (np.arange(count, dtype=np.float64) * step)[:, None] * inverse[None, :]
    wide = np.tile(np.concatenate([angles, angles], axis=1), (1, heads))
    return np.cos(wide).astype(np.float32), np.sin(wide).astype(np.float32)


def remote(src, dst, send, recv, **where):
    return pltpu.make_async_remote_copy(
        src_ref=src, dst_ref=dst, send_sem=send, recv_sem=recv,
        device_id=where, device_id_type=MESH,
    )


def rows_of(index, size):
    return pl.ds(pl.multiple_of(index * size, size), size)


def mm(a, b):
    return jnp.dot(a, b, preferred_element_type=F32)


def mm_t(a, b):
    return lax.dot_general(a, b, (((1,), (1,)), ((), ())), preferred_element_type=F32)


def tm_m(a, b):
    return lax.dot_general(a, b, (((0,), (0,)), ((), ())), preferred_element_type=F32)


class Spread:
    def __init__(self, place, buf, columns, size, send, cross, settled, src=None):
        self.place, self.buf, self.columns, self.size = place, buf, columns, size
        self.send, self.cross, self.settled, self.src = send, cross, settled, src

    def block(self, slot, c):
        return self.buf.at[slot, rows_of(c, self.size), self.columns]

    def start(self, c):
        tp, partner, across, n_chips = self.place
        src = self.block(tp, c) if self.src is None else self.src.at[rows_of(c, self.size), :]
        for k in range(1, n_chips):
            remote(src, self.block(tp, c), self.send, self.cross.at[n_chips - k - 1, c], tp=across(k)).start()
        remote(src, self.block(tp, c), self.send, self.settled.at[c], tp=partner).start()

    def relay(self, c):
        _, partner, across, n_chips = self.place
        for k in range(1, n_chips):
            block = self.block(across(k), c)
            remote(block, block, self.send, self.cross.at[k - 1, c], tp=partner).wait_recv()
            remote(block, block, self.send, self.settled.at[c], tp=partner).start()


def kernel(cfg, *refs):
    n_buf, n_small = len(cfg["buffers"]), 8
    (tokens, w_q, w_k, w_v, w_rq, w_rk, w_rv, w_rg, init, o_att, o_ret) = refs[:11]
    small_hbm = refs[11:11 + n_small - 1]
    out = refs[10 + n_small]
    rest = refs[11 + n_small:]
    w_bufs = rest[:n_buf]
    small = rest[n_buf:n_buf + n_small - 1]
    gain, sink, decay, outer_cos, outer_sin, inner_cos, inner_sin = small
    (wg, gath, xbuf, qs, kbuf, vbuf, mx, qfb, rloc, gs, fterm, bterm, blog, both_in,
     tot_f, tot_b, tots, logs, states, obuf,
     ready, w_sem, wo_sem, tok_sem, small_sem, out_sem,
     tok_send, tok_cross, tok_settled, mix_send, att_cross, ret_cross, mix_settled,
     pw_send, pw_recv, w_send, w_recv,
     halo_send, halo_recv, tot_send, tot_recv, log_send, log_recv) = rest[n_buf + n_small - 1:]
    n_tp, n_sp, n_chips, chunks = cfg["n_tp"], cfg["n_sp"], cfg["n_chips"], cfg["chunks"]
    chan, heads, ret, kv = cfg["chan"], cfg["heads"], cfg["ret"], cfg["kv"]
    rows = chunks * CHUNK
    width = n_tp * chan
    groups = heads // kv
    seq_len = rows * n_sp
    att_w, ret_w = heads * HD, ret * RV
    piece = (att_w + ret_w) // n_sp
    per = CHUNK // MIX
    mixes = rows // MIX
    sp = lax.axis_index("sp")
    tp = lax.axis_index("tp")
    core = lax.rem(tp, 2)
    chip = lax.div(tp, 2)
    partner = chip * 2 + 1 - core

    def across(k):
        return lax.rem(chip + k, n_chips) * 2 + core

    place = (tp, partner, across, n_chips)
    tok = Spread(place, gath, slice(None), CHUNK, tok_send, tok_cross, tok_settled, src=tokens)
    atd = Spread(place, mx, pl.ds(0, att_w), MIX, mix_send, att_cross, mix_settled)
    rtd = Spread(place, mx, pl.ds(att_w, ret_w), MIX, mix_send, ret_cross, mix_settled)

    def arrived(ref, sem):
        pltpu.make_async_copy(ref, ref, sem).wait()

    barrier = pltpu.get_barrier_semaphore()
    for k in range(1, n_tp):
        pl.semaphore_signal(barrier, inc=1, device_id={"tp": lax.rem(tp + k, n_tp)}, device_id_type=MESH)

    @pl.when(sp == 0)
    def _():
        for k in range(1, n_sp):
            pl.semaphore_signal(barrier, inc=1, device_id={"sp": k}, device_id_type=MESH)

    token_copy = pltpu.make_async_copy(tokens, gath.at[tp], tok_sem)
    token_copy.start()
    local = [pltpu.make_async_copy(a, b, small_sem.at[i]) for i, (a, b) in enumerate(zip(small_hbm, small))]
    local.append(pltpu.make_async_copy(init, states, small_sem.at[n_small - 1]))
    weights = (w_q, w_k, w_v, w_rq, w_rk, w_rv, w_rg)
    for w_ref, (b, off, cols) in zip(weights, cfg["places"]):
        dst = w_bufs[b].at[:, pl.ds(off, cols)] if cfg["joined"] else w_bufs[b]
        pltpu.make_async_copy(w_ref, dst, w_sem.at[b]).start()
    halves = ((o_att, 0, att_w), (o_ret, att_w, ret_w))

    def columns(t):
        return pl.ds(pl.multiple_of(t * chan, chan), chan)

    for src, first, count in halves:
        pltpu.make_async_copy(src.at[:, columns(tp)], wg.at[tp, pl.ds(first, count), :], wo_sem).start()
    for copy in local:
        copy.start()

    with scope("barrier"):
        @pl.when(sp == 0)
        def _():
            pl.semaphore_wait(barrier, n_tp - 1)

        @pl.when(sp > 0)
        def _():
            pl.semaphore_wait(barrier, n_tp)
            pl.semaphore_signal(ready, inc=1, device_id={"sp": 0}, device_id_type=MESH)

    others = [lax.rem(chip + k, n_chips) * 2 + p for k in range(1, n_chips) for p in range(2)]

    def w_copy(t, e, send, recv, **where):
        block = wg.at[t, rows_of(e, piece), :]
        return remote(block, block, w_send.at[send], w_recv.at[recv], **where)

    def w_done(sem, pieces):
        left, full = pieces * len(others) * piece, att_w + ret_w
        while left > 0:
            arrived(wg.at[0, 0:min(left, full), :], sem)
            left -= full

    def w_first(src, first):
        for t in others:
            remote(src.at[rows_of(sp - first // piece, piece), columns(t)], wg.at[tp, rows_of(sp, piece), :],
                   w_send.at[0], w_recv.at[0], tp=t).start()

    @pl.when(sp * piece < att_w)
    def _():
        w_first(o_att, 0)

    @pl.when(sp * piece >= att_w)
    def _():
        w_first(o_ret, att_w)

    def order(i):
        return lax.rem(i + chunks - 1, chunks)

    def first_sends(i, carry):
        tok.start(order(i))
        return carry

    lax.fori_loop(0, chunks, first_sends, 0)

    for src, first, count in halves:
        remote(src.at[:, columns(partner)], wg.at[tp, pl.ds(first, count), :], pw_send, pw_recv, tp=partner).start()

    with scope("lwait"):
        for copy in local:
            copy.wait()
        token_copy.wait()
        for i, buf in enumerate(w_bufs):
            arrived(buf, w_sem.at[i])
        arrived(wg.at[tp], wo_sem)

    for h in range(ret):
        total = jnp.sum(decay[h:h + 1, :], axis=1, keepdims=True)
        logs[sp, h] = jnp.broadcast_to(total, (8, 128))

    @pl.when(sp == 0)
    def _():
        kbuf[0:WINDOW, :] = jnp.zeros((WINDOW, kbuf.shape[1]), BF16)
        vbuf[0:WINDOW, :] = jnp.zeros((WINDOW, vbuf.shape[1]), BF16)

    @pl.when(sp == n_sp - 1)
    def _():
        kbuf[rows + WINDOW:, :] = jnp.zeros((WINDOW, kbuf.shape[1]), BF16)
        vbuf[rows + WINDOW:, :] = jnp.zeros((WINDOW, vbuf.shape[1]), BF16)

    with scope("ready"):
        @pl.when(sp == 0)
        def _():
            pl.semaphore_wait(ready, n_sp - 1)
            for k in range(1, n_sp):
                pl.semaphore_signal(ready, inc=1, device_id={"sp": k}, device_id_type=MESH)

        @pl.when(sp > 0)
        def _():
            pl.semaphore_wait(ready, 1)

    for k in range(1, n_sp):
        remote(logs.at[sp], logs.at[sp], log_send, log_recv, sp=lax.rem(sp + k, n_sp)).start()

    beside = sp + 1 - 2 * lax.rem(sp, 2)
    half_sp = n_sp // 2
    with scope("wfwd"):
        w_done(w_recv.at[0], 1)

        def w_pass(k, carry):
            for t in others:
                w_copy(t, sp, 1, 1, sp=lax.rem(sp + 2 * k, n_sp)).start()
            return carry

        lax.fori_loop(1, half_sp, w_pass, 0)
        for t in others:
            w_copy(t, sp, 2, 2, sp=beside).start()

    def w_aside():
        w_done(w_recv.at[1], half_sp - 1)

        def w_over(k, carry):
            for t in others:
                w_copy(t, lax.rem(sp + 2 * k, n_sp), 2, 2, sp=beside).start()
            return carry

        lax.fori_loop(1, half_sp, w_over, 0)

    row_i = lax.broadcasted_iota(jnp.int32, (CHUNK, CHUNK), 0)
    col_i = lax.broadcasted_iota(jnp.int32, (CHUNK, CHUNK), 1)
    rw = ret * RK
    p_row = lax.broadcasted_iota(jnp.int32, (rw, rw), 0)
    p_col = lax.broadcasted_iota(jnp.int32, (rw, rw), 1)
    first_half = lax.rem(p_col, RK) < RK // 2
    swap = jnp.where(
        first_half & (p_row == p_col + RK // 2), -1.0,
        jnp.where(jnp.logical_not(first_half) & (p_row == p_col - RK // 2), 1.0, 0.0),
    ).astype(BF16)

    def attend(i):
        here = rows_of(i, MIX)
        span = pl.ds(pl.multiple_of(i * MIX, MIX), MIX + 2 * WINDOW)
        shape = (MIX, MIX + 2 * WINDOW)
        q_i = lax.broadcasted_iota(jnp.int32, shape, 0)
        k_i = lax.broadcasted_iota(jnp.int32, shape, 1)
        key_pos = k_i + (sp * rows + i * MIX - WINDOW)
        allowed = (k_i >= q_i) & (k_i <= q_i + 2 * WINDOW) & (key_pos >= 0) & (key_pos < seq_len)
        allowed = jnp.concatenate([allowed.astype(F32)] * groups, axis=0) > 0.5
        done = []
        for g in range(kv):
            query = jnp.concatenate(
                [qs[here, (g * groups + j) * HD:(g * groups + j + 1) * HD] for j in range(groups)], axis=0)
            key = kbuf[span, g * HD:(g + 1) * HD]
            value = vbuf[span, g * HD:(g + 1) * HD]
            scores = jnp.where(allowed, mm_t(query, key), -jnp.inf)
            sink_col = jnp.concatenate(
                [jnp.broadcast_to(sink[0:1, g * groups + j:g * groups + j + 1], (MIX, 1))
                 for j in range(groups)], axis=0)
            top = jnp.maximum(jnp.max(scores, axis=1, keepdims=True), sink_col)
            raised = jnp.exp(scores - top)
            denominator = jnp.sum(raised, axis=1, keepdims=True) + jnp.exp(sink_col - top)
            result = mm(raised.astype(BF16), value) / denominator
            for j in range(groups):
                done.append(result[j * MIX:(j + 1) * MIX])
        mx[tp, here, 0:att_w] = jnp.concatenate(done, axis=1).astype(BF16)
        atd.start(i)

    left, right = sp - 1, sp + 1

    def halo(side, i, where):
        buf = (kbuf, vbuf)[i]
        src, dst = ((rows, 0), (WINDOW, rows + WINDOW))[side]
        return remote(buf.at[pl.ds(src, WINDOW), :], buf.at[pl.ds(dst, WINDOW), :],
                      halo_send.at[side], halo_recv.at[side], sp=where)

    def chunk(c, last, between):
        here = rows_of(c, CHUNK)
        with scope("x1"):
            tok.relay(c)
        between()
        with scope("x2"):
            arrived(gath.at[0:n_chips, here, :], tok_settled.at[c])
        ctx = scope("phaseA")
        ctx.__enter__()
        squares = jnp.zeros((CHUNK, 1), F32)
        for s in range(n_tp):
            part = gath[s, here, :].astype(F32)
            squares = squares + jnp.sum(part * part, axis=1, keepdims=True)
            xbuf[:, s * chan:(s + 1) * chan] = (part * gain[0:1, s * chan:(s + 1) * chan]).astype(BF16)
        inv_rms = lax.rsqrt(squares / width + NORM_EPS)
        found = {}

        def product(first):
            for b, off, cols, names in cfg["dots"]:
                if (names[0][0] in ("rq", "rk", "rv")) != first:
                    continue
                block = (mm(xbuf[...], w_bufs[b][:, off:off + cols]) * inv_rms).astype(BF16)
                at = 0
                for name, count in names:
                    found[name] = block[:, at:at + count]
                    at += count

        product(True)
        spot = sp * chunks + c
        oc, os_ = outer_cos[pl.ds(spot, 1), :], outer_sin[pl.ds(spot, 1), :]
        ic, is_ = inner_cos[...], inner_sin[...]
        cosine = oc * ic - os_ * is_
        sine = os_ * ic + oc * is_
        query_rot = found["rq"].astype(F32) * cosine + mm(found["rq"], swap) * sine
        key_rot = (found["rk"].astype(F32) * cosine + mm(found["rk"], swap) * sine) * RK ** -0.5
        kept = []
        for h in range(ret):
            log_row = decay[h:h + 1, here]
            wide = jnp.broadcast_to(log_row, (CHUNK, CHUNK))
            log_col = jnp.sum(jnp.where(row_i == col_i, wide, 0.0), axis=1, keepdims=True)
            cum_col = jnp.sum(jnp.where(col_i <= row_i, wide, 0.0), axis=1, keepdims=True)
            total = jnp.sum(log_row, axis=1, keepdims=True)
            key = key_rot[:, h * RK:(h + 1) * RK]
            value = found["rv"][:, h * RV:(h + 1) * RV]
            up = jnp.exp(cum_col)
            down = jnp.exp(jnp.minimum(total - cum_col, 0.0))
            both = jnp.concatenate([key * down, key * up], axis=1).astype(BF16)
            terms = tm_m(both, value)
            fterm[h, c] = terms[:RK]
            bterm[h, c] = terms[RK:]
            blog[h, c] = jnp.broadcast_to(total, (8, 128))
            kept.append((log_col, cum_col, up, down, key, value))
        ctx.__exit__(None, None, None)
        if last:
            with scope("totals"):
                send_totals()
        ctx = scope("phaseB")
        ctx.__enter__()
        product(False)
        qs[here, :] = found["q"] * jnp.asarray(HD ** -0.5, BF16)
        shifted = pl.ds(pl.multiple_of(c * CHUNK + WINDOW, 128), CHUNK)
        kbuf[shifted, :] = found["k"]
        vbuf[shifted, :] = found["v"]
        gs[here, :] = found["g"]
        for h in range(ret):
            log_col, cum_col, up, down, key, value = kept[h]
            cum_row = jnp.sum(jnp.where(row_i <= col_i, log_col, 0.0), axis=0, keepdims=True)
            query = query_rot[:, h * RK:(h + 1) * RK]
            inner = mm_t(query.astype(BF16), key.astype(BF16)) * jnp.exp(-jnp.abs(cum_col - cum_row))
            rloc[h, here, :] = mm(inner.astype(BF16), value)
            qfb[h, here, :] = jnp.concatenate([query * up, query * down], axis=1).astype(BF16)
        ctx.__exit__(None, None, None)

    def send_totals():
        for h in range(ret):
            state = jnp.zeros((RK, RV), F32)
            back = jnp.zeros((RK, RV), F32)
            for c in range(chunks):
                state = jnp.exp(blog[h, c, 0:1, :]) * state + fterm[h, c]
                back = jnp.exp(blog[h, chunks - 1 - c, 0:1, :]) * back + bterm[h, chunks - 1 - c]
            tot_f[h] = state.astype(BF16)
            tot_b[h] = back.astype(BF16)

        def send_f(d, carry):
            remote(tot_f, tots.at[sp], tot_send, tot_recv, sp=d).start()
            return carry

        def send_b(d, carry):
            remote(tot_b, tots.at[sp], tot_send, tot_recv, sp=d).start()
            return carry

        lax.fori_loop(sp + 1, n_sp, send_f, 0)
        lax.fori_loop(0, sp, send_b, 0)

    def block_of(j):
        return lax.select(j == 0, 0, lax.select(j == 1, mixes - 1, j - 1))

    def halo_wait(side):
        arrived(kbuf.at[0:2 * WINDOW, :], halo_recv.at[side])

    def one(j):
        with scope("attend"):
            attend(j)

    def chunk_body(i, carry):
        c = order(i)

        @pl.when(i == 2)
        def _():
            w_aside()

            @pl.when(sp > 0)
            def _():
                halo_wait(0)
            one(0)

        @pl.when(i > 2)
        def _():
            one(per * (i - 3) + 1)

        def between():
            @pl.when((i == 2) & (sp < n_sp - 1))
            def _():
                halo_wait(1)

            @pl.when(i == 2)
            def _():
                one(mixes - 1)

            @pl.when(i > 2)
            def _():
                one(per * (i - 3) + 2)

        chunk(c, False, between)

        @pl.when((i == 0) & (sp < n_sp - 1))
        def _():
            for b in range(2):
                halo(0, b, right).start()

        @pl.when((i == 1) & (sp > 0))
        def _():
            for b in range(2):
                halo(1, b, left).start()

        return carry

    lax.fori_loop(0, chunks - 1, chunk_body, 0)
    early = per * (chunks - 3) + 1
    one(early - per)
    chunk(chunks - 2, True, lambda: one(early - per + 1))

    def late(j, carry):
        with scope("late"):
            attend(j)
        with scope("lrelay"):
            atd.relay(block_of(j - early))
        return carry

    lax.fori_loop(early, mixes - 1, late, 0)

    with scope("states"):
        arrived(logs.at[0:n_sp - 1], log_recv)
        arrived(tots.at[0:n_sp - 1], tot_recv)

        def from_low(e, carry):
            for h in range(ret):
                states[0, h] = jnp.exp(logs[e, h, 0:1, :]) * states[0, h] + tots[e, h].astype(F32)
            return carry

        def from_high(i, carry):
            e = n_sp - 1 - i
            for h in range(ret):
                states[1, h] = jnp.exp(logs[e, h, 0:1, :]) * states[1, h] + tots[e, h].astype(F32)
            return carry

        lax.fori_loop(0, sp, from_low, 0)
        lax.fori_loop(0, n_sp - 1 - sp, from_high, 0)

        for h in range(ret):
            state = states[0, h]
            back = states[1, h]
            for c in range(chunks):
                both_in[h, c, 0:RK] = state.astype(BF16)
                state = jnp.exp(blog[h, c, 0:1, :]) * state + fterm[h, c]
                r = chunks - 1 - c
                both_in[h, r, RK:2 * RK] = back.astype(BF16)
                back = jnp.exp(blog[h, r, 0:1, :]) * back + bterm[h, r]

    def retain(c):
        here = rows_of(c, MIX)
        at = lax.div(c, per)
        pieces = []
        for h in range(ret):
            combined = rloc[h, here, :] + mm(qfb[h, here, :], both_in[h, at])
            centered = combined - jnp.mean(combined, axis=1, keepdims=True)
            normed = centered * lax.rsqrt(jnp.mean(centered * centered, axis=1, keepdims=True) + NORM_EPS)
            gate = gs[here, h * RV:(h + 1) * RV].astype(F32)
            pieces.append((gate / (1.0 + jnp.exp(-gate)) * normed).astype(BF16))
        mx[tp, here, att_w:att_w + ret_w] = jnp.concatenate(pieces, axis=1) if ret > 1 else pieces[0]
        rtd.start(c)

    def ret_body(c, carry):
        with scope("retain"):
            retain(c)
        return carry

    lax.fori_loop(0, mixes, ret_body, 0)

    def att_rest(j, carry):
        atd.relay(block_of(j))
        return carry

    with scope("attrest"):
        lax.fori_loop(mixes - 1 - early, mixes, att_rest, 0)

    with scope("wsettle"):
        arrived(wg.at[0], pw_recv)
        w_done(w_recv.at[2], half_sp)

    def mix(c):
        here = rows_of(c, MIX)
        with scope("msettle"):
            arrived(mx.at[0:n_chips, here, :], mix_settled.at[c])
        with scope("mix"):
            total = mm(mx[0, here, :], wg[0])
            for t in range(1, n_tp):
                total = total + mm(mx[t, here, :], wg[t])
            obuf[here, :] = total.astype(BF16)
            pltpu.make_async_copy(obuf.at[here, :], out.at[here, :], out_sem).start()

    def mix_body(c, carry):
        @pl.when(c < mixes)
        def _():
            with scope("rrelay"):
                rtd.relay(c)

        @pl.when(c > 0)
        def _():
            mix(c - 1)

        return carry

    lax.fori_loop(0, mixes + 1, mix_body, 0)

    with scope("drain"):
        sent = 2 * n_chips - 1
        arrived(gath.at[0:sent], tok_send)
        arrived(mx.at[0:sent], mix_send)
        arrived(wg.at[0], pw_send)
        w_done(w_send.at[0], 1)
        w_done(w_send.at[1], half_sp - 1)
        w_done(w_send.at[2], half_sp)
        arrived(logs.at[0:n_sp - 1], log_send)
        arrived(tots.at[0:n_sp - 1], tot_send)

        @pl.when(sp < n_sp - 1)
        def _():
            arrived(kbuf.at[0:2 * WINDOW, :], halo_send.at[0])

        @pl.when(sp > 0)
        def _():
            arrived(kbuf.at[0:2 * WINDOW, :], halo_send.at[1])

        arrived(obuf, out_sem)


def body(n_sp, n_tp, tokens, norm_gain, w_q, w_k, w_v, w_rq, w_rk, w_rv, w_rg, att_sink,
         decay_log, init_state, out_att, out_ret):
    rows, chan = tokens.shape
    width = n_tp * chan
    ret = decay_log.shape[0]
    heads = att_sink.shape[0]
    kv_cols = w_k.shape[1]
    kv = kv_cols // HD
    chunks = rows // CHUNK
    n_chips = n_tp // 2
    weights = (w_q, w_k, w_v, w_rq, w_rk, w_rv, w_rg)
    names = ("q", "k", "v", "rq", "rk", "rv", "g")
    cols = [w.shape[1] for w in weights]
    joined = all(count % 128 == 0 for count in cols)
    places, dots = [], []
    if joined:
        buffers = [sum(cols)]
        at = 0
        for count in cols:
            places.append((0, at, count))
            at += count
        for group in ((3, 4), (5,), (1, 2), (0,), (6,)):
            dots.append((0, places[group[0]][1], sum(cols[i] for i in group),
                         tuple((names[i], cols[i]) for i in group)))
    else:
        buffers = cols
        for i, count in enumerate(cols):
            places.append((i, 0, count))
            dots.append((i, 0, count, ((names[i], count),)))
    cfg = dict(n_sp=n_sp, n_tp=n_tp, n_chips=n_chips, chunks=chunks, chan=chan, heads=heads,
               ret=ret, kv=kv, buffers=buffers, places=places, dots=dots, joined=joined)
    tables = rope_tables(n_sp * chunks, CHUNK, ret) + rope_tables(CHUNK, 1, ret)
    small = [norm_gain.reshape(1, width), att_sink.reshape(1, heads), decay_log]
    small += [jnp.asarray(t) for t in tables]
    anyw = pl.BlockSpec(memory_space=pl.ANY)
    dma = pltpu.SemaphoreType.DMA
    att_w, ret_w = heads * HD, ret * RV
    mixes = rows // MIX
    scratch = [pltpu.VMEM((width, count), BF16) for count in buffers] + [
        pltpu.VMEM(a.shape, F32) for a in small] + [
        pltpu.VMEM((n_tp, att_w + ret_w, chan), BF16),
        pltpu.VMEM((n_tp, rows, chan), BF16),
        pltpu.VMEM((CHUNK, width), BF16),
        pltpu.VMEM((rows, att_w), BF16),
        pltpu.VMEM((rows + 2 * WINDOW, kv_cols), BF16),
        pltpu.VMEM((rows + 2 * WINDOW, kv_cols), BF16),
        pltpu.VMEM((n_tp, rows, att_w + ret_w), BF16),
        pltpu.VMEM((ret, rows, 2 * RK), BF16),
        pltpu.VMEM((ret, rows, RV), F32),
        pltpu.VMEM((rows, ret_w), BF16),
        pltpu.VMEM((ret, chunks, RK, RV), F32),
        pltpu.VMEM((ret, chunks, RK, RV), F32),
        pltpu.VMEM((ret, chunks, 8, 128), F32),
        pltpu.VMEM((ret, chunks, 2 * RK, RV), BF16),
        pltpu.VMEM((ret, RK, RV), BF16),
        pltpu.VMEM((ret, RK, RV), BF16),
        pltpu.VMEM((n_sp, ret, RK, RV), BF16),
        pltpu.VMEM((n_sp, ret, 8, 128), F32),
        pltpu.VMEM((2, ret, RK, RV), F32),
        pltpu.VMEM((rows, chan), BF16),
        pltpu.SemaphoreType.REGULAR,
        dma((len(buffers),)), dma, dma, dma((len(small) + 1,)), dma,
        dma, dma((n_chips - 1, chunks)), dma((chunks,)),
        dma, dma((n_chips - 1, mixes)), dma((n_chips - 1, mixes)), dma((mixes,)),
        dma, dma, dma((3,)), dma((3,)),
        dma((2,)), dma((2,)),
        dma, dma, dma, dma,
    ]
    return pl.pallas_call(
        functools.partial(kernel, cfg),
        out_shape=jax.ShapeDtypeStruct((rows, chan), BF16),
        in_specs=[anyw] * (11 + len(small)),
        out_specs=anyw,
        scratch_shapes=scratch,
        compiler_params=pltpu.CompilerParams(
            collective_id=0, has_side_effects=True, vmem_limit_bytes=60 * 1024 * 1024),
    )(tokens, *weights, init_state, out_att, out_ret, *small)


def solution(mesh):
    n_sp, n_tp = mesh.shape["sp"], mesh.shape["tp"]
    in_specs = (
        P("sp", "tp"),
        P(),
        P(None, "tp"),
        P(None, "tp"),
        P(None, "tp"),
        P(None, "tp"),
        P(None, "tp"),
        P(None, "tp"),
        P(None, "tp"),
        P("tp"),
        P("tp", "sp"),
        P(None, "tp", None, None),
        P("tp", None),
        P("tp", None),
    )
    return jax.shard_map(functools.partial(body, n_sp, n_tp), mesh=mesh, in_specs=in_specs,
                         out_specs=P("sp", "tp"), check_vma=False)
```

```python
import contextlib
import functools

import jax
import jax.numpy as jnp
import numpy as np
from jax import lax
from jax.experimental import pallas as pl
from jax.experimental.pallas import tpu as pltpu
from jax.sharding import PartitionSpec as P

HD = 64
RK = 64
RV = 128
WINDOW = 128
CHUNK = 256
MIX = 128
NORM_EPS = 1e-06
ROPE_BASE = 10000.0
F32 = jnp.float32
BF16 = jnp.bfloat16
MESH = pl.DeviceIdType.MESH


def scope(name):
    return contextlib.nullcontext()


def rope_tables(count, step, heads):
    half = RK // 2
    inverse = ROPE_BASE ** (-2.0 * np.arange(half, dtype=np.float64) / RK)
    angles = (np.arange(count, dtype=np.float64) * step)[:, None] * inverse[None, :]
    wide = np.tile(np.concatenate([angles, angles], axis=1), (1, heads))
    return np.cos(wide).astype(np.float32), np.sin(wide).astype(np.float32)


def remote(src, dst, send, recv, **where):
    return pltpu.make_async_remote_copy(
        src_ref=src, dst_ref=dst, send_sem=send, recv_sem=recv,
        device_id=where, device_id_type=MESH,
    )


def rows_of(index, size):
    return pl.ds(pl.multiple_of(index * size, size), size)


def mm(a, b):
    return jnp.dot(a, b, preferred_element_type=F32)


def mm_t(a, b):
    return lax.dot_general(a, b, (((1,), (1,)), ((), ())), preferred_element_type=F32)


def tm_m(a, b):
    return lax.dot_general(a, b, (((0,), (0,)), ((), ())), preferred_element_type=F32)


class Spread:
    def __init__(self, place, buf, columns, size, send, cross, settled, src=None):
        self.place, self.buf, self.columns, self.size = place, buf, columns, size
        self.send, self.cross, self.settled, self.src = send, cross, settled, src

    def block(self, slot, c):
        return self.buf.at[slot, rows_of(c, self.size), self.columns]

    def start(self, c):
        tp, partner, across, n_chips = self.place
        src = self.block(tp, c) if self.src is None else self.src.at[rows_of(c, self.size), :]
        for k in range(1, n_chips):
            remote(src, self.block(tp, c), self.send, self.cross.at[n_chips - k - 1, c], tp=across(k)).start()
        remote(src, self.block(tp, c), self.send, self.settled.at[c], tp=partner).start()

    def relay(self, c):
        _, partner, across, n_chips = self.place
        for k in range(1, n_chips):
            block = self.block(across(k), c)
            remote(block, block, self.send, self.cross.at[k - 1, c], tp=partner).wait_recv()
            remote(block, block, self.send, self.settled.at[c], tp=partner).start()


def kernel(cfg, *refs):
    n_buf, n_small = len(cfg["buffers"]), 8
    (tokens, w_q, w_k, w_v, w_rq, w_rk, w_rv, w_rg, init, o_att, o_ret) = refs[:11]
    small_hbm = refs[11:11 + n_small - 1]
    out = refs[10 + n_small]
    rest = refs[11 + n_small:]
    w_bufs = rest[:n_buf]
    small = rest[n_buf:n_buf + n_small - 1]
    gain, sink, decay, outer_cos, outer_sin, inner_cos, inner_sin = small
    (wg, gath, xbuf, qs, kbuf, vbuf, mx, qfb, rloc, gs, fterm, bterm, blog, both_in,
     tot_f, tot_b, tots, logs, states,
     ready, w_sem, wo_sem, tok_sem, small_sem,
     tok_send, tok_cross, tok_settled, mix_send, att_cross, ret_cross, mix_settled,
     pw_send, pw_recv, w_send, w_recv,
     halo_send, halo_recv, tot_send, tot_recv, log_send, log_recv) = rest[n_buf + n_small - 1:]
    n_tp, n_sp, n_chips, chunks = cfg["n_tp"], cfg["n_sp"], cfg["n_chips"], cfg["chunks"]
    chan, heads, ret, kv = cfg["chan"], cfg["heads"], cfg["ret"], cfg["kv"]
    rows = chunks * CHUNK
    width = n_tp * chan
    groups = heads // kv
    seq_len = rows * n_sp
    att_w, ret_w = heads * HD, ret * RV
    piece = (att_w + ret_w) // n_sp
    per = CHUNK // MIX
    mixes = rows // MIX
    sp = lax.axis_index("sp")
    tp = lax.axis_index("tp")
    core = lax.rem(tp, 2)
    chip = lax.div(tp, 2)
    partner = chip * 2 + 1 - core

    def across(k):
        return lax.rem(chip + k, n_chips) * 2 + core

    place = (tp, partner, across, n_chips)
    tok = Spread(place, gath, slice(None), CHUNK, tok_send, tok_cross, tok_settled, src=tokens)
    atd = Spread(place, mx, pl.ds(0, att_w), MIX, mix_send, att_cross, mix_settled)
    rtd = Spread(place, mx, pl.ds(att_w, ret_w), MIX, mix_send, ret_cross, mix_settled)

    def arrived(ref, sem):
        pltpu.make_async_copy(ref, ref, sem).wait()

    barrier = pltpu.get_barrier_semaphore()
    for k in range(1, n_tp):
        pl.semaphore_signal(barrier, inc=1, device_id={"tp": lax.rem(tp + k, n_tp)}, device_id_type=MESH)

    @pl.when(sp == 0)
    def _():
        for k in range(1, n_sp):
            pl.semaphore_signal(barrier, inc=1, device_id={"sp": k}, device_id_type=MESH)

    token_copy = pltpu.make_async_copy(tokens, gath.at[tp], tok_sem)
    token_copy.start()
    local = [pltpu.make_async_copy(a, b, small_sem.at[i]) for i, (a, b) in enumerate(zip(small_hbm, small))]
    local.append(pltpu.make_async_copy(init, states, small_sem.at[n_small - 1]))
    weights = (w_q, w_k, w_v, w_rq, w_rk, w_rv, w_rg)
    for w_ref, (b, off, cols) in zip(weights, cfg["places"]):
        dst = w_bufs[b].at[:, pl.ds(off, cols)] if cfg["joined"] else w_bufs[b]
        pltpu.make_async_copy(w_ref, dst, w_sem.at[b]).start()
    halves = ((o_att, 0, att_w), (o_ret, att_w, ret_w))

    def columns(t):
        return pl.ds(pl.multiple_of(t * chan, chan), chan)

    for src, first, count in halves:
        pltpu.make_async_copy(src.at[:, columns(tp)], wg.at[tp, pl.ds(first, count), :], wo_sem).start()
    for copy in local:
        copy.start()

    with scope("barrier"):
        @pl.when(sp == 0)
        def _():
            pl.semaphore_wait(barrier, n_tp - 1)

        @pl.when(sp > 0)
        def _():
            pl.semaphore_wait(barrier, n_tp)
            pl.semaphore_signal(ready, inc=1, device_id={"sp": 0}, device_id_type=MESH)

    others = [lax.rem(chip + k, n_chips) * 2 + p for k in range(1, n_chips) for p in range(2)]

    def w_copy(t, e, send, recv, **where):
        block = wg.at[t, rows_of(e, piece), :]
        return remote(block, block, w_send.at[send], w_recv.at[recv], **where)

    def w_done(sem, pieces):
        left, full = pieces * len(others) * piece, att_w + ret_w
        while left > 0:
            arrived(wg.at[0, 0:min(left, full), :], sem)
            left -= full

    def w_first(src, first):
        for t in others:
            remote(src.at[rows_of(sp - first // piece, piece), columns(t)], wg.at[tp, rows_of(sp, piece), :],
                   w_send.at[0], w_recv.at[0], tp=t).start()

    @pl.when(sp * piece < att_w)
    def _():
        w_first(o_att, 0)

    @pl.when(sp * piece >= att_w)
    def _():
        w_first(o_ret, att_w)

    def order(i):
        return lax.rem(i + chunks - 1, chunks)

    def first_sends(i, carry):
        tok.start(order(i))
        return carry

    lax.fori_loop(0, chunks, first_sends, 0)

    for src, first, count in halves:
        remote(src.at[:, columns(partner)], wg.at[tp, pl.ds(first, count), :], pw_send, pw_recv, tp=partner).start()

    with scope("lwait"):
        for copy in local:
            copy.wait()
        token_copy.wait()
        for i, buf in enumerate(w_bufs):
            arrived(buf, w_sem.at[i])
        arrived(wg.at[tp], wo_sem)

    for h in range(ret):
        total = jnp.sum(decay[h:h + 1, :], axis=1, keepdims=True)
        logs[sp, h] = jnp.broadcast_to(total, (8, 128))

    @pl.when(sp == 0)
    def _():
        kbuf[0:WINDOW, :] = jnp.zeros((WINDOW, kbuf.shape[1]), BF16)
        vbuf[0:WINDOW, :] = jnp.zeros((WINDOW, vbuf.shape[1]), BF16)

    @pl.when(sp == n_sp - 1)
    def _():
        kbuf[rows + WINDOW:, :] = jnp.zeros((WINDOW, kbuf.shape[1]), BF16)
        vbuf[rows + WINDOW:, :] = jnp.zeros((WINDOW, vbuf.shape[1]), BF16)

    with scope("ready"):
        @pl.when(sp == 0)
        def _():
            pl.semaphore_wait(ready, n_sp - 1)
            for k in range(1, n_sp):
                pl.semaphore_signal(ready, inc=1, device_id={"sp": k}, device_id_type=MESH)

        @pl.when(sp > 0)
        def _():
            pl.semaphore_wait(ready, 1)

    for k in range(1, n_sp):
        remote(logs.at[sp], logs.at[sp], log_send, log_recv, sp=lax.rem(sp + k, n_sp)).start()

    beside = sp + 1 - 2 * lax.rem(sp, 2)
    half_sp = n_sp // 2
    with scope("wfwd"):
        w_done(w_recv.at[0], 1)

        def w_pass(k, carry):
            for t in others:
                w_copy(t, sp, 1, 1, sp=lax.rem(sp + 2 * k, n_sp)).start()
            return carry

        lax.fori_loop(1, half_sp, w_pass, 0)
        for t in others:
            w_copy(t, sp, 2, 2, sp=beside).start()

    def w_aside():
        w_done(w_recv.at[1], half_sp - 1)

        def w_over(k, carry):
            for t in others:
                w_copy(t, lax.rem(sp + 2 * k, n_sp), 2, 2, sp=beside).start()
            return carry

        lax.fori_loop(1, half_sp, w_over, 0)

    row_i = lax.broadcasted_iota(jnp.int32, (CHUNK, CHUNK), 0)
    col_i = lax.broadcasted_iota(jnp.int32, (CHUNK, CHUNK), 1)
    rw = ret * RK
    p_row = lax.broadcasted_iota(jnp.int32, (rw, rw), 0)
    p_col = lax.broadcasted_iota(jnp.int32, (rw, rw), 1)
    first_half = lax.rem(p_col, RK) < RK // 2
    swap = jnp.where(
        first_half & (p_row == p_col + RK // 2), -1.0,
        jnp.where(jnp.logical_not(first_half) & (p_row == p_col - RK // 2), 1.0, 0.0),
    ).astype(BF16)

    def attend(i):
        here = rows_of(i, MIX)
        span = pl.ds(pl.multiple_of(i * MIX, MIX), MIX + 2 * WINDOW)
        shape = (MIX, MIX + 2 * WINDOW)
        q_i = lax.broadcasted_iota(jnp.int32, shape, 0)
        k_i = lax.broadcasted_iota(jnp.int32, shape, 1)
        key_pos = k_i + (sp * rows + i * MIX - WINDOW)
        allowed = (k_i >= q_i) & (k_i <= q_i + 2 * WINDOW) & (key_pos >= 0) & (key_pos < seq_len)
        allowed = jnp.concatenate([allowed.astype(F32)] * groups, axis=0) > 0.5
        done = []
        for g in range(kv):
            query = jnp.concatenate(
                [qs[here, (g * groups + j) * HD:(g * groups + j + 1) * HD] for j in range(groups)], axis=0)
            key = kbuf[span, g * HD:(g + 1) * HD]
            value = vbuf[span, g * HD:(g + 1) * HD]
            scores = jnp.where(allowed, mm_t(query, key), -jnp.inf)
            sink_col = jnp.concatenate(
                [jnp.broadcast_to(sink[0:1, g * groups + j:g * groups + j + 1], (MIX, 1))
                 for j in range(groups)], axis=0)
            top = jnp.maximum(jnp.max(scores, axis=1, keepdims=True), sink_col)
            raised = jnp.exp(scores - top)
            denominator = jnp.sum(raised, axis=1, keepdims=True) + jnp.exp(sink_col - top)
            result = mm(raised.astype(BF16), value) / denominator
            for j in range(groups):
                done.append(result[j * MIX:(j + 1) * MIX])
        mx[tp, here, 0:att_w] = jnp.concatenate(done, axis=1).astype(BF16)
        atd.start(i)

    left, right = sp - 1, sp + 1

    def halo(side, i, where):
        buf = (kbuf, vbuf)[i]
        src, dst = ((rows, 0), (WINDOW, rows + WINDOW))[side]
        return remote(buf.at[pl.ds(src, WINDOW), :], buf.at[pl.ds(dst, WINDOW), :],
                      halo_send.at[side], halo_recv.at[side], sp=where)

    def chunk(c, last, between):
        here = rows_of(c, CHUNK)
        with scope("x1"):
            tok.relay(c)
        between()
        with scope("x2"):
            arrived(gath.at[0:n_chips, here, :], tok_settled.at[c])
        ctx = scope("phaseA")
        ctx.__enter__()
        squares = jnp.zeros((CHUNK, 1), F32)
        for s in range(n_tp):
            part = gath[s, here, :].astype(F32)
            squares = squares + jnp.sum(part * part, axis=1, keepdims=True)
            xbuf[:, s * chan:(s + 1) * chan] = (part * gain[0:1, s * chan:(s + 1) * chan]).astype(BF16)
        inv_rms = lax.rsqrt(squares / width + NORM_EPS)
        found = {}

        def product(first):
            for b, off, cols, names in cfg["dots"]:
                if (names[0][0] in ("rq", "rk", "rv")) != first:
                    continue
                block = (mm(xbuf[...], w_bufs[b][:, off:off + cols]) * inv_rms).astype(BF16)
                at = 0
                for name, count in names:
                    found[name] = block[:, at:at + count]
                    at += count

        product(True)
        spot = sp * chunks + c
        oc, os_ = outer_cos[pl.ds(spot, 1), :], outer_sin[pl.ds(spot, 1), :]
        ic, is_ = inner_cos[...], inner_sin[...]
        cosine = oc * ic - os_ * is_
        sine = os_ * ic + oc * is_
        query_rot = found["rq"].astype(F32) * cosine + mm(found["rq"], swap) * sine
        key_rot = (found["rk"].astype(F32) * cosine + mm(found["rk"], swap) * sine) * RK ** -0.5
        kept = []
        for h in range(ret):
            log_row = decay[h:h + 1, here]
            wide = jnp.broadcast_to(log_row, (CHUNK, CHUNK))
            log_col = jnp.sum(jnp.where(row_i == col_i, wide, 0.0), axis=1, keepdims=True)
            cum_col = jnp.sum(jnp.where(col_i <= row_i, wide, 0.0), axis=1, keepdims=True)
            total = jnp.sum(log_row, axis=1, keepdims=True)
            key = key_rot[:, h * RK:(h + 1) * RK]
            value = found["rv"][:, h * RV:(h + 1) * RV]
            up = jnp.exp(cum_col)
            down = jnp.exp(jnp.minimum(total - cum_col, 0.0))
            both = jnp.concatenate([key * down, key * up], axis=1).astype(BF16)
            terms = tm_m(both, value)
            fterm[h, c] = terms[:RK]
            bterm[h, c] = terms[RK:]
            blog[h, c] = jnp.broadcast_to(total, (8, 128))
            kept.append((log_col, cum_col, up, down, key, value))
        ctx.__exit__(None, None, None)
        if last:
            with scope("totals"):
                send_totals()
        ctx = scope("phaseB")
        ctx.__enter__()
        product(False)
        qs[here, :] = found["q"] * jnp.asarray(HD ** -0.5, BF16)
        shifted = pl.ds(pl.multiple_of(c * CHUNK + WINDOW, 128), CHUNK)
        kbuf[shifted, :] = found["k"]
        vbuf[shifted, :] = found["v"]
        gs[here, :] = found["g"]
        for h in range(ret):
            log_col, cum_col, up, down, key, value = kept[h]
            cum_row = jnp.sum(jnp.where(row_i <= col_i, log_col, 0.0), axis=0, keepdims=True)
            query = query_rot[:, h * RK:(h + 1) * RK]
            inner = mm_t(query.astype(BF16), key.astype(BF16)) * jnp.exp(-jnp.abs(cum_col - cum_row))
            rloc[h, here, :] = mm(inner.astype(BF16), value)
            qfb[h, here, :] = jnp.concatenate([query * up, query * down], axis=1).astype(BF16)
        ctx.__exit__(None, None, None)

    def send_totals():
        for h in range(ret):
            state = jnp.zeros((RK, RV), F32)
            back = jnp.zeros((RK, RV), F32)
            for c in range(chunks):
                state = jnp.exp(blog[h, c, 0:1, :]) * state + fterm[h, c]
                back = jnp.exp(blog[h, chunks - 1 - c, 0:1, :]) * back + bterm[h, chunks - 1 - c]
            tot_f[h] = state.astype(BF16)
            tot_b[h] = back.astype(BF16)

        def send_f(d, carry):
            remote(tot_f, tots.at[sp], tot_send, tot_recv, sp=d).start()
            return carry

        def send_b(d, carry):
            remote(tot_b, tots.at[sp], tot_send, tot_recv, sp=d).start()
            return carry

        lax.fori_loop(sp + 1, n_sp, send_f, 0)
        lax.fori_loop(0, sp, send_b, 0)

    early = per * (chunks - 3) + 1

    def block_of(j):
        turn = early - per
        return lax.select(j < turn, j, lax.select(j == turn, mixes - 1, j - 1))

    def halo_wait(side):
        arrived(kbuf.at[0:2 * WINDOW, :], halo_recv.at[side])

    def one(j):
        with scope("attend"):
            attend(j)

    def chunk_body(i, carry):
        c = order(i)

        @pl.when(i > 2)
        def _():
            one(per * (i - 3) + 1)

        def between():
            @pl.when(i == 2)
            def _():
                with scope("aside"):
                    w_aside()

            @pl.when((i == 2) & (sp > 0))
            def _():
                with scope("halo0"):
                    halo_wait(0)

            @pl.when(i == 2)
            def _():
                one(0)

            @pl.when(i > 2)
            def _():
                one(per * (i - 3) + 2)

        chunk(c, False, between)

        @pl.when((i == 0) & (sp < n_sp - 1))
        def _():
            for b in range(2):
                halo(0, b, right).start()

        @pl.when((i == 1) & (sp > 0))
        def _():
            for b in range(2):
                halo(1, b, left).start()

        return carry

    lax.fori_loop(0, chunks - 1, chunk_body, 0)

    @pl.when(sp < n_sp - 1)
    def _():
        with scope("halo1"):
            halo_wait(1)

    one(mixes - 1)
    one(early - per)
    chunk(chunks - 2, True, lambda: one(early - per + 1))

    def late(j, carry):
        with scope("late"):
            attend(j)
        with scope("lrelay"):
            atd.relay(block_of(j - early))
        return carry

    lax.fori_loop(early, mixes - 1, late, 0)

    with scope("states"):
        arrived(logs.at[0:n_sp - 1], log_recv)
        arrived(tots.at[0:n_sp - 1], tot_recv)

        def from_low(e, carry):
            for h in range(ret):
                states[0, h] = jnp.exp(logs[e, h, 0:1, :]) * states[0, h] + tots[e, h].astype(F32)
            return carry

        def from_high(i, carry):
            e = n_sp - 1 - i
            for h in range(ret):
                states[1, h] = jnp.exp(logs[e, h, 0:1, :]) * states[1, h] + tots[e, h].astype(F32)
            return carry

        lax.fori_loop(0, sp, from_low, 0)
        lax.fori_loop(0, n_sp - 1 - sp, from_high, 0)

        for h in range(ret):
            state = states[0, h]
            back = states[1, h]
            for c in range(chunks):
                both_in[h, c, 0:RK] = state.astype(BF16)
                state = jnp.exp(blog[h, c, 0:1, :]) * state + fterm[h, c]
                r = chunks - 1 - c
                both_in[h, r, RK:2 * RK] = back.astype(BF16)
                back = jnp.exp(blog[h, r, 0:1, :]) * back + bterm[h, r]

    def retain(c):
        here = rows_of(c, MIX)
        at = lax.div(c, per)
        pieces = []
        for h in range(ret):
            combined = rloc[h, here, :] + mm(qfb[h, here, :], both_in[h, at])
            centered = combined - jnp.mean(combined, axis=1, keepdims=True)
            normed = centered * lax.rsqrt(jnp.mean(centered * centered, axis=1, keepdims=True) + NORM_EPS)
            gate = gs[here, h * RV:(h + 1) * RV].astype(F32)
            pieces.append((gate / (1.0 + jnp.exp(-gate)) * normed).astype(BF16))
        mx[tp, here, att_w:att_w + ret_w] = jnp.concatenate(pieces, axis=1) if ret > 1 else pieces[0]
        rtd.start(c)

    def ret_body(c, carry):
        with scope("retain"):
            retain(c)
        return carry

    lax.fori_loop(0, mixes, ret_body, 0)

    def att_rest(j, carry):
        atd.relay(block_of(j))
        return carry

    with scope("attrest"):
        lax.fori_loop(mixes - 1 - early, mixes, att_rest, 0)

    with scope("wsettle"):
        arrived(wg.at[0], pw_recv)
        w_done(w_recv.at[2], half_sp)

    def mix(c):
        here = rows_of(c, MIX)
        with scope("msettle"):
            arrived(mx.at[0:n_chips, here, :], mix_settled.at[c])
        with scope("mix"):
            total = mm(mx[0, here, :], wg[0])
            for t in range(1, n_tp):
                total = total + mm(mx[t, here, :], wg[t])
            out[here, :] = total.astype(BF16)

    def mix_body(c, carry):
        @pl.when(c < mixes)
        def _():
            with scope("rrelay"):
                rtd.relay(c)

        @pl.when(c > 0)
        def _():
            mix(c - 1)

        return carry

    lax.fori_loop(0, mixes + 1, mix_body, 0)

    with scope("drain"):
        sent = 2 * n_chips - 1
        arrived(gath.at[0:sent], tok_send)
        arrived(mx.at[0:sent], mix_send)
        arrived(wg.at[0], pw_send)
        w_done(w_send.at[0], 1)
        w_done(w_send.at[1], half_sp - 1)
        w_done(w_send.at[2], half_sp)
        arrived(logs.at[0:n_sp - 1], log_send)
        arrived(tots.at[0:n_sp - 1], tot_send)

        @pl.when(sp < n_sp - 1)
        def _():
            arrived(kbuf.at[0:2 * WINDOW, :], halo_send.at[0])

        @pl.when(sp > 0)
        def _():
            arrived(kbuf.at[0:2 * WINDOW, :], halo_send.at[1])


def body(n_sp, n_tp, tokens, norm_gain, w_q, w_k, w_v, w_rq, w_rk, w_rv, w_rg, att_sink,
         decay_log, init_state, out_att, out_ret):
    rows, chan = tokens.shape
    width = n_tp * chan
    ret = decay_log.shape[0]
    heads = att_sink.shape[0]
    kv_cols = w_k.shape[1]
    kv = kv_cols // HD
    chunks = rows // CHUNK
    n_chips = n_tp // 2
    weights = (w_q, w_k, w_v, w_rq, w_rk, w_rv, w_rg)
    names = ("q", "k", "v", "rq", "rk", "rv", "g")
    cols = [w.shape[1] for w in weights]
    joined = all(count % 128 == 0 for count in cols)
    places, dots = [], []
    if joined:
        buffers = [sum(cols)]
        at = 0
        for count in cols:
            places.append((0, at, count))
            at += count
        for group in ((3, 4), (5,), (1, 2), (0,), (6,)):
            dots.append((0, places[group[0]][1], sum(cols[i] for i in group),
                         tuple((names[i], cols[i]) for i in group)))
    else:
        buffers = cols
        for i, count in enumerate(cols):
            places.append((i, 0, count))
            dots.append((i, 0, count, ((names[i], count),)))
    cfg = dict(n_sp=n_sp, n_tp=n_tp, n_chips=n_chips, chunks=chunks, chan=chan, heads=heads,
               ret=ret, kv=kv, buffers=buffers, places=places, dots=dots, joined=joined)
    tables = rope_tables(n_sp * chunks, CHUNK, ret) + rope_tables(CHUNK, 1, ret)
    small = [norm_gain.reshape(1, width), att_sink.reshape(1, heads), decay_log]
    small += [jnp.asarray(t) for t in tables]
    anyw = pl.BlockSpec(memory_space=pl.ANY)
    dma = pltpu.SemaphoreType.DMA
    att_w, ret_w = heads * HD, ret * RV
    mixes = rows // MIX
    scratch = [pltpu.VMEM((width, count), BF16) for count in buffers] + [
        pltpu.VMEM(a.shape, F32) for a in small] + [
        pltpu.VMEM((n_tp, att_w + ret_w, chan), BF16),
        pltpu.VMEM((n_tp, rows, chan), BF16),
        pltpu.VMEM((CHUNK, width), BF16),
        pltpu.VMEM((rows, att_w), BF16),
        pltpu.VMEM((rows + 2 * WINDOW, kv_cols), BF16),
        pltpu.VMEM((rows + 2 * WINDOW, kv_cols), BF16),
        pltpu.VMEM((n_tp, rows, att_w + ret_w), BF16),
        pltpu.VMEM((ret, rows, 2 * RK), BF16),
        pltpu.VMEM((ret, rows, RV), F32),
        pltpu.VMEM((rows, ret_w), BF16),
        pltpu.VMEM((ret, chunks, RK, RV), F32),
        pltpu.VMEM((ret, chunks, RK, RV), F32),
        pltpu.VMEM((ret, chunks, 8, 128), F32),
        pltpu.VMEM((ret, chunks, 2 * RK, RV), BF16),
        pltpu.VMEM((ret, RK, RV), BF16),
        pltpu.VMEM((ret, RK, RV), BF16),
        pltpu.VMEM((n_sp, ret, RK, RV), BF16),
        pltpu.VMEM((n_sp, ret, 8, 128), F32),
        pltpu.VMEM((2, ret, RK, RV), F32),
        pltpu.SemaphoreType.REGULAR,
        dma((len(buffers),)), dma, dma, dma((len(small) + 1,)),
        dma, dma((n_chips - 1, chunks)), dma((chunks,)),
        dma, dma((n_chips - 1, mixes)), dma((n_chips - 1, mixes)), dma((mixes,)),
        dma, dma, dma((3,)), dma((3,)),
        dma((2,)), dma((2,)),
        dma, dma, dma, dma,
    ]
    return pl.pallas_call(
        functools.partial(kernel, cfg),
        out_shape=pltpu.VMEM((rows, chan), BF16),
        in_specs=[anyw] * (11 + len(small)),
        out_specs=pl.BlockSpec(memory_space=pltpu.VMEM),
        scratch_shapes=scratch,
        compiler_params=pltpu.CompilerParams(
            collective_id=0, has_side_effects=True, vmem_limit_bytes=60 * 1024 * 1024),
    )(tokens, *weights, init_state, out_att, out_ret, *small)


def solution(mesh):
    n_sp, n_tp = mesh.shape["sp"], mesh.shape["tp"]
    in_specs = (
        P("sp", "tp"),
        P(),
        P(None, "tp"),
        P(None, "tp"),
        P(None, "tp"),
        P(None, "tp"),
        P(None, "tp"),
        P(None, "tp"),
        P(None, "tp"),
        P("tp"),
        P("tp", "sp"),
        P(None, "tp", None, None),
        P("tp", None),
        P("tp", None),
    )
    return jax.shard_map(functools.partial(body, n_sp, n_tp), mesh=mesh, in_specs=in_specs,
                         out_specs=P("sp", "tp"), check_vma=False)
```

```python
import contextlib
import functools

import jax
import jax.numpy as jnp
import numpy as np
from jax import lax
from jax.experimental import pallas as pl
from jax.experimental.pallas import tpu as pltpu
from jax.sharding import PartitionSpec as P

HD = 64
RK = 64
RV = 128
WINDOW = 128
CHUNK = 256
MIX = 128
NORM_EPS = 1e-06
ROPE_BASE = 10000.0
F32 = jnp.float32
BF16 = jnp.bfloat16
MESH = pl.DeviceIdType.MESH


def scope(name):
    return contextlib.nullcontext()


def rope_tables(count, step, heads):
    half = RK // 2
    inverse = ROPE_BASE ** (-2.0 * np.arange(half, dtype=np.float64) / RK)
    angles = (np.arange(count, dtype=np.float64) * step)[:, None] * inverse[None, :]
    wide = np.tile(np.concatenate([angles, angles], axis=1), (1, heads))
    return np.cos(wide).astype(np.float32), np.sin(wide).astype(np.float32)


def remote(src, dst, send, recv, **where):
    return pltpu.make_async_remote_copy(
        src_ref=src, dst_ref=dst, send_sem=send, recv_sem=recv,
        device_id=where, device_id_type=MESH,
    )


def rows_of(index, size):
    return pl.ds(pl.multiple_of(index * size, size), size)


def mm(a, b):
    return jnp.dot(a, b, preferred_element_type=F32)


def mm_t(a, b):
    return lax.dot_general(a, b, (((1,), (1,)), ((), ())), preferred_element_type=F32)


def tm_m(a, b):
    return lax.dot_general(a, b, (((0,), (0,)), ((), ())), preferred_element_type=F32)


class Spread:
    def __init__(self, place, buf, columns, size, send, cross, near, settled, src=None):
        self.place, self.buf, self.columns, self.size = place, buf, columns, size
        self.send, self.cross, self.near, self.settled, self.src = send, cross, near, settled, src

    def block(self, slot, c):
        return self.buf.at[slot, rows_of(c, self.size), self.columns]

    def start(self, c):
        tp, partner, across, n_chips = self.place
        src = self.block(tp, c) if self.src is None else self.src.at[rows_of(c, self.size), :]
        for k in range(1, n_chips):
            remote(src, self.block(tp, c), self.send, self.cross.at[n_chips - k - 1, c], tp=across(k)).start()
        remote(src, self.block(tp, c), self.send, self.near.at[c], tp=partner).start()

    def relay(self, c):
        _, partner, across, n_chips = self.place
        for k in range(1, n_chips):
            block = self.block(across(k), c)
            remote(block, block, self.send, self.cross.at[k - 1, c], tp=partner).wait_recv()
            remote(block, block, self.send, self.settled.at[c], tp=partner).start()


def kernel(cfg, *refs):
    n_buf, n_small = len(cfg["buffers"]), 8
    (tokens, w_q, w_k, w_v, w_rq, w_rk, w_rv, w_rg, init, o_att, o_ret) = refs[:11]
    small_hbm = refs[11:11 + n_small - 1]
    out = refs[10 + n_small]
    rest = refs[11 + n_small:]
    w_bufs = rest[:n_buf]
    small = rest[n_buf:n_buf + n_small - 1]
    parts = rest[n_buf + n_small - 1:n_buf + n_small - 1 + len(cfg["dots"])]
    gain, sink, decay, outer_cos, outer_sin, inner_cos, inner_sin = small
    (wg, gath, xbuf, qs, kbuf, vbuf, mx, qfb, rloc, gs, fterm, bterm, blog, both_in,
     sqs, dm, kfac, qfac, bias,
     tot_f, tot_b, tots, logs, states,
     ready, w_sem, wo_sem, tok_sem, small_sem,
     tok_send, tok_cross, tok_near, tok_settled, mix_send, att_cross, ret_cross, mix_settled,
     pw_send, pw_recv, w_send, w_recv,
     halo_send, halo_recv, tot_send, tot_recv, log_send, log_recv) = rest[n_buf + n_small - 1 + len(parts):]
    n_tp, n_sp, n_chips, chunks = cfg["n_tp"], cfg["n_sp"], cfg["n_chips"], cfg["chunks"]
    chan, heads, ret, kv = cfg["chan"], cfg["heads"], cfg["ret"], cfg["kv"]
    rows = chunks * CHUNK
    width = n_tp * chan
    groups = heads // kv
    seq_len = rows * n_sp
    att_w, ret_w = heads * HD, ret * RV
    piece = (att_w + ret_w) // n_sp
    per = CHUNK // MIX
    mixes = rows // MIX
    sp = lax.axis_index("sp")
    tp = lax.axis_index("tp")
    core = lax.rem(tp, 2)
    chip = lax.div(tp, 2)
    partner = chip * 2 + 1 - core

    def across(k):
        return lax.rem(chip + k, n_chips) * 2 + core

    place = (tp, partner, across, n_chips)
    tok = Spread(place, gath, slice(None), CHUNK, tok_send, tok_cross, tok_near, tok_settled, src=tokens)
    atd = Spread(place, mx, pl.ds(0, att_w), MIX, mix_send, att_cross, mix_settled, mix_settled)
    rtd = Spread(place, mx, pl.ds(att_w, ret_w), MIX, mix_send, ret_cross, mix_settled, mix_settled)

    def arrived(ref, sem):
        pltpu.make_async_copy(ref, ref, sem).wait()

    barrier = pltpu.get_barrier_semaphore()
    for k in range(1, n_tp):
        pl.semaphore_signal(barrier, inc=1, device_id={"tp": lax.rem(tp + k, n_tp)}, device_id_type=MESH)

    @pl.when(sp == 0)
    def _():
        for k in range(1, n_sp):
            pl.semaphore_signal(barrier, inc=1, device_id={"sp": k}, device_id_type=MESH)

    token_copy = pltpu.make_async_copy(tokens, gath.at[tp], tok_sem)
    token_copy.start()
    local = [pltpu.make_async_copy(a, b, small_sem.at[i]) for i, (a, b) in enumerate(zip(small_hbm, small))]
    local.append(pltpu.make_async_copy(init, states, small_sem.at[n_small - 1]))
    weights = (w_q, w_k, w_v, w_rq, w_rk, w_rv, w_rg)
    for w_ref, (b, off, cols) in zip(weights, cfg["places"]):
        dst = w_bufs[b].at[:, pl.ds(off, cols)] if cfg["joined"] else w_bufs[b]
        pltpu.make_async_copy(w_ref, dst, w_sem.at[b]).start()
    paired = cfg["paired"]

    def att_row(row):
        if not paired:
            return row
        spot, within = row // HD, row % HD
        return (spot % kv * groups + spot // kv) * HD + within

    runs = [(o_att, att_row(b * HD), b * HD, HD) for b in range(heads)] if paired else [(o_att, 0, 0, att_w)]
    runs.append((o_ret, 0, att_w, ret_w))

    def columns(t):
        return pl.ds(pl.multiple_of(t * chan, chan), chan)

    for src, row, first, count in runs:
        pltpu.make_async_copy(src.at[pl.ds(row, count), columns(tp)], wg.at[tp, pl.ds(first, count), :], wo_sem).start()
    for copy in local:
        copy.start()

    with scope("barrier"):
        @pl.when(sp == 0)
        def _():
            pl.semaphore_wait(barrier, n_tp - 1)

        @pl.when(sp > 0)
        def _():
            pl.semaphore_wait(barrier, n_tp)
            pl.semaphore_signal(ready, inc=1, device_id={"sp": 0}, device_id_type=MESH)

    others = [lax.rem(chip + k, n_chips) * 2 + p for k in range(1, n_chips) for p in range(2)]

    def w_copy(t, e, send, recv, **where):
        block = wg.at[t, rows_of(e, piece), :]
        return remote(block, block, w_send.at[send], w_recv.at[recv], **where)

    def w_done(sem, pieces):
        left, full = pieces * len(others) * piece, att_w + ret_w
        while left > 0:
            arrived(wg.at[0, 0:min(left, full), :], sem)
            left -= full

    def w_first(src, row):
        for t in others:
            remote(src.at[pl.ds(pl.multiple_of(row, piece), piece), columns(t)], wg.at[tp, rows_of(sp, piece), :],
                   w_send.at[0], w_recv.at[0], tp=t).start()

    @pl.when(sp * piece < att_w)
    def _():
        w_first(o_att, att_row(sp * piece))

    @pl.when(sp * piece >= att_w)
    def _():
        w_first(o_ret, sp * piece - att_w)

    def order(i):
        return lax.rem(i + chunks - 1, chunks)

    def first_sends(i, carry):
        tok.start(order(i))
        return carry

    lax.fori_loop(0, chunks, first_sends, 0)

    for src, row, first, count in runs:
        remote(src.at[pl.ds(row, count), columns(partner)], wg.at[tp, pl.ds(first, count), :],
               pw_send, pw_recv, tp=partner).start()

    with scope("lwait"):
        for copy in local:
            copy.wait()
        token_copy.wait()
        for i, buf in enumerate(w_bufs):
            arrived(buf, w_sem.at[i])
        arrived(wg.at[tp], wo_sem)

    for h in range(ret):
        total = jnp.sum(decay[h:h + 1, :], axis=1, keepdims=True)
        logs[sp, h] = jnp.broadcast_to(total, (8, 128))

    @pl.when(sp == 0)
    def _():
        kbuf[0:WINDOW, :] = jnp.zeros((WINDOW, kbuf.shape[1]), BF16)
        vbuf[0:WINDOW, :] = jnp.zeros((WINDOW, vbuf.shape[1]), BF16)

    @pl.when(sp == n_sp - 1)
    def _():
        kbuf[rows + WINDOW:, :] = jnp.zeros((WINDOW, kbuf.shape[1]), BF16)
        vbuf[rows + WINDOW:, :] = jnp.zeros((WINDOW, vbuf.shape[1]), BF16)

    row_i = lax.broadcasted_iota(jnp.int32, (CHUNK, CHUNK), 0)
    col_i = lax.broadcasted_iota(jnp.int32, (CHUNK, CHUNK), 1)
    low = lax.broadcasted_iota(jnp.int32, (CHUNK, 2 * RK), 1) < RK

    def decays(c, carry):
        here = rows_of(c, CHUNK)
        for h in range(ret):
            log_row = decay[h:h + 1, here]
            wide = jnp.broadcast_to(log_row, (CHUNK, CHUNK))
            log_col = jnp.sum(jnp.where(row_i == col_i, wide, 0.0), axis=1, keepdims=True)
            cum_col = jnp.sum(jnp.where(col_i <= row_i, wide, 0.0), axis=1, keepdims=True)
            cum_row = jnp.sum(jnp.where(row_i <= col_i, log_col, 0.0), axis=0, keepdims=True)
            total = jnp.sum(log_row, axis=1, keepdims=True)
            dm[h, c] = jnp.exp(-jnp.abs(cum_col - cum_row))
            up = jnp.exp(cum_col)
            down = jnp.exp(jnp.minimum(total - cum_col, 0.0))
            kfac[h, here, :] = jnp.where(low, down, up)
            qfac[h, here, :] = jnp.where(low, up, down)
            blog[h, c] = jnp.broadcast_to(total, (8, 128))
        return carry

    with scope("decays"):
        lax.fori_loop(0, chunks, decays, 0)

    shape = (MIX, MIX + 2 * WINDOW)
    q_i = lax.broadcasted_iota(jnp.int32, shape, 0)
    k_i = lax.broadcasted_iota(jnp.int32, shape, 1)
    band = (k_i >= q_i) & (k_i <= q_i + 2 * WINDOW)
    bias[0] = jnp.where(band, 0.0, -jnp.inf)
    bias[1] = jnp.where(band & (k_i >= WINDOW), 0.0, -jnp.inf)
    bias[2] = jnp.where(band & (k_i < MIX + WINDOW), 0.0, -jnp.inf)

    def normed(c, which, dst):
        here = rows_of(c, CHUNK)
        squares = jnp.zeros((CHUNK, 1), F32)
        for p in range(2):
            slot = which * 2 + p
            x = gath[slot, here, :].astype(F32)
            squares = squares + jnp.sum(x * x, axis=1, keepdims=True)
            xbuf[dst, :, p * chan:(p + 1) * chan] = (x * gain[0:1, columns(slot)]).astype(BF16)
        return squares

    def product(which, src, b, off, cols):
        span = pl.ds(pl.multiple_of(which * (2 * chan), 2 * chan), 2 * chan)
        return mm(xbuf[src], w_bufs[b][span, off:off + cols])

    def near(i, carry):
        c = order(i)
        here = rows_of(c, CHUNK)
        arrived(gath.at[0, here, :], tok_near.at[c])
        sqs[here, :] = normed(c, chip, 0)
        for part, (b, off, cols, _) in zip(parts, cfg["dots"]):
            part[here, :] = product(chip, 0, b, off, cols)
        return carry

    with scope("near"):
        lax.fori_loop(0, chunks // 2, near, 0)

    with scope("ready"):
        @pl.when(sp == 0)
        def _():
            pl.semaphore_wait(ready, n_sp - 1)
            for k in range(1, n_sp):
                pl.semaphore_signal(ready, inc=1, device_id={"sp": k}, device_id_type=MESH)

        @pl.when(sp > 0)
        def _():
            pl.semaphore_wait(ready, 1)

    for k in range(1, n_sp):
        remote(logs.at[sp], logs.at[sp], log_send, log_recv, sp=lax.rem(sp + k, n_sp)).start()

    beside = sp + 1 - 2 * lax.rem(sp, 2)
    half_sp = n_sp // 2
    with scope("wfwd"):
        w_done(w_recv.at[0], 1)

        def w_pass(k, carry):
            for t in others:
                w_copy(t, sp, 1, 1, sp=lax.rem(sp + 2 * k, n_sp)).start()
            return carry

        lax.fori_loop(1, half_sp, w_pass, 0)
        for t in others:
            w_copy(t, sp, 2, 2, sp=beside).start()

    def w_aside():
        w_done(w_recv.at[1], half_sp - 1)

        def w_over(k, carry):
            for t in others:
                w_copy(t, lax.rem(sp + 2 * k, n_sp), 2, 2, sp=beside).start()
            return carry

        lax.fori_loop(1, half_sp, w_over, 0)

    with scope("near"):
        lax.fori_loop(chunks // 2, chunks, near, 0)

    rw = ret * RK
    p_row = lax.broadcasted_iota(jnp.int32, (rw, rw), 0)
    p_col = lax.broadcasted_iota(jnp.int32, (rw, rw), 1)
    first_half = lax.rem(p_col, RK) < RK // 2
    swap = jnp.where(
        first_half & (p_row == p_col + RK // 2), -1.0,
        jnp.where(jnp.logical_not(first_half) & (p_row == p_col - RK // 2), 1.0, 0.0),
    ).astype(BF16)
    lower = lax.broadcasted_iota(jnp.int32, (MIX, 2 * HD), 1) < HD

    def attend(i):
        here = rows_of(i, MIX)
        span = pl.ds(pl.multiple_of(i * MIX, MIX), MIX + 2 * WINDOW)
        edge = lax.select((sp == 0) & (i == 0), 1, lax.select((sp == n_sp - 1) & (i == mixes - 1), 2, 0))
        block = bias[edge]
        done = {}
        for g in range(kv):
            if paired:
                spots = [(j * kv + g) * 2 * HD for j in range(groups)]
                query = jnp.concatenate([qs[here, at:at + 2 * HD] for at in spots], axis=0)
                key, value = kbuf[span, :], vbuf[span, :]
            else:
                spots = [(g * groups + j) * HD for j in range(groups)]
                query = jnp.concatenate([qs[here, at:at + HD] for at in spots], axis=0)
                key, value = kbuf[span, g * HD:(g + 1) * HD], vbuf[span, g * HD:(g + 1) * HD]
            scores = mm_t(query, key)
            probs, scales = [], []
            for j in range(groups):
                mine = scores[j * MIX:(j + 1) * MIX] + block
                sink_col = jnp.broadcast_to(sink[0:1, g * groups + j:g * groups + j + 1], (MIX, 1))
                top = jnp.maximum(jnp.max(mine, axis=1, keepdims=True), sink_col)
                raised = jnp.exp(mine - top)
                scales.append(1.0 / (jnp.sum(raised, axis=1, keepdims=True) + jnp.exp(sink_col - top)))
                probs.append(raised.astype(BF16))
            result = mm(jnp.concatenate(probs, axis=0), value)
            for j in range(groups):
                done[g, j] = result[j * MIX:(j + 1) * MIX] * scales[j]
        if paired:
            for j in range(groups):
                mx[tp, here, j * 2 * HD:(j + 1) * 2 * HD] = jnp.where(lower, done[0, j], done[1, j]).astype(BF16)
        else:
            mx[tp, here, 0:att_w] = jnp.concatenate(
                [done[g, j] for g in range(kv) for j in range(groups)], axis=1).astype(BF16)
        atd.start(i)

    left, right = sp - 1, sp + 1

    def halo(side, i, where):
        buf = (kbuf, vbuf)[i]
        src, dst = ((rows, 0), (WINDOW, rows + WINDOW))[side]
        return remote(buf.at[pl.ds(src, WINDOW), :], buf.at[pl.ds(dst, WINDOW), :],
                      halo_send.at[side], halo_recv.at[side], sp=where)

    def chunk(c, last, between):
        here = rows_of(c, CHUNK)
        with scope("x1"):
            tok.relay(c)
        between()
        with scope("x2"):
            arrived(gath.at[0:n_chips - 1, here, :], tok_settled.at[c])
        ctx = scope("phaseA")
        ctx.__enter__()
        squares = sqs[here, :]
        far = [(k - 1, lax.rem(chip + k, n_chips)) for k in range(1, n_chips)]
        for at, which in far:
            squares = squares + normed(c, which, at)
        inv_rms = lax.rsqrt(squares / width + NORM_EPS)
        found = {}

        def finish(first):
            for part, (b, off, cols, names) in zip(parts, cfg["dots"]):
                if (names[0][0] in ("rq", "rk", "rv")) != first:
                    continue
                total = part[here, :]
                for at, which in far:
                    total = total + product(which, at, b, off, cols)
                block = (total * inv_rms).astype(BF16)
                at = 0
                for name, count in names:
                    found[name] = block[:, at:at + count]
                    at += count

        finish(True)
        spot = sp * chunks + c
        oc, os_ = outer_cos[pl.ds(spot, 1), :], outer_sin[pl.ds(spot, 1), :]
        ic, is_ = inner_cos[...], inner_sin[...]
        cosine = oc * ic - os_ * is_
        sine = os_ * ic + oc * is_
        query_rot = found["rq"].astype(F32) * cosine + mm(found["rq"], swap) * sine
        key_rot = (found["rk"].astype(F32) * cosine + mm(found["rk"], swap) * sine) * RK ** -0.5

        def doubled(x):
            if ret == 2:
                turned = pltpu.roll(x, RK, 1)
                return jnp.where(low, x, turned), jnp.where(low, turned, x)
            return [jnp.concatenate([x[:, h * RK:(h + 1) * RK]] * 2, axis=1) for h in range(ret)]

        keys = doubled(key_rot)
        for h in range(ret):
            both = (keys[h] * kfac[h, here, :]).astype(BF16)
            terms = tm_m(both, found["rv"][:, h * RV:(h + 1) * RV])
            fterm[h, c] = terms[:RK]
            bterm[h, c] = terms[RK:]
        ctx.__exit__(None, None, None)
        if last:
            with scope("totals"):
                send_totals()
        ctx = scope("phaseB")
        ctx.__enter__()
        finish(False)
        scaled = found["q"] * jnp.asarray(HD ** -0.5, BF16)
        if paired:
            wide = scaled.astype(F32)
            head = [wide[:, at:at + 2 * HD] for at in range(0, att_w, 2 * HD)]
            turned = [pltpu.roll(x, HD, 1) for x in head]
            for j in range(groups):
                for g in range(kv):
                    at = (g * groups + j) * HD
                    x = (head if at % (2 * HD) == g * HD else turned)[at // (2 * HD)]
                    keep = low if g == 0 else jnp.logical_not(low)
                    to = (j * kv + g) * 2 * HD
                    qs[here, to:to + 2 * HD] = jnp.where(keep, x, 0.0).astype(BF16)
        else:
            qs[here, :] = scaled
        shifted = pl.ds(pl.multiple_of(c * CHUNK + WINDOW, 128), CHUNK)
        kbuf[shifted, :] = found["k"]
        vbuf[shifted, :] = found["v"]
        gs[here, :] = found["g"]
        queries = doubled(query_rot)
        key_bf = key_rot.astype(BF16)
        for h in range(ret):
            if ret == 2:
                keep = low if h == 0 else jnp.logical_not(low)
                inner = mm_t(jnp.where(keep, query_rot, 0.0).astype(BF16), key_bf)
            else:
                inner = mm_t(query_rot[:, h * RK:(h + 1) * RK].astype(BF16), key_bf[:, h * RK:(h + 1) * RK])
            rloc[h, here, :] = mm((inner * dm[h, c]).astype(BF16), found["rv"][:, h * RV:(h + 1) * RV])
            qfb[h, here, :] = (queries[h] * qfac[h, here, :]).astype(BF16)
        ctx.__exit__(None, None, None)

    def send_totals():
        for h in range(ret):
            state = jnp.zeros((RK, RV), F32)
            back = jnp.zeros((RK, RV), F32)
            for c in range(chunks):
                state = jnp.exp(blog[h, c, 0:1, :]) * state + fterm[h, c]
                back = jnp.exp(blog[h, chunks - 1 - c, 0:1, :]) * back + bterm[h, chunks - 1 - c]
            tot_f[h] = state.astype(BF16)
            tot_b[h] = back.astype(BF16)

        def send_f(d, carry):
            remote(tot_f, tots.at[sp], tot_send, tot_recv, sp=d).start()
            return carry

        def send_b(d, carry):
            remote(tot_b, tots.at[sp], tot_send, tot_recv, sp=d).start()
            return carry

        lax.fori_loop(sp + 1, n_sp, send_f, 0)
        lax.fori_loop(0, sp, send_b, 0)

    early = per * (chunks - 3) + 1

    def block_of(j):
        turn = early - per
        return lax.select(j < turn, j, lax.select(j == turn, mixes - 1, j - 1))

    def halo_wait(side):
        arrived(kbuf.at[0:2 * WINDOW, :], halo_recv.at[side])

    def one(j):
        with scope("attend"):
            attend(j)

    def chunk_body(i, carry):
        c = order(i)

        if chunks > 4:
            @pl.when(i > 2)
            def _():
                one(per * (i - 3) + 1)

        def between():
            @pl.when(i == 2)
            def _():
                with scope("aside"):
                    w_aside()

            @pl.when((i == 2) & (sp > 0))
            def _():
                with scope("halo0"):
                    halo_wait(0)

            @pl.when(i == 2)
            def _():
                one(0)

            if chunks > 4:
                @pl.when(i > 2)
                def _():
                    one(per * (i - 3) + 2)

        chunk(c, False, between)

        @pl.when((i == 0) & (sp < n_sp - 1))
        def _():
            for b in range(2):
                halo(0, b, right).start()

        @pl.when((i == 1) & (sp > 0))
        def _():
            for b in range(2):
                halo(1, b, left).start()

        return carry

    lax.fori_loop(0, chunks - 1, chunk_body, 0)

    @pl.when(sp < n_sp - 1)
    def _():
        with scope("halo1"):
            halo_wait(1)

    one(mixes - 1)
    one(early - per)
    chunk(chunks - 2, True, lambda: one(early - per + 1))

    def late(j, carry):
        with scope("late"):
            attend(j)
        with scope("lrelay"):
            atd.relay(block_of(j - early))
        return carry

    lax.fori_loop(early, mixes - 1, late, 0)

    with scope("states"):
        arrived(logs.at[0:n_sp - 1], log_recv)
        arrived(tots.at[0:n_sp - 1], tot_recv)

        def from_low(e, carry):
            for h in range(ret):
                states[0, h] = jnp.exp(logs[e, h, 0:1, :]) * states[0, h] + tots[e, h].astype(F32)
            return carry

        def from_high(i, carry):
            e = n_sp - 1 - i
            for h in range(ret):
                states[1, h] = jnp.exp(logs[e, h, 0:1, :]) * states[1, h] + tots[e, h].astype(F32)
            return carry

        lax.fori_loop(0, sp, from_low, 0)
        lax.fori_loop(0, n_sp - 1 - sp, from_high, 0)

        for h in range(ret):
            state = states[0, h]
            back = states[1, h]
            for c in range(chunks):
                both_in[h, c, 0:RK] = state.astype(BF16)
                state = jnp.exp(blog[h, c, 0:1, :]) * state + fterm[h, c]
                r = chunks - 1 - c
                both_in[h, r, RK:2 * RK] = back.astype(BF16)
                back = jnp.exp(blog[h, r, 0:1, :]) * back + bterm[h, r]

    def retain(c):
        here = rows_of(c, MIX)
        at = lax.div(c, per)
        pieces = []
        for h in range(ret):
            combined = rloc[h, here, :] + mm(qfb[h, here, :], both_in[h, at])
            centered = combined - jnp.mean(combined, axis=1, keepdims=True)
            normed = centered * lax.rsqrt(jnp.mean(centered * centered, axis=1, keepdims=True) + NORM_EPS)
            gate = gs[here, h * RV:(h + 1) * RV].astype(F32)
            pieces.append((gate / (1.0 + jnp.exp(-gate)) * normed).astype(BF16))
        mx[tp, here, att_w:att_w + ret_w] = jnp.concatenate(pieces, axis=1) if ret > 1 else pieces[0]
        rtd.start(c)

    def ret_body(c, carry):
        with scope("retain"):
            retain(c)
        return carry

    lax.fori_loop(0, mixes, ret_body, 0)

    def att_rest(j, carry):
        atd.relay(block_of(j))
        return carry

    with scope("attrest"):
        lax.fori_loop(mixes - 1 - early, mixes, att_rest, 0)

    with scope("wsettle"):
        arrived(wg.at[0], pw_recv)
        w_done(w_recv.at[2], half_sp)

    def mix(c):
        here = rows_of(c, MIX)
        with scope("msettle"):
            arrived(mx.at[0:n_chips, here, :], mix_settled.at[c])
        with scope("mix"):
            total = mm(mx[0, here, :], wg[0])
            for t in range(1, n_tp):
                total = total + mm(mx[t, here, :], wg[t])
            out[here, :] = total.astype(BF16)

    def mix_body(c, carry):
        @pl.when(c < mixes)
        def _():
            with scope("rrelay"):
                rtd.relay(c)

        @pl.when(c > 0)
        def _():
            mix(c - 1)

        return carry

    lax.fori_loop(0, mixes + 1, mix_body, 0)

    with scope("drain"):
        sent = 2 * n_chips - 1
        arrived(gath.at[0:sent], tok_send)
        arrived(mx.at[0:sent], mix_send)
        arrived(wg.at[0], pw_send)
        w_done(w_send.at[0], 1)
        w_done(w_send.at[1], half_sp - 1)
        w_done(w_send.at[2], half_sp)
        arrived(logs.at[0:n_sp - 1], log_send)
        arrived(tots.at[0:n_sp - 1], tot_send)

        @pl.when(sp < n_sp - 1)
        def _():
            arrived(kbuf.at[0:2 * WINDOW, :], halo_send.at[0])

        @pl.when(sp > 0)
        def _():
            arrived(kbuf.at[0:2 * WINDOW, :], halo_send.at[1])


def body(n_sp, n_tp, tokens, norm_gain, w_q, w_k, w_v, w_rq, w_rk, w_rv, w_rg, att_sink,
         decay_log, init_state, out_att, out_ret):
    rows, chan = tokens.shape
    width = n_tp * chan
    ret = decay_log.shape[0]
    heads = att_sink.shape[0]
    kv_cols = w_k.shape[1]
    kv = kv_cols // HD
    chunks = rows // CHUNK
    n_chips = n_tp // 2
    weights = (w_q, w_k, w_v, w_rq, w_rk, w_rv, w_rg)
    names = ("q", "k", "v", "rq", "rk", "rv", "g")
    cols = [w.shape[1] for w in weights]
    joined = all(count % 128 == 0 for count in cols)
    places, dots = [], []
    if joined:
        buffers = [sum(cols)]
        at = 0
        for count in cols:
            places.append((0, at, count))
            at += count
        for group in ((3, 4), (5,), (1, 2), (0,), (6,)):
            dots.append((0, places[group[0]][1], sum(cols[i] for i in group),
                         tuple((names[i], cols[i]) for i in group)))
    else:
        buffers = cols
        for i, count in enumerate(cols):
            places.append((i, 0, count))
            dots.append((i, 0, count, ((names[i], count),)))
    att_w, ret_w = heads * HD, ret * RV
    paired = kv == 2 and 2 * HD == 128 and HD % ((att_w + ret_w) // n_sp) == 0
    cfg = dict(paired=paired, n_sp=n_sp, n_tp=n_tp, n_chips=n_chips, chunks=chunks, chan=chan, heads=heads,
               ret=ret, kv=kv, buffers=buffers, places=places, dots=dots, joined=joined)
    tables = rope_tables(n_sp * chunks, CHUNK, ret) + rope_tables(CHUNK, 1, ret)
    small = [norm_gain.reshape(1, width), att_sink.reshape(1, heads), decay_log]
    small += [jnp.asarray(t) for t in tables]
    anyw = pl.BlockSpec(memory_space=pl.ANY)
    dma = pltpu.SemaphoreType.DMA
    mixes = rows // MIX
    scratch = [pltpu.VMEM((width, count), BF16) for count in buffers] + [
        pltpu.VMEM(a.shape, F32) for a in small] + [
        pltpu.VMEM((rows, group[2]), F32) for group in dots] + [
        pltpu.VMEM((n_tp, att_w + ret_w, chan), BF16),
        pltpu.VMEM((n_tp, rows, chan), BF16),
        pltpu.VMEM((max(n_chips - 1, 1), CHUNK, 2 * chan), BF16),
        pltpu.VMEM((rows, att_w * (2 if paired else 1)), BF16),
        pltpu.VMEM((rows + 2 * WINDOW, kv_cols), BF16),
        pltpu.VMEM((rows + 2 * WINDOW, kv_cols), BF16),
        pltpu.VMEM((n_tp, rows, att_w + ret_w), BF16),
        pltpu.VMEM((ret, rows, 2 * RK), BF16),
        pltpu.VMEM((ret, rows, RV), F32),
        pltpu.VMEM((rows, ret_w), BF16),
        pltpu.VMEM((ret, chunks, RK, RV), F32),
        pltpu.VMEM((ret, chunks, RK, RV), F32),
        pltpu.VMEM((ret, chunks, 8, 128), F32),
        pltpu.VMEM((ret, chunks, 2 * RK, RV), BF16),
        pltpu.VMEM((rows, 1), F32),
        pltpu.VMEM((ret, chunks, CHUNK, CHUNK), F32),
        pltpu.VMEM((ret, rows, 2 * RK), F32),
        pltpu.VMEM((ret, rows, 2 * RK), F32),
        pltpu.VMEM((3, MIX, MIX + 2 * WINDOW), F32),
        pltpu.VMEM((ret, RK, RV), BF16),
        pltpu.VMEM((ret, RK, RV), BF16),
        pltpu.VMEM((n_sp, ret, RK, RV), BF16),
        pltpu.VMEM((n_sp, ret, 8, 128), F32),
        pltpu.VMEM((2, ret, RK, RV), F32),
        pltpu.SemaphoreType.REGULAR,
        dma((len(buffers),)), dma, dma, dma((len(small) + 1,)),
        dma, dma((n_chips - 1, chunks)), dma((chunks,)), dma((chunks,)),
        dma, dma((n_chips - 1, mixes)), dma((n_chips - 1, mixes)), dma((mixes,)),
        dma, dma, dma((3,)), dma((3,)),
        dma((2,)), dma((2,)),
        dma, dma, dma, dma,
    ]
    return pl.pallas_call(
        functools.partial(kernel, cfg),
        out_shape=pltpu.VMEM((rows, chan), BF16),
        in_specs=[anyw] * (11 + len(small)),
        out_specs=pl.BlockSpec(memory_space=pltpu.VMEM),
        scratch_shapes=scratch,
        compiler_params=pltpu.CompilerParams(
            collective_id=0, has_side_effects=True, vmem_limit_bytes=60 * 1024 * 1024),
    )(tokens, *weights, init_state, out_att, out_ret, *small)


def solution(mesh):
    n_sp, n_tp = mesh.shape["sp"], mesh.shape["tp"]
    in_specs = (
        P("sp", "tp"),
        P(),
        P(None, "tp"),
        P(None, "tp"),
        P(None, "tp"),
        P(None, "tp"),
        P(None, "tp"),
        P(None, "tp"),
        P(None, "tp"),
        P("tp"),
        P("tp", "sp"),
        P(None, "tp", None, None),
        P("tp", None),
        P("tp", None),
    )
    return jax.shard_map(functools.partial(body, n_sp, n_tp), mesh=mesh, in_specs=in_specs,
                         out_specs=P("sp", "tp"), check_vma=False)
```

```python
import contextlib
import functools

import jax
import jax.numpy as jnp
import numpy as np
from jax import lax
from jax.experimental import pallas as pl
from jax.experimental.pallas import tpu as pltpu
from jax.sharding import PartitionSpec as P

HD = 64
RK = 64
RV = 128
WINDOW = 128
CHUNK = 256
MIX = 128
NORM_EPS = 1e-06
ROPE_BASE = 10000.0
F32 = jnp.float32
BF16 = jnp.bfloat16
MESH = pl.DeviceIdType.MESH


def scope(name):
    return contextlib.nullcontext()


def rope_tables(count, step, heads):
    half = RK // 2
    inverse = ROPE_BASE ** (-2.0 * np.arange(half, dtype=np.float64) / RK)
    angles = (np.arange(count, dtype=np.float64) * step)[:, None] * inverse[None, :]
    wide = np.tile(np.concatenate([angles, angles], axis=1), (1, heads))
    return np.cos(wide).astype(np.float32), np.sin(wide).astype(np.float32)


def remote(src, dst, send, recv, **where):
    return pltpu.make_async_remote_copy(
        src_ref=src, dst_ref=dst, send_sem=send, recv_sem=recv,
        device_id=where, device_id_type=MESH,
    )


def rows_of(index, size):
    return pl.ds(pl.multiple_of(index * size, size), size)


def mm(a, b):
    return jnp.dot(a, b, preferred_element_type=F32)


def mm_t(a, b):
    return lax.dot_general(a, b, (((1,), (1,)), ((), ())), preferred_element_type=F32)


def tm_m(a, b):
    return lax.dot_general(a, b, (((0,), (0,)), ((), ())), preferred_element_type=F32)


class Spread:
    def __init__(self, place, buf, columns, size, send, cross, near, settled, src=None):
        self.place, self.buf, self.columns, self.size = place, buf, columns, size
        self.send, self.cross, self.near, self.settled, self.src = send, cross, near, settled, src

    def block(self, slot, c):
        return self.buf.at[slot, rows_of(c, self.size), self.columns]

    def start(self, c):
        tp, partner, across, n_chips = self.place
        src = self.block(tp, c) if self.src is None else self.src.at[rows_of(c, self.size), :]
        for k in range(1, n_chips):
            remote(src, self.block(tp, c), self.send, self.cross.at[n_chips - k - 1, c], tp=across(k)).start()
        remote(src, self.block(tp, c), self.send, self.near.at[c], tp=partner).start()

    def relay(self, c):
        _, partner, across, n_chips = self.place
        for k in range(1, n_chips):
            block = self.block(across(k), c)
            remote(block, block, self.send, self.cross.at[k - 1, c], tp=partner).wait_recv()
            remote(block, block, self.send, self.settled.at[c], tp=partner).start()


def kernel(cfg, *refs):
    n_buf, n_small = len(cfg["buffers"]), 8
    (tokens, w_q, w_k, w_v, w_rq, w_rk, w_rv, w_rg, init, o_att, o_ret) = refs[:11]
    small_hbm = refs[11:11 + n_small - 1]
    out = refs[10 + n_small]
    rest = refs[11 + n_small:]
    w_bufs = rest[:n_buf]
    small = rest[n_buf:n_buf + n_small - 1]
    parts = rest[n_buf + n_small - 1:n_buf + n_small - 1 + len(cfg["dots"])]
    gain, sink, decay, outer_cos, outer_sin, inner_cos, inner_sin = small
    (wg, gath, xbuf, qs, kbuf, vt, mx, qfb, rloc, gs, fterm, bterm, blog, both_in,
     sqs, dm, kfac, qfac, bias,
     tot_f, tot_b, tots, logs, states,
     ready, w_sem, wo_sem, tok_sem, small_sem,
     tok_send, tok_cross, tok_near, tok_settled, mix_send, att_cross, ret_cross, mix_settled,
     pw_send, pw_recv, w_send, w_recv,
     halo_send, halo_recv, tot_send, tot_recv, log_send, log_recv) = rest[n_buf + n_small - 1 + len(parts):]
    n_tp, n_sp, n_chips, chunks = cfg["n_tp"], cfg["n_sp"], cfg["n_chips"], cfg["chunks"]
    chan, heads, ret, kv = cfg["chan"], cfg["heads"], cfg["ret"], cfg["kv"]
    rows = chunks * CHUNK
    width = n_tp * chan
    groups = heads // kv
    seq_len = rows * n_sp
    att_w, ret_w = heads * HD, ret * RV
    piece = (att_w + ret_w) // n_sp
    per = CHUNK // MIX
    mixes = rows // MIX
    sp = lax.axis_index("sp")
    tp = lax.axis_index("tp")
    core = lax.rem(tp, 2)
    chip = lax.div(tp, 2)
    partner = chip * 2 + 1 - core

    def across(k):
        return lax.rem(chip + k, n_chips) * 2 + core

    place = (tp, partner, across, n_chips)
    tok = Spread(place, gath, slice(None), CHUNK, tok_send, tok_cross, tok_near, tok_settled, src=tokens)
    atd = Spread(place, mx, pl.ds(0, att_w), MIX, mix_send, att_cross, mix_settled, mix_settled)
    rtd = Spread(place, mx, pl.ds(att_w, ret_w), MIX, mix_send, ret_cross, mix_settled, mix_settled)

    def arrived(ref, sem):
        pltpu.make_async_copy(ref, ref, sem).wait()

    barrier = pltpu.get_barrier_semaphore()
    for k in range(1, n_tp):
        pl.semaphore_signal(barrier, inc=1, device_id={"tp": lax.rem(tp + k, n_tp)}, device_id_type=MESH)

    @pl.when(sp == 0)
    def _():
        for k in range(1, n_sp):
            pl.semaphore_signal(barrier, inc=1, device_id={"sp": k}, device_id_type=MESH)

    token_copy = pltpu.make_async_copy(tokens, gath.at[tp], tok_sem)
    token_copy.start()
    local = [pltpu.make_async_copy(a, b, small_sem.at[i]) for i, (a, b) in enumerate(zip(small_hbm, small))]
    local.append(pltpu.make_async_copy(init, states, small_sem.at[n_small - 1]))
    weights = (w_q, w_k, w_v, w_rq, w_rk, w_rv, w_rg)
    for w_ref, (b, off, cols) in zip(weights, cfg["places"]):
        dst = w_bufs[b].at[:, pl.ds(off, cols)] if cfg["joined"] else w_bufs[b]
        pltpu.make_async_copy(w_ref, dst, w_sem.at[b]).start()
    paired = cfg["paired"]

    def att_row(row):
        if kv == 1:
            return row
        spot, within = row // HD, row % HD
        return (spot % kv * groups + spot // kv) * HD + within

    runs = [(o_att, att_row(b * HD), b * HD, HD) for b in range(heads)]
    runs.append((o_ret, 0, att_w, ret_w))

    def columns(t):
        return pl.ds(pl.multiple_of(t * chan, chan), chan)

    for src, row, first, count in runs:
        pltpu.make_async_copy(src.at[pl.ds(row, count), columns(tp)], wg.at[tp, pl.ds(first, count), :], wo_sem).start()
    for copy in local:
        copy.start()

    with scope("barrier"):
        @pl.when(sp == 0)
        def _():
            pl.semaphore_wait(barrier, n_tp - 1)

        @pl.when(sp > 0)
        def _():
            pl.semaphore_wait(barrier, n_tp)
            pl.semaphore_signal(ready, inc=1, device_id={"sp": 0}, device_id_type=MESH)

    others = [lax.rem(chip + k, n_chips) * 2 + p for k in range(1, n_chips) for p in range(2)]

    def w_copy(t, e, send, recv, **where):
        block = wg.at[t, rows_of(e, piece), :]
        return remote(block, block, w_send.at[send], w_recv.at[recv], **where)

    def w_done(sem, pieces):
        left, full = pieces * len(others) * piece, att_w + ret_w
        while left > 0:
            arrived(wg.at[0, 0:min(left, full), :], sem)
            left -= full

    def w_first(src, row):
        for t in others:
            remote(src.at[pl.ds(pl.multiple_of(row, piece), piece), columns(t)], wg.at[tp, rows_of(sp, piece), :],
                   w_send.at[0], w_recv.at[0], tp=t).start()

    @pl.when(sp * piece < att_w)
    def _():
        w_first(o_att, att_row(sp * piece))

    @pl.when(sp * piece >= att_w)
    def _():
        w_first(o_ret, sp * piece - att_w)

    def order(i):
        return lax.rem(i + chunks - 1, chunks)

    def first_sends(i, carry):
        tok.start(order(i))
        return carry

    lax.fori_loop(0, chunks, first_sends, 0)

    for src, row, first, count in runs:
        remote(src.at[pl.ds(row, count), columns(partner)], wg.at[tp, pl.ds(first, count), :],
               pw_send, pw_recv, tp=partner).start()

    with scope("lwait"):
        for copy in local:
            copy.wait()
        token_copy.wait()
        for i, buf in enumerate(w_bufs):
            arrived(buf, w_sem.at[i])
        arrived(wg.at[tp], wo_sem)

    for h in range(ret):
        total = jnp.sum(decay[h:h + 1, :], axis=1, keepdims=True)
        logs[sp, h] = jnp.broadcast_to(total, (8, 128))

    @pl.when(sp == 0)
    def _():
        kbuf[0:WINDOW, :] = jnp.zeros((WINDOW, kbuf.shape[1]), BF16)
        vt[:, 0:WINDOW] = jnp.zeros((vt.shape[0], WINDOW), BF16)

    @pl.when(sp == n_sp - 1)
    def _():
        kbuf[rows + WINDOW:, :] = jnp.zeros((WINDOW, kbuf.shape[1]), BF16)
        vt[:, rows + WINDOW:] = jnp.zeros((vt.shape[0], WINDOW), BF16)

    row_i = lax.broadcasted_iota(jnp.int32, (CHUNK, CHUNK), 0)
    col_i = lax.broadcasted_iota(jnp.int32, (CHUNK, CHUNK), 1)
    low = lax.broadcasted_iota(jnp.int32, (CHUNK, 2 * RK), 1) < RK

    def decays(c, carry):
        here = rows_of(c, CHUNK)
        for h in range(ret):
            log_row = decay[h:h + 1, here]
            wide = jnp.broadcast_to(log_row, (CHUNK, CHUNK))
            log_col = jnp.sum(jnp.where(row_i == col_i, wide, 0.0), axis=1, keepdims=True)
            cum_col = jnp.sum(jnp.where(col_i <= row_i, wide, 0.0), axis=1, keepdims=True)
            cum_row = jnp.sum(jnp.where(row_i <= col_i, log_col, 0.0), axis=0, keepdims=True)
            total = jnp.sum(log_row, axis=1, keepdims=True)
            dm[h, c] = jnp.exp(-jnp.abs(cum_col - cum_row))
            up = jnp.exp(cum_col)
            down = jnp.exp(jnp.minimum(total - cum_col, 0.0))
            kfac[h, here, :] = jnp.where(low, down, up)
            qfac[h, here, :] = jnp.where(low, up, down)
            blog[h, c] = jnp.broadcast_to(total, (8, 128))
        return carry

    with scope("decays"):
        lax.fori_loop(0, chunks, decays, 0)

    shape = (MIX + 2 * WINDOW, MIX)
    q_i = lax.broadcasted_iota(jnp.int32, shape, 1)
    k_i = lax.broadcasted_iota(jnp.int32, shape, 0)
    band = (k_i >= q_i) & (k_i <= q_i + 2 * WINDOW)
    bias[0] = jnp.where(band, 0.0, -jnp.inf)
    bias[1] = jnp.where(band & (k_i >= WINDOW), 0.0, -jnp.inf)
    bias[2] = jnp.where(band & (k_i < MIX + WINDOW), 0.0, -jnp.inf)

    def normed(c, which, dst):
        here = rows_of(c, CHUNK)
        squares = jnp.zeros((CHUNK, 1), F32)
        for p in range(2):
            slot = which * 2 + p
            x = gath[slot, here, :].astype(F32)
            squares = squares + jnp.sum(x * x, axis=1, keepdims=True)
            xbuf[dst, :, p * chan:(p + 1) * chan] = (x * gain[0:1, columns(slot)]).astype(BF16)
        return squares

    def product(which, src, b, off, cols):
        span = pl.ds(pl.multiple_of(which * (2 * chan), 2 * chan), 2 * chan)
        return mm(xbuf[src], w_bufs[b][span, off:off + cols])

    def near(i, carry):
        c = order(i)
        here = rows_of(c, CHUNK)
        arrived(gath.at[0, here, :], tok_near.at[c])
        sqs[here, :] = normed(c, chip, 0)
        for part, (b, off, cols, _) in zip(parts, cfg["dots"]):
            part[here, :] = product(chip, 0, b, off, cols)
        return carry

    with scope("near"):
        lax.fori_loop(0, chunks // 2, near, 0)

    with scope("ready"):
        @pl.when(sp == 0)
        def _():
            pl.semaphore_wait(ready, n_sp - 1)
            for k in range(1, n_sp):
                pl.semaphore_signal(ready, inc=1, device_id={"sp": k}, device_id_type=MESH)

        @pl.when(sp > 0)
        def _():
            pl.semaphore_wait(ready, 1)

    for k in range(1, n_sp):
        remote(logs.at[sp], logs.at[sp], log_send, log_recv, sp=lax.rem(sp + k, n_sp)).start()

    beside = sp + 1 - 2 * lax.rem(sp, 2)
    half_sp = n_sp // 2
    with scope("wfwd"):
        w_done(w_recv.at[0], 1)

        def w_pass(k, carry):
            for t in others:
                w_copy(t, sp, 1, k + 1, sp=lax.rem(sp + 2 * k, n_sp)).start()
            return carry

        lax.fori_loop(1, half_sp, w_pass, 0)
        for t in others:
            w_copy(t, sp, 2, 1, sp=beside).start()

    def w_aside(first, end):
        def w_over(k, carry):
            w_done(w_recv.at[k + 1], 1)
            for t in others:
                w_copy(t, lax.rem(sp + n_sp - 2 * k, n_sp), 2, 1, sp=beside).start()
            return carry

        lax.fori_loop(first, end, w_over, 0)

    with scope("near"):
        lax.fori_loop(chunks // 2, chunks, near, 0)

    rw = ret * RK
    p_row = lax.broadcasted_iota(jnp.int32, (rw, rw), 0)
    p_col = lax.broadcasted_iota(jnp.int32, (rw, rw), 1)
    first_half = lax.rem(p_col, RK) < RK // 2
    swap = jnp.where(
        first_half & (p_row == p_col + RK // 2), -1.0,
        jnp.where(jnp.logical_not(first_half) & (p_row == p_col - RK // 2), 1.0, 0.0),
    ).astype(BF16)
    ones = jnp.ones((HD, MIX + 2 * WINDOW), BF16)

    def attend(i):
        here = rows_of(i, MIX)
        span = pl.ds(pl.multiple_of(i * MIX, MIX), MIX + 2 * WINDOW)
        edge = lax.select((sp == 0) & (i == 0), 1, lax.select((sp == n_sp - 1) & (i == mixes - 1), 2, 0))
        block = bias[edge]
        block = jnp.concatenate([block] * groups, axis=1)
        done = []
        for g in range(kv):
            if paired:
                spots = [(j * kv + g) * 2 * HD for j in range(groups)]
                query = jnp.concatenate([qs[here, at:at + 2 * HD] for at in spots], axis=0)
                key = kbuf[span, :]
            else:
                spots = [(g * groups + j) * HD for j in range(groups)]
                query = jnp.concatenate([qs[here, at:at + HD] for at in spots], axis=0)
                key = kbuf[span, g * HD:(g + 1) * HD]
            value = jnp.concatenate([vt[g * HD:(g + 1) * HD, span], ones], axis=0)
            scores = mm_t(key, query) + block
            sink_row = jnp.concatenate(
                [jnp.broadcast_to(sink[0:1, g * groups + j:g * groups + j + 1], (1, MIX)) for j in range(groups)],
                axis=1)
            top = jnp.maximum(jnp.max(scores, axis=0, keepdims=True), sink_row)
            result = mm(value, jnp.exp(scores - top).astype(BF16))
            scale = 1.0 / (result[HD:HD + 1, :] + jnp.exp(sink_row - top))
            done.append(result[0:HD, :] * scale)
        both = jnp.concatenate(done, axis=0) if kv > 1 else done[0]
        turned = [jnp.transpose(both[:, j * MIX:(j + 1) * MIX]).astype(BF16) for j in range(groups)]
        if kv * HD % 128 == 0:
            for j in range(groups):
                mx[tp, here, j * kv * HD:(j + 1) * kv * HD] = turned[j]
        else:
            mx[tp, here, 0:att_w] = jnp.concatenate(turned, axis=1)
        atd.start(i)

    left, right = sp - 1, sp + 1

    def halo(side, i, where):
        def part(at):
            return kbuf.at[pl.ds(at, WINDOW), :] if i == 0 else vt.at[:, pl.ds(at, WINDOW)]

        src, dst = ((rows, 0), (WINDOW, rows + WINDOW))[side]
        return remote(part(src), part(dst), halo_send.at[side], halo_recv.at[side], sp=where)

    def chunk(c, last, between):
        here = rows_of(c, CHUNK)
        with scope("x1"):
            tok.relay(c)
        between()
        with scope("x2"):
            arrived(gath.at[0:n_chips - 1, here, :], tok_settled.at[c])
        ctx = scope("phaseA")
        ctx.__enter__()
        squares = sqs[here, :]
        far = [(k - 1, lax.rem(chip + k, n_chips)) for k in range(1, n_chips)]
        for at, which in far:
            squares = squares + normed(c, which, at)
        inv_rms = lax.rsqrt(squares / width + NORM_EPS)
        found = {}

        def finish(first):
            for part, (b, off, cols, names) in zip(parts, cfg["dots"]):
                if (names[0][0] in ("rq", "rk", "rv")) != first:
                    continue
                total = part[here, :]
                for at, which in far:
                    total = total + product(which, at, b, off, cols)
                block = (total * inv_rms).astype(BF16)
                at = 0
                for name, count in names:
                    found[name] = block[:, at:at + count]
                    at += count

        finish(True)
        spot = sp * chunks + c
        oc, os_ = outer_cos[pl.ds(spot, 1), :], outer_sin[pl.ds(spot, 1), :]
        ic, is_ = inner_cos[...], inner_sin[...]
        cosine = oc * ic - os_ * is_
        sine = os_ * ic + oc * is_
        query_rot = found["rq"].astype(F32) * cosine + mm(found["rq"], swap) * sine
        key_rot = (found["rk"].astype(F32) * cosine + mm(found["rk"], swap) * sine) * RK ** -0.5

        def doubled(x):
            if ret == 2:
                turned = pltpu.roll(x, RK, 1)
                return jnp.where(low, x, turned), jnp.where(low, turned, x)
            return [jnp.concatenate([x[:, h * RK:(h + 1) * RK]] * 2, axis=1) for h in range(ret)]

        keys = doubled(key_rot)
        for h in range(ret):
            both = (keys[h] * kfac[h, here, :]).astype(BF16)
            terms = tm_m(both, found["rv"][:, h * RV:(h + 1) * RV])
            fterm[h, c] = terms[:RK]
            bterm[h, c] = terms[RK:]
        ctx.__exit__(None, None, None)
        if last:
            with scope("totals"):
                send_totals()
        ctx = scope("phaseB")
        ctx.__enter__()
        finish(False)
        scaled = found["q"] * jnp.asarray(HD ** -0.5, BF16)
        if paired:
            wide = scaled.astype(F32)
            head = [wide[:, at:at + 2 * HD] for at in range(0, att_w, 2 * HD)]
            turned = [pltpu.roll(x, HD, 1) for x in head]
            for j in range(groups):
                for g in range(kv):
                    at = (g * groups + j) * HD
                    x = (head if at % (2 * HD) == g * HD else turned)[at // (2 * HD)]
                    keep = low if g == 0 else jnp.logical_not(low)
                    to = (j * kv + g) * 2 * HD
                    qs[here, to:to + 2 * HD] = jnp.where(keep, x, 0.0).astype(BF16)
        else:
            qs[here, :] = scaled
        shifted = pl.ds(pl.multiple_of(c * CHUNK + WINDOW, 128), CHUNK)
        kbuf[shifted, :] = found["k"]
        vt[:, shifted] = jnp.transpose(found["v"].astype(F32)).astype(BF16)
        gs[here, :] = found["g"]
        queries = doubled(query_rot)
        key_bf = key_rot.astype(BF16)
        for h in range(ret):
            if ret == 2:
                keep = low if h == 0 else jnp.logical_not(low)
                inner = mm_t(jnp.where(keep, query_rot, 0.0).astype(BF16), key_bf)
            else:
                inner = mm_t(query_rot[:, h * RK:(h + 1) * RK].astype(BF16), key_bf[:, h * RK:(h + 1) * RK])
            rloc[h, here, :] = mm((inner * dm[h, c]).astype(BF16), found["rv"][:, h * RV:(h + 1) * RV])
            qfb[h, here, :] = (queries[h] * qfac[h, here, :]).astype(BF16)
        ctx.__exit__(None, None, None)

    def send_totals():
        for h in range(ret):
            state = jnp.zeros((RK, RV), F32)
            back = jnp.zeros((RK, RV), F32)
            for c in range(chunks):
                state = jnp.exp(blog[h, c, 0:1, :]) * state + fterm[h, c]
                back = jnp.exp(blog[h, chunks - 1 - c, 0:1, :]) * back + bterm[h, chunks - 1 - c]
            tot_f[h] = state.astype(BF16)
            tot_b[h] = back.astype(BF16)

        def send_f(d, carry):
            remote(tot_f, tots.at[sp], tot_send, tot_recv, sp=d).start()
            return carry

        def send_b(d, carry):
            remote(tot_b, tots.at[sp], tot_send, tot_recv, sp=d).start()
            return carry

        lax.fori_loop(sp + 1, n_sp, send_f, 0)
        lax.fori_loop(0, sp, send_b, 0)

    early = per * (chunks - 3) + 1

    def block_of(j):
        turn = early - per
        return lax.select(j < turn, j, lax.select(j == turn, mixes - 1, j - 1))

    def halo_wait(side):
        arrived(kbuf.at[0:2 * WINDOW, :], halo_recv.at[side])

    def one(j):
        with scope("attend"):
            attend(j)

    def chunk_body(i, carry):
        c = order(i)

        if chunks > 4:
            @pl.when(i > 2)
            def _():
                one(per * (i - 3) + 1)

        def between():
            @pl.when(i == chunks - 2)
            def _():
                with scope("aside"):
                    w_aside(chunks - 1, half_sp)

            @pl.when((i == 2) & (sp > 0))
            def _():
                with scope("halo0"):
                    halo_wait(0)

            @pl.when(i == 2)
            def _():
                one(0)

            if chunks > 4:
                @pl.when(i > 2)
                def _():
                    one(per * (i - 3) + 2)

        chunk(c, False, between)

        @pl.when((i == 0) & (sp < n_sp - 1))
        def _():
            for b in range(2):
                halo(0, b, right).start()

        @pl.when(i < min(chunks - 2, half_sp - 1))
        def _():
            with scope("aside"):
                w_aside(i + 1, i + 2)

        @pl.when((i == 1) & (sp > 0))
        def _():
            for b in range(2):
                halo(1, b, left).start()

        return carry

    lax.fori_loop(0, chunks - 1, chunk_body, 0)

    @pl.when(sp < n_sp - 1)
    def _():
        with scope("halo1"):
            halo_wait(1)

    one(mixes - 1)
    one(early - per)
    chunk(chunks - 2, True, lambda: one(early - per + 1))

    def late(j, carry):
        with scope("late"):
            attend(j)
        with scope("lrelay"):
            atd.relay(block_of(j - early))
        return carry

    lax.fori_loop(early, mixes - 1, late, 0)

    with scope("states"):
        arrived(logs.at[0:n_sp - 1], log_recv)
        arrived(tots.at[0:n_sp - 1], tot_recv)

        def from_low(e, carry):
            for h in range(ret):
                states[0, h] = jnp.exp(logs[e, h, 0:1, :]) * states[0, h] + tots[e, h].astype(F32)
            return carry

        def from_high(i, carry):
            e = n_sp - 1 - i
            for h in range(ret):
                states[1, h] = jnp.exp(logs[e, h, 0:1, :]) * states[1, h] + tots[e, h].astype(F32)
            return carry

        lax.fori_loop(0, sp, from_low, 0)
        lax.fori_loop(0, n_sp - 1 - sp, from_high, 0)

        for h in range(ret):
            state = states[0, h]
            back = states[1, h]
            for c in range(chunks):
                both_in[h, c, 0:RK] = state.astype(BF16)
                state = jnp.exp(blog[h, c, 0:1, :]) * state + fterm[h, c]
                r = chunks - 1 - c
                both_in[h, r, RK:2 * RK] = back.astype(BF16)
                back = jnp.exp(blog[h, r, 0:1, :]) * back + bterm[h, r]

    def retain(c):
        here = rows_of(c, MIX)
        at = lax.div(c, per)
        pieces = []
        for h in range(ret):
            combined = rloc[h, here, :] + mm(qfb[h, here, :], both_in[h, at])
            centered = combined - jnp.mean(combined, axis=1, keepdims=True)
            normed = centered * lax.rsqrt(jnp.mean(centered * centered, axis=1, keepdims=True) + NORM_EPS)
            gate = gs[here, h * RV:(h + 1) * RV].astype(F32)
            pieces.append((gate / (1.0 + jnp.exp(-gate)) * normed).astype(BF16))
        mx[tp, here, att_w:att_w + ret_w] = jnp.concatenate(pieces, axis=1) if ret > 1 else pieces[0]
        rtd.start(c)

    def ret_body(c, carry):
        with scope("retain"):
            retain(c)
        return carry

    lax.fori_loop(0, mixes, ret_body, 0)

    def att_rest(j, carry):
        atd.relay(block_of(j))
        return carry

    with scope("attrest"):
        lax.fori_loop(mixes - 1 - early, mixes, att_rest, 0)

    with scope("wsettle"):
        arrived(wg.at[0], pw_recv)
        w_done(w_recv.at[1], half_sp)

    def mix(c):
        here = rows_of(c, MIX)
        with scope("msettle"):
            arrived(mx.at[0:n_chips, here, :], mix_settled.at[c])
        with scope("mix"):
            total = mm(mx[0, here, :], wg[0])
            for t in range(1, n_tp):
                total = total + mm(mx[t, here, :], wg[t])
            out[here, :] = total.astype(BF16)

    def mix_body(c, carry):
        @pl.when(c < mixes)
        def _():
            with scope("rrelay"):
                rtd.relay(c)

        @pl.when(c > 0)
        def _():
            mix(c - 1)

        return carry

    lax.fori_loop(0, mixes + 1, mix_body, 0)

    with scope("drain"):
        sent = 2 * n_chips - 1
        arrived(gath.at[0:sent], tok_send)
        arrived(mx.at[0:sent], mix_send)
        arrived(wg.at[0], pw_send)
        w_done(w_send.at[0], 1)
        w_done(w_send.at[1], half_sp - 1)
        w_done(w_send.at[2], half_sp)
        arrived(logs.at[0:n_sp - 1], log_send)
        arrived(tots.at[0:n_sp - 1], tot_send)

        @pl.when(sp < n_sp - 1)
        def _():
            arrived(kbuf.at[0:2 * WINDOW, :], halo_send.at[0])

        @pl.when(sp > 0)
        def _():
            arrived(kbuf.at[0:2 * WINDOW, :], halo_send.at[1])


def body(n_sp, n_tp, tokens, norm_gain, w_q, w_k, w_v, w_rq, w_rk, w_rv, w_rg, att_sink,
         decay_log, init_state, out_att, out_ret):
    rows, chan = tokens.shape
    width = n_tp * chan
    ret = decay_log.shape[0]
    heads = att_sink.shape[0]
    kv_cols = w_k.shape[1]
    kv = kv_cols // HD
    chunks = rows // CHUNK
    n_chips = n_tp // 2
    weights = (w_q, w_k, w_v, w_rq, w_rk, w_rv, w_rg)
    names = ("q", "k", "v", "rq", "rk", "rv", "g")
    cols = [w.shape[1] for w in weights]
    joined = all(count % 128 == 0 for count in cols)
    places, dots = [], []
    if joined:
        buffers = [sum(cols)]
        at = 0
        for count in cols:
            places.append((0, at, count))
            at += count
        for group in ((3, 4), (5,), (1, 2), (0,), (6,)):
            dots.append((0, places[group[0]][1], sum(cols[i] for i in group),
                         tuple((names[i], cols[i]) for i in group)))
    else:
        buffers = cols
        for i, count in enumerate(cols):
            places.append((i, 0, count))
            dots.append((i, 0, count, ((names[i], count),)))
    att_w, ret_w = heads * HD, ret * RV
    paired = kv == 2 and 2 * HD == 128
    assert kv == 1 or HD % ((att_w + ret_w) // n_sp) == 0
    cfg = dict(paired=paired, n_sp=n_sp, n_tp=n_tp, n_chips=n_chips, chunks=chunks, chan=chan, heads=heads,
               ret=ret, kv=kv, buffers=buffers, places=places, dots=dots, joined=joined)
    tables = rope_tables(n_sp * chunks, CHUNK, ret) + rope_tables(CHUNK, 1, ret)
    small = [norm_gain.reshape(1, width), att_sink.reshape(1, heads), decay_log]
    small += [jnp.asarray(t) for t in tables]
    anyw = pl.BlockSpec(memory_space=pl.ANY)
    dma = pltpu.SemaphoreType.DMA
    mixes = rows // MIX
    scratch = [pltpu.VMEM((width, count), BF16) for count in buffers] + [
        pltpu.VMEM(a.shape, F32) for a in small] + [
        pltpu.VMEM((rows, group[2]), F32) for group in dots] + [
        pltpu.VMEM((n_tp, att_w + ret_w, chan), BF16),
        pltpu.VMEM((n_tp, rows, chan), BF16),
        pltpu.VMEM((max(n_chips - 1, 1), CHUNK, 2 * chan), BF16),
        pltpu.VMEM((rows, att_w * (2 if paired else 1)), BF16),
        pltpu.VMEM((rows + 2 * WINDOW, kv_cols), BF16),
        pltpu.VMEM((kv_cols, rows + 2 * WINDOW), BF16),
        pltpu.VMEM((n_tp, rows, att_w + ret_w), BF16),
        pltpu.VMEM((ret, rows, 2 * RK), BF16),
        pltpu.VMEM((ret, rows, RV), F32),
        pltpu.VMEM((rows, ret_w), BF16),
        pltpu.VMEM((ret, chunks, RK, RV), F32),
        pltpu.VMEM((ret, chunks, RK, RV), F32),
        pltpu.VMEM((ret, chunks, 8, 128), F32),
        pltpu.VMEM((ret, chunks, 2 * RK, RV), BF16),
        pltpu.VMEM((rows, 1), F32),
        pltpu.VMEM((ret, chunks, CHUNK, CHUNK), F32),
        pltpu.VMEM((ret, rows, 2 * RK), F32),
        pltpu.VMEM((ret, rows, 2 * RK), F32),
        pltpu.VMEM((3, MIX + 2 * WINDOW, MIX), F32),
        pltpu.VMEM((ret, RK, RV), BF16),
        pltpu.VMEM((ret, RK, RV), BF16),
        pltpu.VMEM((n_sp, ret, RK, RV), BF16),
        pltpu.VMEM((n_sp, ret, 8, 128), F32),
        pltpu.VMEM((2, ret, RK, RV), F32),
        pltpu.SemaphoreType.REGULAR,
        dma((len(buffers),)), dma, dma, dma((len(small) + 1,)),
        dma, dma((n_chips - 1, chunks)), dma((chunks,)), dma((chunks,)),
        dma, dma((n_chips - 1, mixes)), dma((n_chips - 1, mixes)), dma((mixes,)),
        dma, dma, dma((3,)), dma((n_sp // 2 + 1,)),
        dma((2,)), dma((2,)),
        dma, dma, dma, dma,
    ]
    return pl.pallas_call(
        functools.partial(kernel, cfg),
        out_shape=pltpu.VMEM((rows, chan), BF16),
        in_specs=[anyw] * (11 + len(small)),
        out_specs=pl.BlockSpec(memory_space=pltpu.VMEM),
        scratch_shapes=scratch,
        compiler_params=pltpu.CompilerParams(
            collective_id=0, has_side_effects=True, vmem_limit_bytes=60 * 1024 * 1024),
    )(tokens, *weights, init_state, out_att, out_ret, *small)


def solution(mesh):
    n_sp, n_tp = mesh.shape["sp"], mesh.shape["tp"]
    in_specs = (
        P("sp", "tp"),
        P(),
        P(None, "tp"),
        P(None, "tp"),
        P(None, "tp"),
        P(None, "tp"),
        P(None, "tp"),
        P(None, "tp"),
        P(None, "tp"),
        P("tp"),
        P("tp", "sp"),
        P(None, "tp", None, None),
        P("tp", None),
        P("tp", None),
    )
    return jax.shard_map(functools.partial(body, n_sp, n_tp), mesh=mesh, in_specs=in_specs,
                         out_specs=P("sp", "tp"), check_vma=False)
```

```python
import contextlib
import functools

import jax
import jax.numpy as jnp
import numpy as np
from jax import lax
from jax.experimental import pallas as pl
from jax.experimental.pallas import tpu as pltpu
from jax.sharding import PartitionSpec as P

HD = 64
RK = 64
RV = 128
WINDOW = 128
CHUNK = 256
MIX = 128
NORM_EPS = 1e-06
ROPE_BASE = 10000.0
F32 = jnp.float32
BF16 = jnp.bfloat16
MESH = pl.DeviceIdType.MESH


def scope(name):
    return contextlib.nullcontext()


def rope_tables(count, step, heads):
    half = RK // 2
    inverse = ROPE_BASE ** (-2.0 * np.arange(half, dtype=np.float64) / RK)
    angles = (np.arange(count, dtype=np.float64) * step)[:, None] * inverse[None, :]
    wide = np.tile(np.concatenate([angles, angles], axis=1), (1, heads))
    return np.cos(wide).astype(np.float32), np.sin(wide).astype(np.float32)


def remote(src, dst, send, recv, **where):
    return pltpu.make_async_remote_copy(
        src_ref=src, dst_ref=dst, send_sem=send, recv_sem=recv,
        device_id=where, device_id_type=MESH,
    )


def rows_of(index, size):
    return pl.ds(pl.multiple_of(index * size, size), size)


def mm(a, b):
    return jnp.dot(a, b, preferred_element_type=F32)


def mm_t(a, b):
    return lax.dot_general(a, b, (((1,), (1,)), ((), ())), preferred_element_type=F32)


def tm_m(a, b):
    return lax.dot_general(a, b, (((0,), (0,)), ((), ())), preferred_element_type=F32)


class Spread:
    def __init__(self, place, buf, columns, size, send, cross, near, settled, src=None):
        self.place, self.buf, self.columns, self.size = place, buf, columns, size
        self.send, self.cross, self.near, self.settled, self.src = send, cross, near, settled, src

    def block(self, slot, c):
        return self.buf.at[slot, rows_of(c, self.size), self.columns]

    def start(self, c):
        tp, partner, across, n_chips = self.place
        src = self.block(tp, c) if self.src is None else self.src.at[rows_of(c, self.size), :]
        for k in range(1, n_chips):
            remote(src, self.block(tp, c), self.send, self.cross.at[n_chips - k - 1, c], tp=across(k)).start()
        remote(src, self.block(tp, c), self.send, self.near.at[c], tp=partner).start()

    def relay(self, c):
        _, partner, across, n_chips = self.place
        for k in range(1, n_chips):
            block = self.block(across(k), c)
            remote(block, block, self.send, self.cross.at[k - 1, c], tp=partner).wait_recv()
            remote(block, block, self.send, self.settled.at[c], tp=partner).start()


def kernel(cfg, *refs):
    n_buf, n_small = len(cfg["buffers"]), 8
    (tokens, w_q, w_k, w_v, w_rq, w_rk, w_rv, w_rg, init, o_att, o_ret) = refs[:11]
    small_hbm = refs[11:11 + n_small - 1]
    out = refs[10 + n_small]
    rest = refs[11 + n_small:]
    w_bufs = rest[:n_buf]
    small = rest[n_buf:n_buf + n_small - 1]
    parts = rest[n_buf + n_small - 1:n_buf + n_small - 1 + len(cfg["dots"])]
    gain, sink, decay, outer_cos, outer_sin, inner_cos, inner_sin = small
    (wg, gath, xbuf, qs, kbuf, vt, mx, qfb, rloc, gs, fterm, bterm, blog, both_in,
     sqs, dm, kfac, qfac, bias,
     tot_f, tot_b, tots, logs, states,
     ready, w_sem, wo_sem, tok_sem, small_sem,
     tok_send, tok_cross, tok_near, tok_settled, mix_send, att_cross, ret_cross, mix_settled,
     pw_send, pw_recv, w_send, w_recv,
     halo_send, halo_recv, tot_send, tot_recv, log_send, log_recv) = rest[n_buf + n_small - 1 + len(parts):]
    n_tp, n_sp, n_chips, chunks = cfg["n_tp"], cfg["n_sp"], cfg["n_chips"], cfg["chunks"]
    chan, heads, ret, kv = cfg["chan"], cfg["heads"], cfg["ret"], cfg["kv"]
    rows = chunks * CHUNK
    width = n_tp * chan
    groups = heads // kv
    seq_len = rows * n_sp
    att_w, ret_w = heads * HD, ret * RV
    piece = (att_w + ret_w) // n_sp
    per = CHUNK // MIX
    mixes = rows // MIX
    sp = lax.axis_index("sp")
    tp = lax.axis_index("tp")
    core = lax.rem(tp, 2)
    chip = lax.div(tp, 2)
    partner = chip * 2 + 1 - core

    def across(k):
        return lax.rem(chip + k, n_chips) * 2 + core

    place = (tp, partner, across, n_chips)
    tok = Spread(place, gath, slice(None), CHUNK, tok_send, tok_cross, tok_near, tok_settled, src=tokens)
    atd = Spread(place, mx, pl.ds(0, att_w), MIX, mix_send, att_cross, mix_settled, mix_settled)
    rtd = [Spread(place, mx, pl.ds(att_w + h * RV, RV), MIX, mix_send, ret_cross.at[h], mix_settled, mix_settled)
           for h in range(ret)]

    def arrived(ref, sem):
        pltpu.make_async_copy(ref, ref, sem).wait()

    barrier = pltpu.get_barrier_semaphore()
    for k in range(1, n_tp):
        pl.semaphore_signal(barrier, inc=1, device_id={"tp": lax.rem(tp + k, n_tp)}, device_id_type=MESH)

    @pl.when(sp == 0)
    def _():
        for k in range(1, n_sp):
            pl.semaphore_signal(barrier, inc=1, device_id={"sp": k}, device_id_type=MESH)

    token_copy = pltpu.make_async_copy(tokens, gath.at[tp], tok_sem)
    token_copy.start()
    local = [pltpu.make_async_copy(a, b, small_sem.at[i]) for i, (a, b) in enumerate(zip(small_hbm, small))]
    local.append(pltpu.make_async_copy(init, states, small_sem.at[n_small - 1]))
    weights = (w_q, w_k, w_v, w_rq, w_rk, w_rv, w_rg)
    for w_ref, (b, off, cols) in zip(weights, cfg["places"]):
        dst = w_bufs[b].at[:, pl.ds(off, cols)] if cfg["joined"] else w_bufs[b]
        pltpu.make_async_copy(w_ref, dst, w_sem.at[b]).start()
    paired = cfg["paired"]

    def att_row(row):
        if kv == 1:
            return row
        spot, within = row // HD, row % HD
        return (spot % kv * groups + spot // kv) * HD + within

    runs = [(o_att, att_row(b * HD), b * HD, HD) for b in range(heads)]
    runs.append((o_ret, 0, att_w, ret_w))

    def columns(t):
        return pl.ds(pl.multiple_of(t * chan, chan), chan)

    for src, row, first, count in runs:
        pltpu.make_async_copy(src.at[pl.ds(row, count), columns(tp)], wg.at[tp, pl.ds(first, count), :], wo_sem).start()
    for copy in local:
        copy.start()

    with scope("barrier"):
        @pl.when(sp == 0)
        def _():
            pl.semaphore_wait(barrier, n_tp - 1)

        @pl.when(sp > 0)
        def _():
            pl.semaphore_wait(barrier, n_tp)
            pl.semaphore_signal(ready, inc=1, device_id={"sp": 0}, device_id_type=MESH)

    others = [lax.rem(chip + k, n_chips) * 2 + p for k in range(1, n_chips) for p in range(2)]

    def w_copy(t, e, send, recv, **where):
        block = wg.at[t, rows_of(e, piece), :]
        return remote(block, block, w_send.at[send], w_recv.at[recv], **where)

    def w_done(sem, pieces):
        left, full = pieces * len(others) * piece, att_w + ret_w
        while left > 0:
            arrived(wg.at[0, 0:min(left, full), :], sem)
            left -= full

    def w_first(src, row):
        for t in others:
            remote(src.at[pl.ds(pl.multiple_of(row, piece), piece), columns(t)], wg.at[tp, rows_of(sp, piece), :],
                   w_send.at[0], w_recv.at[0], tp=t).start()

    @pl.when(sp * piece < att_w)
    def _():
        w_first(o_att, att_row(sp * piece))

    @pl.when(sp * piece >= att_w)
    def _():
        w_first(o_ret, sp * piece - att_w)

    def order(i):
        return lax.rem(i + chunks - 1, chunks)

    def first_sends(i, carry):
        tok.start(order(i))
        return carry

    lax.fori_loop(0, chunks, first_sends, 0)

    for src, row, first, count in runs:
        remote(src.at[pl.ds(row, count), columns(partner)], wg.at[tp, pl.ds(first, count), :],
               pw_send, pw_recv, tp=partner).start()

    with scope("lwait"):
        for copy in local:
            copy.wait()
        token_copy.wait()
        for i, buf in enumerate(w_bufs):
            arrived(buf, w_sem.at[i])
        arrived(wg.at[tp], wo_sem)

    for h in range(ret):
        total = jnp.sum(decay[h:h + 1, :], axis=1, keepdims=True)
        logs[sp, h] = jnp.broadcast_to(total, (8, 128))

    @pl.when(sp == 0)
    def _():
        kbuf[0:WINDOW, :] = jnp.zeros((WINDOW, kbuf.shape[1]), BF16)
        vt[:, 0:WINDOW] = jnp.zeros((vt.shape[0], WINDOW), BF16)

    @pl.when(sp == n_sp - 1)
    def _():
        kbuf[rows + WINDOW:, :] = jnp.zeros((WINDOW, kbuf.shape[1]), BF16)
        vt[:, rows + WINDOW:] = jnp.zeros((vt.shape[0], WINDOW), BF16)

    row_i = lax.broadcasted_iota(jnp.int32, (CHUNK, CHUNK), 0)
    col_i = lax.broadcasted_iota(jnp.int32, (CHUNK, CHUNK), 1)
    low = lax.broadcasted_iota(jnp.int32, (CHUNK, 2 * RK), 1) < RK

    def decays(c, carry):
        here = rows_of(c, CHUNK)
        for h in range(ret):
            log_row = decay[h:h + 1, here]
            wide = jnp.broadcast_to(log_row, (CHUNK, CHUNK))
            log_col = jnp.sum(jnp.where(row_i == col_i, wide, 0.0), axis=1, keepdims=True)
            cum_col = jnp.sum(jnp.where(col_i <= row_i, wide, 0.0), axis=1, keepdims=True)
            cum_row = jnp.sum(jnp.where(row_i <= col_i, log_col, 0.0), axis=0, keepdims=True)
            total = jnp.sum(log_row, axis=1, keepdims=True)
            dm[h, c] = jnp.exp(-jnp.abs(cum_col - cum_row))
            up = jnp.exp(cum_col)
            down = jnp.exp(jnp.minimum(total - cum_col, 0.0))
            kfac[h, here, :] = jnp.where(low, down, up)
            qfac[h, here, :] = jnp.where(low, up, down)
            blog[h, c] = jnp.broadcast_to(total, (8, 128))
        return carry

    with scope("decays"):
        lax.fori_loop(0, chunks, decays, 0)

    shape = (MIX + 2 * WINDOW, MIX)
    q_i = lax.broadcasted_iota(jnp.int32, shape, 1)
    k_i = lax.broadcasted_iota(jnp.int32, shape, 0)
    band = (k_i >= q_i) & (k_i <= q_i + 2 * WINDOW)
    bias[0] = jnp.where(band, 0.0, -jnp.inf)
    bias[1] = jnp.where(band & (k_i >= WINDOW), 0.0, -jnp.inf)
    bias[2] = jnp.where(band & (k_i < MIX + WINDOW), 0.0, -jnp.inf)

    def normed(c, which, dst):
        here = rows_of(c, CHUNK)
        squares = jnp.zeros((CHUNK, 1), F32)
        for p in range(2):
            slot = which * 2 + p
            x = gath[slot, here, :].astype(F32)
            squares = squares + jnp.sum(x * x, axis=1, keepdims=True)
            xbuf[dst, :, p * chan:(p + 1) * chan] = (x * gain[0:1, columns(slot)]).astype(BF16)
        return squares

    def product(which, src, b, off, cols):
        span = pl.ds(pl.multiple_of(which * (2 * chan), 2 * chan), 2 * chan)
        return mm(xbuf[src], w_bufs[b][span, off:off + cols])

    def near(i, carry):
        c = order(i)
        here = rows_of(c, CHUNK)
        arrived(gath.at[0, here, :], tok_near.at[c])
        sqs[here, :] = normed(c, chip, 0)
        for part, (b, off, cols, _) in zip(parts, cfg["dots"]):
            part[here, :] = product(chip, 0, b, off, cols)
        return carry

    with scope("near"):
        lax.fori_loop(0, chunks // 2, near, 0)

    with scope("ready"):
        @pl.when(sp == 0)
        def _():
            pl.semaphore_wait(ready, n_sp - 1)
            for k in range(1, n_sp):
                pl.semaphore_signal(ready, inc=1, device_id={"sp": k}, device_id_type=MESH)

        @pl.when(sp > 0)
        def _():
            pl.semaphore_wait(ready, 1)

    for k in range(1, n_sp):
        remote(logs.at[sp], logs.at[sp], log_send, log_recv, sp=lax.rem(sp + k, n_sp)).start()

    beside = sp + 1 - 2 * lax.rem(sp, 2)
    half_sp = n_sp // 2
    with scope("wfwd"):
        w_done(w_recv.at[0], 1)

        def w_pass(k, carry):
            for t in others:
                w_copy(t, sp, 1, k + 1, sp=lax.rem(sp + 2 * k, n_sp)).start()
            return carry

        lax.fori_loop(1, half_sp, w_pass, 0)
        for t in others:
            w_copy(t, sp, 2, 1, sp=beside).start()

    def w_aside(first, end):
        def w_over(k, carry):
            w_done(w_recv.at[k + 1], 1)
            for t in others:
                w_copy(t, lax.rem(sp + n_sp - 2 * k, n_sp), 2, 1, sp=beside).start()
            return carry

        lax.fori_loop(first, end, w_over, 0)

    with scope("near"):
        lax.fori_loop(chunks // 2, chunks, near, 0)

    rw = ret * RK
    p_row = lax.broadcasted_iota(jnp.int32, (rw, rw), 0)
    p_col = lax.broadcasted_iota(jnp.int32, (rw, rw), 1)
    first_half = lax.rem(p_col, RK) < RK // 2
    swap = jnp.where(
        first_half & (p_row == p_col + RK // 2), -1.0,
        jnp.where(jnp.logical_not(first_half) & (p_row == p_col - RK // 2), 1.0, 0.0),
    ).astype(BF16)
    ones = jnp.ones((HD, MIX + 2 * WINDOW), BF16)

    def attend(i):
        here = rows_of(i, MIX)
        span = pl.ds(pl.multiple_of(i * MIX, MIX), MIX + 2 * WINDOW)
        edge = lax.select((sp == 0) & (i == 0), 1, lax.select((sp == n_sp - 1) & (i == mixes - 1), 2, 0))
        block = bias[edge]
        block = jnp.concatenate([block] * groups, axis=1)
        done = []
        for g in range(kv):
            if paired:
                spots = [(j * kv + g) * 2 * HD for j in range(groups)]
                query = jnp.concatenate([qs[here, at:at + 2 * HD] for at in spots], axis=0)
                key = kbuf[span, :]
            else:
                spots = [(g * groups + j) * HD for j in range(groups)]
                query = jnp.concatenate([qs[here, at:at + HD] for at in spots], axis=0)
                key = kbuf[span, g * HD:(g + 1) * HD]
            value = jnp.concatenate([vt[g * HD:(g + 1) * HD, span], ones], axis=0)
            scores = mm_t(key, query) + block
            sink_row = jnp.concatenate(
                [jnp.broadcast_to(sink[0:1, g * groups + j:g * groups + j + 1], (1, MIX)) for j in range(groups)],
                axis=1)
            top = jnp.maximum(jnp.max(scores, axis=0, keepdims=True), sink_row)
            result = mm(value, jnp.exp(scores - top).astype(BF16))
            scale = 1.0 / (result[HD:HD + 1, :] + jnp.exp(sink_row - top))
            done.append(result[0:HD, :] * scale)
        both = jnp.concatenate(done, axis=0) if kv > 1 else done[0]
        turned = [jnp.transpose(both[:, j * MIX:(j + 1) * MIX]).astype(BF16) for j in range(groups)]
        if kv * HD % 128 == 0:
            for j in range(groups):
                mx[tp, here, j * kv * HD:(j + 1) * kv * HD] = turned[j]
        else:
            mx[tp, here, 0:att_w] = jnp.concatenate(turned, axis=1)
        atd.start(i)

    left, right = sp - 1, sp + 1

    def halo(side, i, where):
        def part(at):
            return kbuf.at[pl.ds(at, WINDOW), :] if i == 0 else vt.at[:, pl.ds(at, WINDOW)]

        src, dst = ((rows, 0), (WINDOW, rows + WINDOW))[side]
        return remote(part(src), part(dst), halo_send.at[side], halo_recv.at[side], sp=where)

    def chunk(c, last, between):
        here = rows_of(c, CHUNK)
        with scope("x1"):
            tok.relay(c)
        between()
        with scope("x2"):
            arrived(gath.at[0:n_chips - 1, here, :], tok_settled.at[c])
        ctx = scope("phaseA")
        ctx.__enter__()
        squares = sqs[here, :]
        far = [(k - 1, lax.rem(chip + k, n_chips)) for k in range(1, n_chips)]
        for at, which in far:
            squares = squares + normed(c, which, at)
        inv_rms = lax.rsqrt(squares / width + NORM_EPS)
        found = {}

        def finish(first):
            for part, (b, off, cols, names) in zip(parts, cfg["dots"]):
                if (names[0][0] in ("rq", "rk", "rv")) != first:
                    continue
                total = part[here, :]
                for at, which in far:
                    total = total + product(which, at, b, off, cols)
                block = (total * inv_rms).astype(BF16)
                at = 0
                for name, count in names:
                    found[name] = block[:, at:at + count]
                    at += count

        finish(True)
        spot = sp * chunks + c
        oc, os_ = outer_cos[pl.ds(spot, 1), :], outer_sin[pl.ds(spot, 1), :]
        ic, is_ = inner_cos[...], inner_sin[...]
        cosine = oc * ic - os_ * is_
        sine = os_ * ic + oc * is_
        query_rot = found["rq"].astype(F32) * cosine + mm(found["rq"], swap) * sine
        key_rot = (found["rk"].astype(F32) * cosine + mm(found["rk"], swap) * sine) * RK ** -0.5

        def doubled(x):
            if ret == 2:
                turned = pltpu.roll(x, RK, 1)
                return jnp.where(low, x, turned), jnp.where(low, turned, x)
            return [jnp.concatenate([x[:, h * RK:(h + 1) * RK]] * 2, axis=1) for h in range(ret)]

        keys = doubled(key_rot)
        for h in range(ret):
            both = (keys[h] * kfac[h, here, :]).astype(BF16)
            terms = tm_m(both, found["rv"][:, h * RV:(h + 1) * RV])
            fterm[h, c] = terms[:RK]
            bterm[h, c] = terms[RK:]
        ctx.__exit__(None, None, None)
        if last:
            with scope("totals"):
                send_totals()
        ctx = scope("phaseB")
        ctx.__enter__()
        finish(False)
        scaled = found["q"] * jnp.asarray(HD ** -0.5, BF16)
        if paired:
            wide = scaled.astype(F32)
            head = [wide[:, at:at + 2 * HD] for at in range(0, att_w, 2 * HD)]
            turned = [pltpu.roll(x, HD, 1) for x in head]
            for j in range(groups):
                for g in range(kv):
                    at = (g * groups + j) * HD
                    x = (head if at % (2 * HD) == g * HD else turned)[at // (2 * HD)]
                    keep = low if g == 0 else jnp.logical_not(low)
                    to = (j * kv + g) * 2 * HD
                    qs[here, to:to + 2 * HD] = jnp.where(keep, x, 0.0).astype(BF16)
        else:
            qs[here, :] = scaled
        shifted = pl.ds(pl.multiple_of(c * CHUNK + WINDOW, 128), CHUNK)
        kbuf[shifted, :] = found["k"]
        vt[:, shifted] = jnp.transpose(found["v"].astype(F32)).astype(BF16)
        gs[here, :] = found["g"]
        queries = doubled(query_rot)
        key_bf = key_rot.astype(BF16)
        for h in range(ret):
            if ret == 2:
                keep = low if h == 0 else jnp.logical_not(low)
                inner = mm_t(jnp.where(keep, query_rot, 0.0).astype(BF16), key_bf)
            else:
                inner = mm_t(query_rot[:, h * RK:(h + 1) * RK].astype(BF16), key_bf[:, h * RK:(h + 1) * RK])
            rloc[h, here, :] = mm((inner * dm[h, c]).astype(BF16), found["rv"][:, h * RV:(h + 1) * RV])
            qfb[h, here, :] = (queries[h] * qfac[h, here, :]).astype(BF16)
        ctx.__exit__(None, None, None)

    def send_totals():
        for h in range(ret):
            state = jnp.zeros((RK, RV), F32)
            back = jnp.zeros((RK, RV), F32)
            for c in range(chunks):
                state = jnp.exp(blog[h, c, 0:1, :]) * state + fterm[h, c]
                back = jnp.exp(blog[h, chunks - 1 - c, 0:1, :]) * back + bterm[h, chunks - 1 - c]
            tot_f[h] = state.astype(BF16)
            tot_b[h] = back.astype(BF16)

            def send_f(i, carry):
                remote(tot_f.at[h], tots.at[sp, h], tot_send, tot_recv.at[h], sp=n_sp - 1 - i).start()
                return carry

            def send_b(d, carry):
                remote(tot_b.at[h], tots.at[sp, h], tot_send, tot_recv.at[h], sp=d).start()
                return carry

            lax.fori_loop(0, n_sp - 1 - sp, send_f, 0)
            lax.fori_loop(0, sp, send_b, 0)

    early = per * (chunks - 3) + 1

    def block_of(j):
        turn = early - per + 1
        return lax.select(j < turn, j, lax.select(j == turn, mixes - 1, j - 1))

    def halo_wait(side):
        arrived(kbuf.at[0:2 * WINDOW, :], halo_recv.at[side])

    def one(j):
        with scope("attend"):
            attend(j)

    def chunk_body(i, carry):
        c = order(i)

        if chunks > 4:
            @pl.when(i > 2)
            def _():
                one(per * (i - 3) + 1)

        def between():
            @pl.when(i == chunks - 2)
            def _():
                with scope("aside"):
                    w_aside(chunks - 1, half_sp)

            @pl.when((i == 2) & (sp > 0))
            def _():
                with scope("halo0"):
                    halo_wait(0)

            @pl.when(i == 2)
            def _():
                one(0)

            if chunks > 4:
                @pl.when(i > 2)
                def _():
                    one(per * (i - 3) + 2)

        chunk(c, False, between)

        @pl.when((i == 0) & (sp < n_sp - 1))
        def _():
            for b in range(2):
                halo(0, b, right).start()

        @pl.when((i == 1) & (sp > 0))
        def _():
            for b in range(2):
                halo(1, b, left).start()

        @pl.when(i < min(chunks - 2, half_sp - 1))
        def _():
            with scope("aside"):
                w_aside(i + 1, i + 2)

        return carry

    lax.fori_loop(0, chunks - 1, chunk_body, 0)

    one(early - per)

    @pl.when(sp < n_sp - 1)
    def _():
        with scope("halo1"):
            halo_wait(1)

    one(mixes - 1)
    chunk(chunks - 2, True, lambda: one(early - per + 1))

    def late(j, carry):
        with scope("late"):
            attend(j)
        with scope("lrelay"):
            atd.relay(block_of(j - early))
        return carry

    lax.fori_loop(early, mixes - 1, late, 0)

    def states_of(h):
        arrived(tots.at[0:n_sp - 1, 0], tot_recv.at[h])

        def from_low(e, state):
            return jnp.exp(logs[e, h, 0:1, :]) * state + tots[e, h].astype(F32)

        def from_high(i, back):
            e = n_sp - 1 - i
            return jnp.exp(logs[e, h, 0:1, :]) * back + tots[e, h].astype(F32)

        state = lax.fori_loop(0, sp, from_low, states[0, h])
        back = lax.fori_loop(0, n_sp - 1 - sp, from_high, states[1, h])
        for c in range(chunks):
            both_in[h, c, 0:RK] = state.astype(BF16)
            state = jnp.exp(blog[h, c, 0:1, :]) * state + fterm[h, c]
            r = chunks - 1 - c
            both_in[h, r, RK:2 * RK] = back.astype(BF16)
            back = jnp.exp(blog[h, r, 0:1, :]) * back + bterm[h, r]

    def retain(c, h):
        here = rows_of(c, MIX)
        combined = rloc[h, here, :] + mm(qfb[h, here, :], both_in[h, lax.div(c, per)])
        centered = combined - jnp.mean(combined, axis=1, keepdims=True)
        normed_ret = centered * lax.rsqrt(jnp.mean(centered * centered, axis=1, keepdims=True) + NORM_EPS)
        gate = gs[here, h * RV:(h + 1) * RV].astype(F32)
        mx[tp, here, att_w + h * RV:att_w + (h + 1) * RV] = (gate / (1.0 + jnp.exp(-gate)) * normed_ret).astype(BF16)
        rtd[h].start(c)

    arrived(logs.at[0:n_sp - 1], log_recv)
    for h in range(ret):
        with scope("states"):
            states_of(h)

        def ret_body(c, carry):
            retain(c, h)
            return carry

        with scope("retain"):
            lax.fori_loop(0, mixes, ret_body, 0)

    def att_rest(j, carry):
        atd.relay(block_of(j))
        return carry

    with scope("attrest"):
        lax.fori_loop(mixes - 1 - early, mixes, att_rest, 0)

    def ret_relay(h):
        def relayed(c, carry):
            rtd[h].relay(c)
            return carry

        with scope("hrelay"):
            lax.fori_loop(0, mixes, relayed, 0)

    for h in range(ret - 1):
        ret_relay(h)

    with scope("wsettle"):
        arrived(wg.at[0], pw_recv)
        w_done(w_recv.at[1], half_sp)

    def mix(c):
        here = rows_of(c, MIX)
        with scope("msettle"):
            arrived(mx.at[0:n_chips, here, :], mix_settled.at[c])
        with scope("mix"):
            total = mm(mx[0, here, :], wg[0])
            for t in range(1, n_tp):
                total = total + mm(mx[t, here, :], wg[t])
            out[here, :] = total.astype(BF16)

    def mix_body(c, carry):
        @pl.when(c < mixes)
        def _():
            with scope("rrelay"):
                rtd[ret - 1].relay(c)

        @pl.when(c > 0)
        def _():
            mix(c - 1)

        return carry

    lax.fori_loop(0, mixes + 1, mix_body, 0)

    with scope("drain"):
        sent = 2 * n_chips - 1
        arrived(gath.at[0:sent], tok_send)
        arrived(mx.at[0:sent], mix_send)
        arrived(wg.at[0], pw_send)
        w_done(w_send.at[0], 1)
        w_done(w_send.at[1], half_sp - 1)
        w_done(w_send.at[2], half_sp)
        arrived(logs.at[0:n_sp - 1], log_send)
        arrived(tots.at[0:n_sp - 1], tot_send)

        @pl.when(sp < n_sp - 1)
        def _():
            arrived(kbuf.at[0:2 * WINDOW, :], halo_send.at[0])

        @pl.when(sp > 0)
        def _():
            arrived(kbuf.at[0:2 * WINDOW, :], halo_send.at[1])


def body(n_sp, n_tp, tokens, norm_gain, w_q, w_k, w_v, w_rq, w_rk, w_rv, w_rg, att_sink,
         decay_log, init_state, out_att, out_ret):
    rows, chan = tokens.shape
    width = n_tp * chan
    ret = decay_log.shape[0]
    heads = att_sink.shape[0]
    kv_cols = w_k.shape[1]
    kv = kv_cols // HD
    chunks = rows // CHUNK
    n_chips = n_tp // 2
    weights = (w_q, w_k, w_v, w_rq, w_rk, w_rv, w_rg)
    names = ("q", "k", "v", "rq", "rk", "rv", "g")
    cols = [w.shape[1] for w in weights]
    joined = all(count % 128 == 0 for count in cols)
    places, dots = [], []
    if joined:
        buffers = [sum(cols)]
        at = 0
        for count in cols:
            places.append((0, at, count))
            at += count
        for group in ((3, 4), (5,), (1, 2), (0,), (6,)):
            dots.append((0, places[group[0]][1], sum(cols[i] for i in group),
                         tuple((names[i], cols[i]) for i in group)))
    else:
        buffers = cols
        for i, count in enumerate(cols):
            places.append((i, 0, count))
            dots.append((i, 0, count, ((names[i], count),)))
    att_w, ret_w = heads * HD, ret * RV
    paired = kv == 2 and 2 * HD == 128
    assert kv == 1 or HD % ((att_w + ret_w) // n_sp) == 0
    cfg = dict(paired=paired, n_sp=n_sp, n_tp=n_tp, n_chips=n_chips, chunks=chunks, chan=chan, heads=heads,
               ret=ret, kv=kv, buffers=buffers, places=places, dots=dots, joined=joined)
    tables = rope_tables(n_sp * chunks, CHUNK, ret) + rope_tables(CHUNK, 1, ret)
    small = [norm_gain.reshape(1, width), att_sink.reshape(1, heads), decay_log]
    small += [jnp.asarray(t) for t in tables]
    anyw = pl.BlockSpec(memory_space=pl.ANY)
    dma = pltpu.SemaphoreType.DMA
    mixes = rows // MIX
    scratch = [pltpu.VMEM((width, count), BF16) for count in buffers] + [
        pltpu.VMEM(a.shape, F32) for a in small] + [
        pltpu.VMEM((rows, group[2]), F32) for group in dots] + [
        pltpu.VMEM((n_tp, att_w + ret_w, chan), BF16),
        pltpu.VMEM((n_tp, rows, chan), BF16),
        pltpu.VMEM((max(n_chips - 1, 1), CHUNK, 2 * chan), BF16),
        pltpu.VMEM((rows, att_w * (2 if paired else 1)), BF16),
        pltpu.VMEM((rows + 2 * WINDOW, kv_cols), BF16),
        pltpu.VMEM((kv_cols, rows + 2 * WINDOW), BF16),
        pltpu.VMEM((n_tp, rows, att_w + ret_w), BF16),
        pltpu.VMEM((ret, rows, 2 * RK), BF16),
        pltpu.VMEM((ret, rows, RV), F32),
        pltpu.VMEM((rows, ret_w), BF16),
        pltpu.VMEM((ret, chunks, RK, RV), F32),
        pltpu.VMEM((ret, chunks, RK, RV), F32),
        pltpu.VMEM((ret, chunks, 8, 128), F32),
        pltpu.VMEM((ret, chunks, 2 * RK, RV), BF16),
        pltpu.VMEM((rows, 1), F32),
        pltpu.VMEM((ret, chunks, CHUNK, CHUNK), F32),
        pltpu.VMEM((ret, rows, 2 * RK), F32),
        pltpu.VMEM((ret, rows, 2 * RK), F32),
        pltpu.VMEM((3, MIX + 2 * WINDOW, MIX), F32),
        pltpu.VMEM((ret, RK, RV), BF16),
        pltpu.VMEM((ret, RK, RV), BF16),
        pltpu.VMEM((n_sp, ret, RK, RV), BF16),
        pltpu.VMEM((n_sp, ret, 8, 128), F32),
        pltpu.VMEM((2, ret, RK, RV), F32),
        pltpu.SemaphoreType.REGULAR,
        dma((len(buffers),)), dma, dma, dma((len(small) + 1,)),
        dma, dma((n_chips - 1, chunks)), dma((chunks,)), dma((chunks,)),
        dma, dma((n_chips - 1, mixes)), dma((ret, n_chips - 1, mixes)), dma((mixes,)),
        dma, dma, dma((3,)), dma((n_sp // 2 + 1,)),
        dma((2,)), dma((2,)),
        dma, dma((ret,)), dma, dma,
    ]
    return pl.pallas_call(
        functools.partial(kernel, cfg),
        out_shape=pltpu.VMEM((rows, chan), BF16),
        in_specs=[anyw] * (11 + len(small)),
        out_specs=pl.BlockSpec(memory_space=pltpu.VMEM),
        scratch_shapes=scratch,
        compiler_params=pltpu.CompilerParams(
            collective_id=0, has_side_effects=True, vmem_limit_bytes=60 * 1024 * 1024),
    )(tokens, *weights, init_state, out_att, out_ret, *small)


def solution(mesh):
    n_sp, n_tp = mesh.shape["sp"], mesh.shape["tp"]
    in_specs = (
        P("sp", "tp"),
        P(),
        P(None, "tp"),
        P(None, "tp"),
        P(None, "tp"),
        P(None, "tp"),
        P(None, "tp"),
        P(None, "tp"),
        P(None, "tp"),
        P("tp"),
        P("tp", "sp"),
        P(None, "tp", None, None),
        P("tp", None),
        P("tp", None),
    )
    return jax.shard_map(functools.partial(body, n_sp, n_tp), mesh=mesh, in_specs=in_specs,
                         out_specs=P("sp", "tp"), check_vma=False)
```

```python
import contextlib
import functools

import jax
import jax.numpy as jnp
import numpy as np
from jax import lax
from jax.experimental import pallas as pl
from jax.experimental.pallas import tpu as pltpu
from jax.sharding import PartitionSpec as P

HD = 64
RK = 64
RV = 128
WINDOW = 128
CHUNK = 256
MIX = 128
NORM_EPS = 1e-06
ROPE_BASE = 10000.0
F32 = jnp.float32
BF16 = jnp.bfloat16
MESH = pl.DeviceIdType.MESH


def scope(name):
    return contextlib.nullcontext()


def rope_tables(count, step, heads):
    half = RK // 2
    inverse = ROPE_BASE ** (-2.0 * np.arange(half, dtype=np.float64) / RK)
    angles = (np.arange(count, dtype=np.float64) * step)[:, None] * inverse[None, :]
    wide = np.tile(np.concatenate([angles, angles], axis=1), (1, heads))
    return np.cos(wide).astype(np.float32), np.sin(wide).astype(np.float32)


def remote(src, dst, send, recv, **where):
    return pltpu.make_async_remote_copy(
        src_ref=src, dst_ref=dst, send_sem=send, recv_sem=recv,
        device_id=where, device_id_type=MESH,
    )


def rows_of(index, size):
    return pl.ds(pl.multiple_of(index * size, size), size)


def mm(a, b):
    return jnp.dot(a, b, preferred_element_type=F32)


def mm_t(a, b):
    return lax.dot_general(a, b, (((1,), (1,)), ((), ())), preferred_element_type=F32)


def tm_m(a, b):
    return lax.dot_general(a, b, (((0,), (0,)), ((), ())), preferred_element_type=F32)


class Spread:
    def __init__(self, place, buf, columns, size, send, cross, near, settled, src=None):
        self.place, self.buf, self.columns, self.size = place, buf, columns, size
        self.send, self.cross, self.near, self.settled, self.src = send, cross, near, settled, src

    def block(self, slot, c):
        return self.buf.at[slot, rows_of(c, self.size), self.columns]

    def start(self, c):
        tp, partner, across, n_chips = self.place
        src = self.block(tp, c) if self.src is None else self.src.at[rows_of(c, self.size), :]
        for k in range(1, n_chips):
            remote(src, self.block(tp, c), self.send, self.cross.at[n_chips - k - 1, c], tp=across(k)).start()
        remote(src, self.block(tp, c), self.send, self.near.at[c], tp=partner).start()

    def relay(self, c):
        _, partner, across, n_chips = self.place
        for k in range(1, n_chips):
            block = self.block(across(k), c)
            remote(block, block, self.send, self.cross.at[k - 1, c], tp=partner).wait_recv()
            remote(block, block, self.send, self.settled.at[c], tp=partner).start()


def kernel(cfg, *refs):
    n_buf, n_small = len(cfg["buffers"]), 8
    (tokens, w_q, w_k, w_v, w_rq, w_rk, w_rv, w_rg, init, o_att, o_ret) = refs[:11]
    small_hbm = refs[11:11 + n_small - 1]
    out = refs[10 + n_small]
    rest = refs[11 + n_small:]
    w_bufs = rest[:n_buf]
    small = rest[n_buf:n_buf + n_small - 1]
    parts = rest[n_buf + n_small - 1:n_buf + n_small - 1 + len(cfg["dots"])]
    gain, sink, decay, outer_cos, outer_sin, inner_cos, inner_sin = small
    (wg, gath, xbuf, qs, kbuf, vt, mx, qfb, rloc, gs, fterm, bterm, blog, both_in,
     sqs, dm, kfac, qfac, bias, base,
     tot_f, tot_b, tots, logs, states,
     ready, w_sem, wo_sem, tok_sem, small_sem,
     tok_send, tok_cross, tok_near, tok_settled, mix_send, att_cross, ret_cross, most_settled, last_settled,
     pw_send, pw_recv, w_send, w_recv,
     halo_send, halo_recv, tot_send, tot_recv, log_send, log_recv) = rest[n_buf + n_small - 1 + len(parts):]
    n_tp, n_sp, n_chips, chunks = cfg["n_tp"], cfg["n_sp"], cfg["n_chips"], cfg["chunks"]
    chan, heads, ret, kv = cfg["chan"], cfg["heads"], cfg["ret"], cfg["kv"]
    rows = chunks * CHUNK
    width = n_tp * chan
    groups = heads // kv
    seq_len = rows * n_sp
    att_w, ret_w = heads * HD, ret * RV
    piece = (att_w + ret_w) // n_sp
    per = CHUNK // MIX
    mixes = rows // MIX
    sp = lax.axis_index("sp")
    tp = lax.axis_index("tp")
    core = lax.rem(tp, 2)
    chip = lax.div(tp, 2)
    partner = chip * 2 + 1 - core

    def across(k):
        return lax.rem(chip + k, n_chips) * 2 + core

    place = (tp, partner, across, n_chips)
    tok = Spread(place, gath, slice(None), CHUNK, tok_send, tok_cross, tok_near, tok_settled, src=tokens)
    atd = Spread(place, mx, pl.ds(0, att_w), MIX, mix_send, att_cross, most_settled, most_settled)
    most = att_w + ret_w - RV
    rtd = []
    for h in range(ret):
        settled = most_settled if h < ret - 1 else last_settled
        rtd.append(Spread(place, mx, pl.ds(att_w + h * RV, RV), MIX, mix_send, ret_cross.at[h], settled, settled))

    def arrived(ref, sem):
        pltpu.make_async_copy(ref, ref, sem).wait()

    barrier = pltpu.get_barrier_semaphore()
    for k in range(1, n_tp):
        pl.semaphore_signal(barrier, inc=1, device_id={"tp": lax.rem(tp + k, n_tp)}, device_id_type=MESH)

    @pl.when(sp == 0)
    def _():
        for k in range(1, n_sp):
            pl.semaphore_signal(barrier, inc=1, device_id={"sp": k}, device_id_type=MESH)

    token_copy = pltpu.make_async_copy(tokens, gath.at[tp], tok_sem)
    token_copy.start()
    local = [pltpu.make_async_copy(a, b, small_sem.at[i]) for i, (a, b) in enumerate(zip(small_hbm, small))]
    local.append(pltpu.make_async_copy(init, states, small_sem.at[n_small - 1]))
    weights = (w_q, w_k, w_v, w_rq, w_rk, w_rv, w_rg)
    for w_ref, (b, off, cols) in zip(weights, cfg["places"]):
        dst = w_bufs[b].at[:, pl.ds(off, cols)] if cfg["joined"] else w_bufs[b]
        pltpu.make_async_copy(w_ref, dst, w_sem.at[b]).start()
    paired = cfg["paired"]

    def att_row(row):
        if kv == 1:
            return row
        spot, within = row // HD, row % HD
        return (spot % kv * groups + spot // kv) * HD + within

    runs = [(o_att, att_row(b * HD), b * HD, HD) for b in range(heads)]
    runs.append((o_ret, 0, att_w, ret_w))

    def columns(t):
        return pl.ds(pl.multiple_of(t * chan, chan), chan)

    for src, row, first, count in runs:
        pltpu.make_async_copy(src.at[pl.ds(row, count), columns(tp)], wg.at[tp, pl.ds(first, count), :], wo_sem).start()
    for copy in local:
        copy.start()

    with scope("barrier"):
        @pl.when(sp == 0)
        def _():
            pl.semaphore_wait(barrier, n_tp - 1)

        @pl.when(sp > 0)
        def _():
            pl.semaphore_wait(barrier, n_tp)
            pl.semaphore_signal(ready, inc=1, device_id={"sp": 0}, device_id_type=MESH)

    others = [lax.rem(chip + k, n_chips) * 2 + p for k in range(1, n_chips) for p in range(2)]

    def w_copy(t, e, send, recv, **where):
        block = wg.at[t, rows_of(e, piece), :]
        return remote(block, block, w_send.at[send], w_recv.at[recv], **where)

    def w_done(sem, pieces):
        left, full = pieces * len(others) * piece, att_w + ret_w
        while left > 0:
            arrived(wg.at[0, 0:min(left, full), :], sem)
            left -= full

    def w_first(src, row):
        for t in others:
            remote(src.at[pl.ds(pl.multiple_of(row, piece), piece), columns(t)], wg.at[tp, rows_of(sp, piece), :],
                   w_send.at[0], w_recv.at[0], tp=t).start()

    @pl.when(sp * piece < att_w)
    def _():
        w_first(o_att, att_row(sp * piece))

    @pl.when(sp * piece >= att_w)
    def _():
        w_first(o_ret, sp * piece - att_w)

    def order(i):
        return lax.rem(i + chunks - 1, chunks)

    def first_sends(i, carry):
        tok.start(order(i))
        return carry

    lax.fori_loop(0, chunks, first_sends, 0)

    for src, row, first, count in runs:
        remote(src.at[pl.ds(row, count), columns(partner)], wg.at[tp, pl.ds(first, count), :],
               pw_send, pw_recv, tp=partner).start()

    with scope("lwait"):
        for copy in local:
            copy.wait()
        token_copy.wait()
        for i, buf in enumerate(w_bufs):
            arrived(buf, w_sem.at[i])
        arrived(wg.at[tp], wo_sem)

    for h in range(ret):
        total = jnp.sum(decay[h:h + 1, :], axis=1, keepdims=True)
        logs[sp, h] = jnp.broadcast_to(total, (8, 128))

    @pl.when(sp == 0)
    def _():
        kbuf[0:WINDOW, :] = jnp.zeros((WINDOW, kbuf.shape[1]), BF16)
        vt[:, 0:WINDOW] = jnp.zeros((vt.shape[0], WINDOW), BF16)

    @pl.when(sp == n_sp - 1)
    def _():
        kbuf[rows + WINDOW:, :] = jnp.zeros((WINDOW, kbuf.shape[1]), BF16)
        vt[:, rows + WINDOW:] = jnp.zeros((vt.shape[0], WINDOW), BF16)

    row_i = lax.broadcasted_iota(jnp.int32, (CHUNK, CHUNK), 0)
    col_i = lax.broadcasted_iota(jnp.int32, (CHUNK, CHUNK), 1)
    low = lax.broadcasted_iota(jnp.int32, (CHUNK, 2 * RK), 1) < RK

    def decays(c, carry):
        here = rows_of(c, CHUNK)
        for h in range(ret):
            log_row = decay[h:h + 1, here]
            wide = jnp.broadcast_to(log_row, (CHUNK, CHUNK))
            log_col = jnp.sum(jnp.where(row_i == col_i, wide, 0.0), axis=1, keepdims=True)
            cum_col = jnp.sum(jnp.where(col_i <= row_i, wide, 0.0), axis=1, keepdims=True)
            cum_row = jnp.sum(jnp.where(row_i <= col_i, log_col, 0.0), axis=0, keepdims=True)
            total = jnp.sum(log_row, axis=1, keepdims=True)
            dm[h, c] = jnp.exp(-jnp.abs(cum_col - cum_row))
            up = jnp.exp(cum_col)
            down = jnp.exp(jnp.minimum(total - cum_col, 0.0))
            kfac[h, here, :] = jnp.where(low, down, up)
            qfac[h, here, :] = jnp.where(low, up, down)
            blog[h, c] = jnp.broadcast_to(total, (8, 128))
        return carry

    with scope("decays"):
        lax.fori_loop(0, chunks, decays, 0)

    shape = (MIX + 2 * WINDOW, MIX)
    q_i = lax.broadcasted_iota(jnp.int32, shape, 1)
    k_i = lax.broadcasted_iota(jnp.int32, shape, 0)
    band = (k_i >= q_i) & (k_i <= q_i + 2 * WINDOW)
    bias[0] = jnp.where(band, 0.0, -jnp.inf)
    bias[1] = jnp.where(band & (k_i >= WINDOW), 0.0, -jnp.inf)
    bias[2] = jnp.where(band & (k_i < MIX + WINDOW), 0.0, -jnp.inf)

    def normed(c, which, dst):
        here = rows_of(c, CHUNK)
        squares = jnp.zeros((CHUNK, 1), F32)
        for p in range(2):
            slot = which * 2 + p
            x = gath[slot, here, :].astype(F32)
            squares = squares + jnp.sum(x * x, axis=1, keepdims=True)
            xbuf[dst, :, p * chan:(p + 1) * chan] = (x * gain[0:1, columns(slot)]).astype(BF16)
        return squares

    def product(which, src, b, off, cols):
        span = pl.ds(pl.multiple_of(which * (2 * chan), 2 * chan), 2 * chan)
        return mm(xbuf[src], w_bufs[b][span, off:off + cols])

    def near(i, carry):
        c = order(i)
        here = rows_of(c, CHUNK)
        arrived(gath.at[0, here, :], tok_near.at[c])
        sqs[here, :] = normed(c, chip, 0)
        for part, (b, off, cols, _) in zip(parts, cfg["dots"]):
            part[here, :] = product(chip, 0, b, off, cols)
        return carry

    with scope("near"):
        lax.fori_loop(0, chunks // 2, near, 0)

    with scope("ready"):
        @pl.when(sp == 0)
        def _():
            pl.semaphore_wait(ready, n_sp - 1)
            for k in range(1, n_sp):
                pl.semaphore_signal(ready, inc=1, device_id={"sp": k}, device_id_type=MESH)

        @pl.when(sp > 0)
        def _():
            pl.semaphore_wait(ready, 1)

    for k in range(1, n_sp):
        remote(logs.at[sp], logs.at[sp], log_send, log_recv, sp=lax.rem(sp + k, n_sp)).start()

    beside = sp + 1 - 2 * lax.rem(sp, 2)
    half_sp = n_sp // 2
    with scope("wfwd"):
        w_done(w_recv.at[0], 1)

        def w_pass(k, carry):
            for t in others:
                w_copy(t, sp, 1, k + 1, sp=lax.rem(sp + 2 * k, n_sp)).start()
            return carry

        lax.fori_loop(1, half_sp, w_pass, 0)
        for t in others:
            w_copy(t, sp, 2, 1, sp=beside).start()

    def w_aside(first, end):
        def w_over(k, carry):
            w_done(w_recv.at[k + 1], 1)
            for t in others:
                w_copy(t, lax.rem(sp + n_sp - 2 * k, n_sp), 2, 1, sp=beside).start()
            return carry

        lax.fori_loop(first, end, w_over, 0)

    with scope("near"):
        lax.fori_loop(chunks // 2, chunks, near, 0)

    rw = ret * RK
    p_row = lax.broadcasted_iota(jnp.int32, (rw, rw), 0)
    p_col = lax.broadcasted_iota(jnp.int32, (rw, rw), 1)
    first_half = lax.rem(p_col, RK) < RK // 2
    swap = jnp.where(
        first_half & (p_row == p_col + RK // 2), -1.0,
        jnp.where(jnp.logical_not(first_half) & (p_row == p_col - RK // 2), 1.0, 0.0),
    ).astype(BF16)
    ones = jnp.ones((HD, MIX + 2 * WINDOW), BF16)

    def attend(i):
        here = rows_of(i, MIX)
        span = pl.ds(pl.multiple_of(i * MIX, MIX), MIX + 2 * WINDOW)
        edge = lax.select((sp == 0) & (i == 0), 1, lax.select((sp == n_sp - 1) & (i == mixes - 1), 2, 0))
        block = bias[edge]
        block = jnp.concatenate([block] * groups, axis=1)
        done = []
        for g in range(kv):
            if paired:
                spots = [(j * kv + g) * 2 * HD for j in range(groups)]
                query = jnp.concatenate([qs[here, at:at + 2 * HD] for at in spots], axis=0)
                key = kbuf[span, :]
            else:
                spots = [(g * groups + j) * HD for j in range(groups)]
                query = jnp.concatenate([qs[here, at:at + HD] for at in spots], axis=0)
                key = kbuf[span, g * HD:(g + 1) * HD]
            value = jnp.concatenate([vt[g * HD:(g + 1) * HD, span], ones], axis=0)
            scores = mm_t(key, query) + block
            sink_row = jnp.concatenate(
                [jnp.broadcast_to(sink[0:1, g * groups + j:g * groups + j + 1], (1, MIX)) for j in range(groups)],
                axis=1)
            top = jnp.maximum(jnp.max(scores, axis=0, keepdims=True), sink_row)
            result = mm(value, jnp.exp(scores - top).astype(BF16))
            scale = 1.0 / (result[HD:HD + 1, :] + jnp.exp(sink_row - top))
            done.append(result[0:HD, :] * scale)
        both = jnp.concatenate(done, axis=0) if kv > 1 else done[0]
        turned = [jnp.transpose(both[:, j * MIX:(j + 1) * MIX]).astype(BF16) for j in range(groups)]
        if kv * HD % 128 == 0:
            for j in range(groups):
                mx[tp, here, j * kv * HD:(j + 1) * kv * HD] = turned[j]
        else:
            mx[tp, here, 0:att_w] = jnp.concatenate(turned, axis=1)
        atd.start(i)

    left, right = sp - 1, sp + 1

    def halo(side, i, where):
        def part(at):
            return kbuf.at[pl.ds(at, WINDOW), :] if i == 0 else vt.at[:, pl.ds(at, WINDOW)]

        src, dst = ((rows, 0), (WINDOW, rows + WINDOW))[side]
        return remote(part(src), part(dst), halo_send.at[side], halo_recv.at[side], sp=where)

    def chunk(c, last, between):
        here = rows_of(c, CHUNK)
        with scope("x1"):
            tok.relay(c)
        between()
        with scope("x2"):
            arrived(gath.at[0:n_chips - 1, here, :], tok_settled.at[c])
        ctx = scope("phaseA")
        ctx.__enter__()
        squares = sqs[here, :]
        far = [(k - 1, lax.rem(chip + k, n_chips)) for k in range(1, n_chips)]
        for at, which in far:
            squares = squares + normed(c, which, at)
        inv_rms = lax.rsqrt(squares / width + NORM_EPS)
        found = {}

        def finish(first):
            for part, (b, off, cols, names) in zip(parts, cfg["dots"]):
                if (names[0][0] in ("rq", "rk", "rv")) != first:
                    continue
                total = part[here, :]
                for at, which in far:
                    total = total + product(which, at, b, off, cols)
                block = (total * inv_rms).astype(BF16)
                at = 0
                for name, count in names:
                    found[name] = block[:, at:at + count]
                    at += count

        finish(True)
        spot = sp * chunks + c
        oc, os_ = outer_cos[pl.ds(spot, 1), :], outer_sin[pl.ds(spot, 1), :]
        ic, is_ = inner_cos[...], inner_sin[...]
        cosine = oc * ic - os_ * is_
        sine = os_ * ic + oc * is_
        query_rot = found["rq"].astype(F32) * cosine + mm(found["rq"], swap) * sine
        key_rot = (found["rk"].astype(F32) * cosine + mm(found["rk"], swap) * sine) * RK ** -0.5

        def doubled(x):
            if ret == 2:
                turned = pltpu.roll(x, RK, 1)
                return jnp.where(low, x, turned), jnp.where(low, turned, x)
            return [jnp.concatenate([x[:, h * RK:(h + 1) * RK]] * 2, axis=1) for h in range(ret)]

        keys = doubled(key_rot)
        for h in range(ret):
            both = (keys[h] * kfac[h, here, :]).astype(BF16)
            terms = tm_m(both, found["rv"][:, h * RV:(h + 1) * RV])
            fterm[h, c] = terms[:RK]
            bterm[h, c] = terms[RK:]
        ctx.__exit__(None, None, None)
        if last:
            with scope("totals"):
                send_totals()
        ctx = scope("phaseB")
        ctx.__enter__()
        finish(False)
        scaled = found["q"] * jnp.asarray(HD ** -0.5, BF16)
        if paired:
            wide = scaled.astype(F32)
            head = [wide[:, at:at + 2 * HD] for at in range(0, att_w, 2 * HD)]
            turned = [pltpu.roll(x, HD, 1) for x in head]
            for j in range(groups):
                for g in range(kv):
                    at = (g * groups + j) * HD
                    x = (head if at % (2 * HD) == g * HD else turned)[at // (2 * HD)]
                    keep = low if g == 0 else jnp.logical_not(low)
                    to = (j * kv + g) * 2 * HD
                    qs[here, to:to + 2 * HD] = jnp.where(keep, x, 0.0).astype(BF16)
        else:
            qs[here, :] = scaled
        shifted = pl.ds(pl.multiple_of(c * CHUNK + WINDOW, 128), CHUNK)
        kbuf[shifted, :] = found["k"]
        vt[:, shifted] = jnp.transpose(found["v"].astype(F32)).astype(BF16)
        gs[here, :] = found["g"]
        queries = doubled(query_rot)
        key_bf = key_rot.astype(BF16)
        for h in range(ret):
            if ret == 2:
                keep = low if h == 0 else jnp.logical_not(low)
                inner = mm_t(jnp.where(keep, query_rot, 0.0).astype(BF16), key_bf)
            else:
                inner = mm_t(query_rot[:, h * RK:(h + 1) * RK].astype(BF16), key_bf[:, h * RK:(h + 1) * RK])
            rloc[h, here, :] = mm((inner * dm[h, c]).astype(BF16), found["rv"][:, h * RV:(h + 1) * RV])
            qfb[h, here, :] = (queries[h] * qfac[h, here, :]).astype(BF16)
        ctx.__exit__(None, None, None)

    def send_totals():
        for h in range(ret):
            state = jnp.zeros((RK, RV), F32)
            back = jnp.zeros((RK, RV), F32)
            for c in range(chunks):
                state = jnp.exp(blog[h, c, 0:1, :]) * state + fterm[h, c]
                back = jnp.exp(blog[h, chunks - 1 - c, 0:1, :]) * back + bterm[h, chunks - 1 - c]
            tot_f[h] = state.astype(BF16)
            tot_b[h] = back.astype(BF16)

            def send_f(i, carry):
                remote(tot_f.at[h], tots.at[sp, h], tot_send, tot_recv.at[h], sp=n_sp - 1 - i).start()
                return carry

            def send_b(d, carry):
                remote(tot_b.at[h], tots.at[sp, h], tot_send, tot_recv.at[h], sp=d).start()
                return carry

            lax.fori_loop(0, n_sp - 1 - sp, send_f, 0)
            lax.fori_loop(0, sp, send_b, 0)

    early = per * (chunks - 3) + 1

    def block_of(j):
        turn = early - per + 1
        return lax.select(j < turn, j, lax.select(j == turn, mixes - 1, j - 1))

    def halo_wait(side):
        arrived(kbuf.at[0:2 * WINDOW, :], halo_recv.at[side])

    def one(j):
        with scope("attend"):
            attend(j)

    def chunk_body(i, carry):
        c = order(i)

        if chunks > 4:
            @pl.when(i > 2)
            def _():
                one(per * (i - 3) + 1)

        def between():
            @pl.when(i == chunks - 2)
            def _():
                with scope("aside"):
                    w_aside(chunks - 1, half_sp)

            @pl.when((i == 2) & (sp > 0))
            def _():
                with scope("halo0"):
                    halo_wait(0)

            @pl.when(i == 2)
            def _():
                one(0)

            if chunks > 4:
                @pl.when(i > 2)
                def _():
                    one(per * (i - 3) + 2)

        chunk(c, False, between)

        @pl.when((i == 0) & (sp < n_sp - 1))
        def _():
            for b in range(2):
                halo(0, b, right).start()

        @pl.when((i == 1) & (sp > 0))
        def _():
            for b in range(2):
                halo(1, b, left).start()

        @pl.when(i < min(chunks - 2, half_sp - 1))
        def _():
            with scope("aside"):
                w_aside(i + 1, i + 2)

        return carry

    lax.fori_loop(0, chunks - 1, chunk_body, 0)

    one(early - per)

    @pl.when(sp < n_sp - 1)
    def _():
        with scope("halo1"):
            halo_wait(1)

    one(mixes - 1)
    chunk(chunks - 2, True, lambda: one(early - per + 1))

    def late(j, carry):
        with scope("late"):
            attend(j)
        with scope("lrelay"):
            atd.relay(block_of(j - early))
        return carry

    lax.fori_loop(early, mixes - 1, late, 0)

    def states_of(h):
        arrived(tots.at[0:n_sp - 1, 0], tot_recv.at[h])

        def from_low(e, state):
            return jnp.exp(logs[e, h, 0:1, :]) * state + tots[e, h].astype(F32)

        def from_high(i, back):
            e = n_sp - 1 - i
            return jnp.exp(logs[e, h, 0:1, :]) * back + tots[e, h].astype(F32)

        state = lax.fori_loop(0, sp, from_low, states[0, h])
        back = lax.fori_loop(0, n_sp - 1 - sp, from_high, states[1, h])
        for c in range(chunks):
            both_in[h, c, 0:RK] = state.astype(BF16)
            state = jnp.exp(blog[h, c, 0:1, :]) * state + fterm[h, c]
            r = chunks - 1 - c
            both_in[h, r, RK:2 * RK] = back.astype(BF16)
            back = jnp.exp(blog[h, r, 0:1, :]) * back + bterm[h, r]

    def retain(c, h):
        here = rows_of(c, MIX)
        combined = rloc[h, here, :] + mm(qfb[h, here, :], both_in[h, lax.div(c, per)])
        centered = combined - jnp.mean(combined, axis=1, keepdims=True)
        normed_ret = centered * lax.rsqrt(jnp.mean(centered * centered, axis=1, keepdims=True) + NORM_EPS)
        gate = gs[here, h * RV:(h + 1) * RV].astype(F32)
        mx[tp, here, att_w + h * RV:att_w + (h + 1) * RV] = (gate / (1.0 + jnp.exp(-gate)) * normed_ret).astype(BF16)
        rtd[h].start(c)

    arrived(logs.at[0:n_sp - 1], log_recv)
    for h in range(ret):
        with scope("states"):
            states_of(h)

        def ret_body(c, carry):
            retain(c, h)
            return carry

        with scope("retain"):
            lax.fori_loop(0, mixes, ret_body, 0)

    def att_rest(j, carry):
        atd.relay(block_of(j))
        return carry

    with scope("attrest"):
        lax.fori_loop(mixes - 1 - early, mixes, att_rest, 0)

    with scope("wsettle"):
        arrived(wg.at[0], pw_recv)
        w_done(w_recv.at[1], half_sp)

    def mix_most(c):
        here = rows_of(c, MIX)
        with scope("bsettle"):
            arrived(mx.at[0:n_chips, here, 0:most], most_settled.at[c])
        with scope("base"):
            total = mm(mx[0, here, 0:most], wg[0, 0:most, :])
            for t in range(1, n_tp):
                total = total + mm(mx[t, here, 0:most], wg[t, 0:most, :])
            base[here, :] = total

    def mix_last(c):
        here = rows_of(c, MIX)
        with scope("msettle"):
            arrived(mx.at[0:n_chips, here, most:most + RV], last_settled.at[c])
        with scope("mix"):
            total = base[here, :]
            for t in range(n_tp):
                total = total + mm(mx[t, here, most:], wg[t, most:, :])
            out[here, :] = total.astype(BF16)

    lag = 2

    def first_heads(c, carry):
        with scope("hrelay"):
            for h in range(ret - 1):
                rtd[h].relay(c)

        @pl.when(c >= lag)
        def _():
            mix_most(c - lag)

        return carry

    def last_head(c, carry):
        with scope("rrelay"):
            rtd[ret - 1].relay(c)

        @pl.when(c < lag)
        def _():
            mix_most(mixes - lag + c)

        @pl.when(c >= lag)
        def _():
            mix_last(c - lag)

        return carry

    def ending(c, carry):
        mix_last(c)
        return carry

    lax.fori_loop(0, mixes, first_heads, 0)
    lax.fori_loop(0, mixes, last_head, 0)
    lax.fori_loop(mixes - lag, mixes, ending, 0)

    with scope("drain"):
        sent = 2 * n_chips - 1
        arrived(gath.at[0:sent], tok_send)
        arrived(mx.at[0:sent], mix_send)
        arrived(wg.at[0], pw_send)
        w_done(w_send.at[0], 1)
        w_done(w_send.at[1], half_sp - 1)
        w_done(w_send.at[2], half_sp)
        arrived(logs.at[0:n_sp - 1], log_send)
        arrived(tots.at[0:n_sp - 1], tot_send)

        @pl.when(sp < n_sp - 1)
        def _():
            arrived(kbuf.at[0:2 * WINDOW, :], halo_send.at[0])

        @pl.when(sp > 0)
        def _():
            arrived(kbuf.at[0:2 * WINDOW, :], halo_send.at[1])


def body(n_sp, n_tp, tokens, norm_gain, w_q, w_k, w_v, w_rq, w_rk, w_rv, w_rg, att_sink,
         decay_log, init_state, out_att, out_ret):
    rows, chan = tokens.shape
    width = n_tp * chan
    ret = decay_log.shape[0]
    heads = att_sink.shape[0]
    kv_cols = w_k.shape[1]
    kv = kv_cols // HD
    chunks = rows // CHUNK
    n_chips = n_tp // 2
    weights = (w_q, w_k, w_v, w_rq, w_rk, w_rv, w_rg)
    names = ("q", "k", "v", "rq", "rk", "rv", "g")
    cols = [w.shape[1] for w in weights]
    joined = all(count % 128 == 0 for count in cols)
    places, dots = [], []
    if joined:
        buffers = [sum(cols)]
        at = 0
        for count in cols:
            places.append((0, at, count))
            at += count
        for group in ((3, 4), (5,), (1, 2), (0,), (6,)):
            dots.append((0, places[group[0]][1], sum(cols[i] for i in group),
                         tuple((names[i], cols[i]) for i in group)))
    else:
        buffers = cols
        for i, count in enumerate(cols):
            places.append((i, 0, count))
            dots.append((i, 0, count, ((names[i], count),)))
    att_w, ret_w = heads * HD, ret * RV
    paired = kv == 2 and 2 * HD == 128
    assert kv == 1 or HD % ((att_w + ret_w) // n_sp) == 0
    cfg = dict(paired=paired, n_sp=n_sp, n_tp=n_tp, n_chips=n_chips, chunks=chunks, chan=chan, heads=heads,
               ret=ret, kv=kv, buffers=buffers, places=places, dots=dots, joined=joined)
    tables = rope_tables(n_sp * chunks, CHUNK, ret) + rope_tables(CHUNK, 1, ret)
    small = [norm_gain.reshape(1, width), att_sink.reshape(1, heads), decay_log]
    small += [jnp.asarray(t) for t in tables]
    anyw = pl.BlockSpec(memory_space=pl.ANY)
    dma = pltpu.SemaphoreType.DMA
    mixes = rows // MIX
    scratch = [pltpu.VMEM((width, count), BF16) for count in buffers] + [
        pltpu.VMEM(a.shape, F32) for a in small] + [
        pltpu.VMEM((rows, group[2]), F32) for group in dots] + [
        pltpu.VMEM((n_tp, att_w + ret_w, chan), BF16),
        pltpu.VMEM((n_tp, rows, chan), BF16),
        pltpu.VMEM((max(n_chips - 1, 1), CHUNK, 2 * chan), BF16),
        pltpu.VMEM((rows, att_w * (2 if paired else 1)), BF16),
        pltpu.VMEM((rows + 2 * WINDOW, kv_cols), BF16),
        pltpu.VMEM((kv_cols, rows + 2 * WINDOW), BF16),
        pltpu.VMEM((n_tp, rows, att_w + ret_w), BF16),
        pltpu.VMEM((ret, rows, 2 * RK), BF16),
        pltpu.VMEM((ret, rows, RV), F32),
        pltpu.VMEM((rows, ret_w), BF16),
        pltpu.VMEM((ret, chunks, RK, RV), F32),
        pltpu.VMEM((ret, chunks, RK, RV), F32),
        pltpu.VMEM((ret, chunks, 8, 128), F32),
        pltpu.VMEM((ret, chunks, 2 * RK, RV), BF16),
        pltpu.VMEM((rows, 1), F32),
        pltpu.VMEM((ret, chunks, CHUNK, CHUNK), F32),
        pltpu.VMEM((ret, rows, 2 * RK), F32),
        pltpu.VMEM((ret, rows, 2 * RK), F32),
        pltpu.VMEM((3, MIX + 2 * WINDOW, MIX), F32),
        pltpu.VMEM((rows, chan), F32),
        pltpu.VMEM((ret, RK, RV), BF16),
        pltpu.VMEM((ret, RK, RV), BF16),
        pltpu.VMEM((n_sp, ret, RK, RV), BF16),
        pltpu.VMEM((n_sp, ret, 8, 128), F32),
        pltpu.VMEM((2, ret, RK, RV), F32),
        pltpu.SemaphoreType.REGULAR,
        dma((len(buffers),)), dma, dma, dma((len(small) + 1,)),
        dma, dma((n_chips - 1, chunks)), dma((chunks,)), dma((chunks,)),
        dma, dma((n_chips - 1, mixes)), dma((ret, n_chips - 1, mixes)), dma((mixes,)), dma((mixes,)),
        dma, dma, dma((3,)), dma((n_sp // 2 + 1,)),
        dma((2,)), dma((2,)),
        dma, dma((ret,)), dma, dma,
    ]
    return pl.pallas_call(
        functools.partial(kernel, cfg),
        out_shape=pltpu.VMEM((rows, chan), BF16),
        in_specs=[anyw] * (11 + len(small)),
        out_specs=pl.BlockSpec(memory_space=pltpu.VMEM),
        scratch_shapes=scratch,
        compiler_params=pltpu.CompilerParams(
            collective_id=0, has_side_effects=True, vmem_limit_bytes=60 * 1024 * 1024),
    )(tokens, *weights, init_state, out_att, out_ret, *small)


def solution(mesh):
    n_sp, n_tp = mesh.shape["sp"], mesh.shape["tp"]
    in_specs = (
        P("sp", "tp"),
        P(),
        P(None, "tp"),
        P(None, "tp"),
        P(None, "tp"),
        P(None, "tp"),
        P(None, "tp"),
        P(None, "tp"),
        P(None, "tp"),
        P("tp"),
        P("tp", "sp"),
        P(None, "tp", None, None),
        P("tp", None),
        P("tp", None),
    )
    return jax.shard_map(functools.partial(body, n_sp, n_tp), mesh=mesh, in_specs=in_specs,
                         out_specs=P("sp", "tp"), check_vma=False)
```

```python
import contextlib
import functools

import jax
import jax.numpy as jnp
import numpy as np
from jax import lax
from jax.experimental import pallas as pl
from jax.experimental.pallas import tpu as pltpu
from jax.sharding import PartitionSpec as P

HD = 64
RK = 64
RV = 128
WINDOW = 128
CHUNK = 256
MIX = 128
NORM_EPS = 1e-06
ROPE_BASE = 10000.0
F32 = jnp.float32
BF16 = jnp.bfloat16
MESH = pl.DeviceIdType.MESH


def scope(name):
    return contextlib.nullcontext()


def rope_tables(count, step, heads):
    half = RK // 2
    inverse = ROPE_BASE ** (-2.0 * np.arange(half, dtype=np.float64) / RK)
    angles = (np.arange(count, dtype=np.float64) * step)[:, None] * inverse[None, :]
    wide = np.tile(np.concatenate([angles, angles], axis=1), (1, heads))
    return np.cos(wide).astype(np.float32), np.sin(wide).astype(np.float32)


def remote(src, dst, send, recv, **where):
    return pltpu.make_async_remote_copy(
        src_ref=src, dst_ref=dst, send_sem=send, recv_sem=recv,
        device_id=where, device_id_type=MESH,
    )


def rows_of(index, size):
    return pl.ds(pl.multiple_of(index * size, size), size)


def mm(a, b):
    return jnp.dot(a, b, preferred_element_type=F32)


def mm_t(a, b):
    return lax.dot_general(a, b, (((1,), (1,)), ((), ())), preferred_element_type=F32)


def tm_m(a, b):
    return lax.dot_general(a, b, (((0,), (0,)), ((), ())), preferred_element_type=F32)


class Spread:
    def __init__(self, place, buf, columns, size, send, cross, near, settled, src=None):
        self.place, self.buf, self.columns, self.size = place, buf, columns, size
        self.send, self.cross, self.near, self.settled, self.src = send, cross, near, settled, src

    def block(self, slot, c):
        return self.buf.at[slot, rows_of(c, self.size), self.columns]

    def start(self, c):
        tp, partner, across, n_chips = self.place
        src = self.block(tp, c) if self.src is None else self.src.at[rows_of(c, self.size), :]
        for k in range(1, n_chips):
            remote(src, self.block(tp, c), self.send, self.cross.at[n_chips - k - 1, c], tp=across(k)).start()
        remote(src, self.block(tp, c), self.send, self.near.at[c], tp=partner).start()

    def relay(self, c):
        _, partner, across, n_chips = self.place
        for k in range(1, n_chips):
            block = self.block(across(k), c)
            remote(block, block, self.send, self.cross.at[k - 1, c], tp=partner).wait_recv()
            remote(block, block, self.send, self.settled.at[c], tp=partner).start()


def kernel(cfg, *refs):
    n_buf, n_small = len(cfg["buffers"]), 8
    (tokens, w_q, w_k, w_v, w_rq, w_rk, w_rv, w_rg, init, o_att, o_ret) = refs[:11]
    small_hbm = refs[11:11 + n_small - 1]
    out = refs[10 + n_small]
    rest = refs[11 + n_small:]
    w_bufs = rest[:n_buf]
    small = rest[n_buf:n_buf + n_small - 1]
    parts = rest[n_buf + n_small - 1:n_buf + n_small - 1 + len(cfg["dots"])]
    gain, sink, decay, outer_cos, outer_sin, inner_cos, inner_sin = small
    (wg, gath, xbuf, qs, kbuf, vt, mx, qfb, rloc, gs, fterm, bterm, blog, both_in,
     sqs, dm, kfac, qfac, bias, base,
     tot_f, tot_b, tots, logs, states,
     ready, w_sem, wo_sem, tok_sem, small_sem,
     tok_send, tok_cross, tok_near, tok_settled, mix_send, att_cross, ret_cross, most_settled, last_settled,
     pw_send, pw_recv, w_send, w_recv,
     halo_send, halo_recv, tot_send, tot_recv, log_send, log_recv) = rest[n_buf + n_small - 1 + len(parts):]
    n_tp, n_sp, n_chips, chunks = cfg["n_tp"], cfg["n_sp"], cfg["n_chips"], cfg["chunks"]
    chan, heads, ret, kv = cfg["chan"], cfg["heads"], cfg["ret"], cfg["kv"]
    rows = chunks * CHUNK
    width = n_tp * chan
    groups = heads // kv
    seq_len = rows * n_sp
    att_w, ret_w = heads * HD, ret * RV
    piece = (att_w + ret_w) // n_sp
    per = CHUNK // MIX
    mixes = rows // MIX
    sp = lax.axis_index("sp")
    tp = lax.axis_index("tp")
    core = lax.rem(tp, 2)
    chip = lax.div(tp, 2)
    partner = chip * 2 + 1 - core

    def across(k):
        return lax.rem(chip + k, n_chips) * 2 + core

    place = (tp, partner, across, n_chips)
    tok = Spread(place, gath, slice(None), CHUNK, tok_send, tok_cross, tok_near, tok_settled, src=tokens)
    atd = Spread(place, mx, pl.ds(0, att_w), MIX, mix_send, att_cross, most_settled, most_settled)
    most = att_w + ret_w - RV
    rtd = []
    for h in range(ret):
        settled = most_settled if h < ret - 1 else last_settled
        rtd.append(Spread(place, mx, pl.ds(att_w + h * RV, RV), MIX, mix_send, ret_cross.at[h], settled, settled))

    def arrived(ref, sem):
        pltpu.make_async_copy(ref, ref, sem).wait()

    barrier = pltpu.get_barrier_semaphore()
    for k in range(1, n_tp):
        pl.semaphore_signal(barrier, inc=1, device_id={"tp": lax.rem(tp + k, n_tp)}, device_id_type=MESH)

    @pl.when(sp == 0)
    def _():
        for k in range(1, n_sp):
            pl.semaphore_signal(barrier, inc=1, device_id={"sp": k}, device_id_type=MESH)

    token_copy = pltpu.make_async_copy(tokens, gath.at[tp], tok_sem)
    token_copy.start()
    local = [pltpu.make_async_copy(a, b, small_sem.at[i]) for i, (a, b) in enumerate(zip(small_hbm, small))]
    local.append(pltpu.make_async_copy(init, states, small_sem.at[n_small - 1]))
    weights = (w_q, w_k, w_v, w_rq, w_rk, w_rv, w_rg)
    for w_ref, (b, off, cols) in zip(weights, cfg["places"]):
        dst = w_bufs[b].at[:, pl.ds(off, cols)] if cfg["joined"] else w_bufs[b]
        pltpu.make_async_copy(w_ref, dst, w_sem.at[b]).start()
    paired = cfg["paired"]

    def att_row(row):
        if kv == 1:
            return row
        spot, within = row // HD, row % HD
        return (spot % kv * groups + spot // kv) * HD + within

    runs = [(o_att, att_row(b * HD), b * HD, HD) for b in range(heads)]
    runs.append((o_ret, 0, att_w, ret_w))

    def columns(t):
        return pl.ds(pl.multiple_of(t * chan, chan), chan)

    for src, row, first, count in runs:
        pltpu.make_async_copy(src.at[pl.ds(row, count), columns(tp)], wg.at[tp, pl.ds(first, count), :], wo_sem).start()
    for copy in local:
        copy.start()

    with scope("barrier"):
        @pl.when(sp == 0)
        def _():
            pl.semaphore_wait(barrier, n_tp - 1)

        @pl.when(sp > 0)
        def _():
            pl.semaphore_wait(barrier, n_tp)
            pl.semaphore_signal(ready, inc=1, device_id={"sp": 0}, device_id_type=MESH)

    others = [lax.rem(chip + k, n_chips) * 2 + p for k in range(1, n_chips) for p in range(2)]

    def w_copy(t, e, send, recv, **where):
        block = wg.at[t, rows_of(e, piece), :]
        return remote(block, block, w_send.at[send], w_recv.at[recv], **where)

    def w_done(sem, pieces):
        left, full = pieces * len(others) * piece, att_w + ret_w
        while left > 0:
            arrived(wg.at[0, 0:min(left, full), :], sem)
            left -= full

    def w_first(src, row):
        for t in others:
            remote(src.at[pl.ds(pl.multiple_of(row, piece), piece), columns(t)], wg.at[tp, rows_of(sp, piece), :],
                   w_send.at[0], w_recv.at[0], tp=t).start()

    @pl.when(sp * piece < att_w)
    def _():
        w_first(o_att, att_row(sp * piece))

    @pl.when(sp * piece >= att_w)
    def _():
        w_first(o_ret, sp * piece - att_w)

    def order(i):
        return lax.rem(i + chunks - 1, chunks)

    def first_sends(i, carry):
        tok.start(order(i))
        return carry

    lax.fori_loop(0, chunks, first_sends, 0)

    for src, row, first, count in runs:
        remote(src.at[pl.ds(row, count), columns(partner)], wg.at[tp, pl.ds(first, count), :],
               pw_send, pw_recv, tp=partner).start()

    with scope("lwait"):
        for copy in local:
            copy.wait()
        token_copy.wait()
        for i, buf in enumerate(w_bufs):
            arrived(buf, w_sem.at[i])
        arrived(wg.at[tp], wo_sem)

    for h in range(ret):
        total = jnp.sum(decay[h:h + 1, :], axis=1, keepdims=True)
        logs[sp, h] = jnp.broadcast_to(total, (8, 128))

    @pl.when(sp == 0)
    def _():
        kbuf[0:WINDOW, :] = jnp.zeros((WINDOW, kbuf.shape[1]), BF16)
        vt[:, 0:WINDOW] = jnp.zeros((vt.shape[0], WINDOW), BF16)

    @pl.when(sp == n_sp - 1)
    def _():
        kbuf[rows + WINDOW:, :] = jnp.zeros((WINDOW, kbuf.shape[1]), BF16)
        vt[:, rows + WINDOW:] = jnp.zeros((vt.shape[0], WINDOW), BF16)

    row_i = lax.broadcasted_iota(jnp.int32, (CHUNK, CHUNK), 0)
    col_i = lax.broadcasted_iota(jnp.int32, (CHUNK, CHUNK), 1)
    low = lax.broadcasted_iota(jnp.int32, (CHUNK, 2 * RK), 1) < RK

    def decays(c, carry):
        here = rows_of(c, CHUNK)
        for h in range(ret):
            log_row = decay[h:h + 1, here]
            wide = jnp.broadcast_to(log_row, (CHUNK, CHUNK))
            log_col = jnp.sum(jnp.where(row_i == col_i, wide, 0.0), axis=1, keepdims=True)
            cum_col = jnp.sum(jnp.where(col_i <= row_i, wide, 0.0), axis=1, keepdims=True)
            cum_row = jnp.sum(jnp.where(row_i <= col_i, log_col, 0.0), axis=0, keepdims=True)
            total = jnp.sum(log_row, axis=1, keepdims=True)
            dm[h, c] = jnp.exp(-jnp.abs(cum_col - cum_row))
            up = jnp.exp(cum_col)
            down = jnp.exp(jnp.minimum(total - cum_col, 0.0))
            kfac[h, here, :] = jnp.where(low, down, up)
            qfac[h, here, :] = jnp.where(low, up, down)
            blog[h, c] = jnp.broadcast_to(total, (8, 128))
        return carry

    with scope("decays"):
        lax.fori_loop(0, chunks, decays, 0)

    shape = (MIX + 2 * WINDOW, MIX)
    q_i = lax.broadcasted_iota(jnp.int32, shape, 1)
    k_i = lax.broadcasted_iota(jnp.int32, shape, 0)
    band = (k_i >= q_i) & (k_i <= q_i + 2 * WINDOW)
    bias[0] = jnp.where(band, 0.0, -jnp.inf)
    bias[1] = jnp.where(band & (k_i >= WINDOW), 0.0, -jnp.inf)
    bias[2] = jnp.where(band & (k_i < MIX + WINDOW), 0.0, -jnp.inf)

    def normed(c, which, dst):
        here = rows_of(c, CHUNK)
        squares = jnp.zeros((CHUNK, 1), F32)
        for p in range(2):
            slot = which * 2 + p
            x = gath[slot, here, :].astype(F32)
            squares = squares + jnp.sum(x * x, axis=1, keepdims=True)
            xbuf[dst, :, p * chan:(p + 1) * chan] = (x * gain[0:1, columns(slot)]).astype(BF16)
        return squares

    def product(which, src, b, off, cols):
        span = pl.ds(pl.multiple_of(which * (2 * chan), 2 * chan), 2 * chan)
        return mm(xbuf[src], w_bufs[b][span, off:off + cols])

    def near(i, carry):
        c = order(i)
        here = rows_of(c, CHUNK)
        arrived(gath.at[0, here, :], tok_near.at[c])
        sqs[here, :] = normed(c, chip, 0)
        for part, (b, off, cols, _) in zip(parts, cfg["dots"]):
            part[here, :] = product(chip, 0, b, off, cols)
        return carry

    with scope("near"):
        lax.fori_loop(0, chunks // 2, near, 0)

    with scope("ready"):
        @pl.when(sp == 0)
        def _():
            pl.semaphore_wait(ready, n_sp - 1)
            for k in range(1, n_sp):
                pl.semaphore_signal(ready, inc=1, device_id={"sp": k}, device_id_type=MESH)

        @pl.when(sp > 0)
        def _():
            pl.semaphore_wait(ready, 1)

    for k in range(1, n_sp):
        remote(logs.at[sp], logs.at[sp], log_send, log_recv, sp=lax.rem(sp + k, n_sp)).start()

    beside = sp + 1 - 2 * lax.rem(sp, 2)
    half_sp = n_sp // 2
    with scope("wfwd"):
        w_done(w_recv.at[0], 1)

        def w_pass(k, carry):
            for t in others:
                w_copy(t, sp, 1, k + 1, sp=lax.rem(sp + 2 * k, n_sp)).start()
            return carry

        lax.fori_loop(1, half_sp, w_pass, 0)
        for t in others:
            w_copy(t, sp, 2, 1, sp=beside).start()

    def w_aside(first, end):
        def w_over(k, carry):
            w_done(w_recv.at[k + 1], 1)
            for t in others:
                w_copy(t, lax.rem(sp + n_sp - 2 * k, n_sp), 2, 1, sp=beside).start()
            return carry

        lax.fori_loop(first, end, w_over, 0)

    with scope("near"):
        lax.fori_loop(chunks // 2, chunks, near, 0)

    rw = ret * RK
    p_row = lax.broadcasted_iota(jnp.int32, (rw, rw), 0)
    p_col = lax.broadcasted_iota(jnp.int32, (rw, rw), 1)
    first_half = lax.rem(p_col, RK) < RK // 2
    swap = jnp.where(
        first_half & (p_row == p_col + RK // 2), -1.0,
        jnp.where(jnp.logical_not(first_half) & (p_row == p_col - RK // 2), 1.0, 0.0),
    ).astype(BF16)
    ones = jnp.ones((HD, MIX + 2 * WINDOW), BF16)

    def attend(i):
        here = rows_of(i, MIX)
        span = pl.ds(pl.multiple_of(i * MIX, MIX), MIX + 2 * WINDOW)
        edge = lax.select((sp == 0) & (i == 0), 1, lax.select((sp == n_sp - 1) & (i == mixes - 1), 2, 0))
        block = bias[edge]
        block = jnp.concatenate([block] * groups, axis=1)
        done = []
        for g in range(kv):
            if paired:
                spots = [(j * kv + g) * 2 * HD for j in range(groups)]
                query = jnp.concatenate([qs[here, at:at + 2 * HD] for at in spots], axis=0)
                key = kbuf[span, :]
            else:
                spots = [(g * groups + j) * HD for j in range(groups)]
                query = jnp.concatenate([qs[here, at:at + HD] for at in spots], axis=0)
                key = kbuf[span, g * HD:(g + 1) * HD]
            value = jnp.concatenate([vt[g * HD:(g + 1) * HD, span], ones], axis=0)
            scores = mm_t(key, query) + block
            sink_row = jnp.concatenate(
                [jnp.broadcast_to(sink[0:1, g * groups + j:g * groups + j + 1], (1, MIX)) for j in range(groups)],
                axis=1)
            top = jnp.maximum(jnp.max(scores, axis=0, keepdims=True), sink_row)
            result = mm(value, jnp.exp(scores - top).astype(BF16))
            scale = 1.0 / (result[HD:HD + 1, :] + jnp.exp(sink_row - top))
            done.append(result[0:HD, :] * scale)
        both = jnp.concatenate(done, axis=0) if kv > 1 else done[0]
        turned = [jnp.transpose(both[:, j * MIX:(j + 1) * MIX]).astype(BF16) for j in range(groups)]
        if kv * HD % 128 == 0:
            for j in range(groups):
                mx[tp, here, j * kv * HD:(j + 1) * kv * HD] = turned[j]
        else:
            mx[tp, here, 0:att_w] = jnp.concatenate(turned, axis=1)
        atd.start(i)

    left, right = sp - 1, sp + 1

    def halo(side, i, where):
        def part(at):
            return kbuf.at[pl.ds(at, WINDOW), :] if i == 0 else vt.at[:, pl.ds(at, WINDOW)]

        src, dst = ((rows, 0), (WINDOW, rows + WINDOW))[side]
        return remote(part(src), part(dst), halo_send.at[side], halo_recv.at[side], sp=where)

    def chunk(c, last, between, while_waiting=None):
        here = rows_of(c, CHUNK)
        with scope("x1"):
            tok.relay(c)
        between()
        with scope("x2"):
            arrived(gath.at[0:n_chips - 1, here, :], tok_settled.at[c])
        ctx = scope("phaseA")
        ctx.__enter__()
        squares = sqs[here, :]
        far = [(k - 1, lax.rem(chip + k, n_chips)) for k in range(1, n_chips)]
        for at, which in far:
            squares = squares + normed(c, which, at)
        inv_rms = lax.rsqrt(squares / width + NORM_EPS)
        found = {}

        def finish(*wanted):
            for part, (b, off, cols, names) in zip(parts, cfg["dots"]):
                if names[0][0] not in wanted:
                    continue
                total = part[here, :]
                for at, which in far:
                    total = total + product(which, at, b, off, cols)
                block = (total * inv_rms).astype(BF16)
                at = 0
                for name, count in names:
                    found[name] = block[:, at:at + count]
                    at += count

        finish("rq", "rk", "rv")
        spot = sp * chunks + c
        oc, os_ = outer_cos[pl.ds(spot, 1), :], outer_sin[pl.ds(spot, 1), :]
        ic, is_ = inner_cos[...], inner_sin[...]
        cosine = oc * ic - os_ * is_
        sine = os_ * ic + oc * is_
        query_rot = found["rq"].astype(F32) * cosine + mm(found["rq"], swap) * sine
        key_rot = (found["rk"].astype(F32) * cosine + mm(found["rk"], swap) * sine) * RK ** -0.5

        def doubled(x):
            if ret == 2:
                turned = pltpu.roll(x, RK, 1)
                return jnp.where(low, x, turned), jnp.where(low, turned, x)
            return [jnp.concatenate([x[:, h * RK:(h + 1) * RK]] * 2, axis=1) for h in range(ret)]

        keys = doubled(key_rot)
        for h in range(ret):
            both = (keys[h] * kfac[h, here, :]).astype(BF16)
            terms = tm_m(both, found["rv"][:, h * RV:(h + 1) * RV])
            fterm[h, c] = terms[:RK]
            bterm[h, c] = terms[RK:]
        ctx.__exit__(None, None, None)
        if last:
            with scope("totals"):
                send_totals()
        ctx = scope("phaseB")
        ctx.__enter__()
        finish("q", "k", "v")
        scaled = found["q"] * jnp.asarray(HD ** -0.5, BF16)
        if paired:
            wide = scaled.astype(F32)
            head = [wide[:, at:at + 2 * HD] for at in range(0, att_w, 2 * HD)]
            turned = [pltpu.roll(x, HD, 1) for x in head]
            for j in range(groups):
                for g in range(kv):
                    at = (g * groups + j) * HD
                    x = (head if at % (2 * HD) == g * HD else turned)[at // (2 * HD)]
                    keep = low if g == 0 else jnp.logical_not(low)
                    to = (j * kv + g) * 2 * HD
                    qs[here, to:to + 2 * HD] = jnp.where(keep, x, 0.0).astype(BF16)
        else:
            qs[here, :] = scaled
        shifted = pl.ds(pl.multiple_of(c * CHUNK + WINDOW, 128), CHUNK)
        kbuf[shifted, :] = found["k"]
        vt[:, shifted] = jnp.transpose(found["v"].astype(F32)).astype(BF16)
        ctx.__exit__(None, None, None)
        if last:
            while_waiting()
        ctx = scope("phaseC")
        ctx.__enter__()
        finish("g")
        gs[here, :] = found["g"]
        queries = doubled(query_rot)
        key_bf = key_rot.astype(BF16)
        for h in range(ret):
            if ret == 2:
                keep = low if h == 0 else jnp.logical_not(low)
                inner = mm_t(jnp.where(keep, query_rot, 0.0).astype(BF16), key_bf)
            else:
                inner = mm_t(query_rot[:, h * RK:(h + 1) * RK].astype(BF16), key_bf[:, h * RK:(h + 1) * RK])
            rloc[h, here, :] = mm((inner * dm[h, c]).astype(BF16), found["rv"][:, h * RV:(h + 1) * RV])
            qfb[h, here, :] = (queries[h] * qfac[h, here, :]).astype(BF16)
        ctx.__exit__(None, None, None)

    def send_totals():
        for h in range(ret):
            state = jnp.zeros((RK, RV), F32)
            back = jnp.zeros((RK, RV), F32)
            for c in range(chunks):
                state = jnp.exp(blog[h, c, 0:1, :]) * state + fterm[h, c]
                back = jnp.exp(blog[h, chunks - 1 - c, 0:1, :]) * back + bterm[h, chunks - 1 - c]
            tot_f[h] = state.astype(BF16)
            tot_b[h] = back.astype(BF16)

            def send_f(i, carry):
                remote(tot_f.at[h], tots.at[sp, h], tot_send, tot_recv.at[h], sp=n_sp - 1 - i).start()
                return carry

            def send_b(d, carry):
                remote(tot_b.at[h], tots.at[sp, h], tot_send, tot_recv.at[h], sp=d).start()
                return carry

            lax.fori_loop(0, n_sp - 1 - sp, send_f, 0)
            lax.fori_loop(0, sp, send_b, 0)

    early = per * (chunks - 3) + 1

    def block_of(j):
        turn = early - per + 1
        return lax.select(j < turn, j, lax.select(j == turn, mixes - 1, j - 1))

    def halo_wait(side):
        arrived(kbuf.at[0:2 * WINDOW, :], halo_recv.at[side])

    def one(j):
        with scope("attend"):
            attend(j)

    def chunk_body(i, carry):
        c = order(i)

        if chunks > 4:
            @pl.when(i > 2)
            def _():
                one(per * (i - 3) + 1)

        def between():
            @pl.when(i == chunks - 2)
            def _():
                with scope("aside"):
                    w_aside(chunks - 1, half_sp)

            @pl.when((i == 2) & (sp > 0))
            def _():
                with scope("halo0"):
                    halo_wait(0)

            @pl.when(i == 2)
            def _():
                one(0)

            if chunks > 4:
                @pl.when(i > 2)
                def _():
                    one(per * (i - 3) + 2)

        chunk(c, False, between)

        @pl.when((i == 0) & (sp < n_sp - 1))
        def _():
            for b in range(2):
                halo(0, b, right).start()

        @pl.when((i == 1) & (sp > 0))
        def _():
            for b in range(2):
                halo(1, b, left).start()

        @pl.when(i < min(chunks - 2, half_sp - 1))
        def _():
            with scope("aside"):
                w_aside(i + 1, i + 2)

        return carry

    lax.fori_loop(0, chunks - 1, chunk_body, 0)

    one(early - per)

    @pl.when(sp < n_sp - 1)
    def _():
        with scope("halo1"):
            halo_wait(1)

    one(mixes - 1)

    def late(j, carry):
        with scope("late"):
            attend(j)
        with scope("lrelay"):
            atd.relay(block_of(j - early))
        return carry

    chunk(chunks - 2, True, lambda: one(early - per + 1), lambda: lax.fori_loop(early, mixes - 1, late, 0))

    def states_of(h):
        arrived(tots.at[0:n_sp - 1, 0], tot_recv.at[h])

        def from_low(e, state):
            return jnp.exp(logs[e, h, 0:1, :]) * state + tots[e, h].astype(F32)

        def from_high(i, back):
            e = n_sp - 1 - i
            return jnp.exp(logs[e, h, 0:1, :]) * back + tots[e, h].astype(F32)

        state = lax.fori_loop(0, sp, from_low, states[0, h])
        back = lax.fori_loop(0, n_sp - 1 - sp, from_high, states[1, h])
        for c in range(chunks):
            both_in[h, c, 0:RK] = state.astype(BF16)
            state = jnp.exp(blog[h, c, 0:1, :]) * state + fterm[h, c]
            r = chunks - 1 - c
            both_in[h, r, RK:2 * RK] = back.astype(BF16)
            back = jnp.exp(blog[h, r, 0:1, :]) * back + bterm[h, r]

    def retain(c, h):
        here = rows_of(c, MIX)
        combined = rloc[h, here, :] + mm(qfb[h, here, :], both_in[h, lax.div(c, per)])
        centered = combined - jnp.mean(combined, axis=1, keepdims=True)
        normed_ret = centered * lax.rsqrt(jnp.mean(centered * centered, axis=1, keepdims=True) + NORM_EPS)
        gate = gs[here, h * RV:(h + 1) * RV].astype(F32)
        mx[tp, here, att_w + h * RV:att_w + (h + 1) * RV] = (gate / (1.0 + jnp.exp(-gate)) * normed_ret).astype(BF16)
        rtd[h].start(c)

    arrived(logs.at[0:n_sp - 1], log_recv)
    for h in range(ret):
        with scope("states"):
            states_of(h)

        def ret_body(c, carry):
            retain(c, h)
            return carry

        with scope("retain"):
            lax.fori_loop(0, mixes, ret_body, 0)

    def att_rest(j, carry):
        atd.relay(block_of(j))
        return carry

    with scope("attrest"):
        lax.fori_loop(mixes - 1 - early, mixes, att_rest, 0)

    with scope("wsettle"):
        arrived(wg.at[0], pw_recv)
        w_done(w_recv.at[1], half_sp)

    def mix_most(c):
        here = rows_of(c, MIX)
        with scope("bsettle"):
            arrived(mx.at[0:n_chips, here, 0:most], most_settled.at[c])
        with scope("base"):
            total = mm(mx[0, here, 0:most], wg[0, 0:most, :])
            for t in range(1, n_tp):
                total = total + mm(mx[t, here, 0:most], wg[t, 0:most, :])
            base[here, :] = total

    def mix_last(c):
        here = rows_of(c, MIX)
        with scope("msettle"):
            arrived(mx.at[0:n_chips, here, most:most + RV], last_settled.at[c])
        with scope("mix"):
            total = base[here, :]
            for t in range(n_tp):
                total = total + mm(mx[t, here, most:], wg[t, most:, :])
            out[here, :] = total.astype(BF16)

    lag = 2

    def first_heads(c, carry):
        with scope("hrelay"):
            for h in range(ret - 1):
                rtd[h].relay(c)

        @pl.when(c >= lag)
        def _():
            mix_most(c - lag)

        return carry

    def last_head(c, carry):
        with scope("rrelay"):
            rtd[ret - 1].relay(c)

        @pl.when(c < lag)
        def _():
            mix_most(mixes - lag + c)

        @pl.when(c >= lag)
        def _():
            mix_last(c - lag)

        return carry

    def ending(c, carry):
        mix_last(c)
        return carry

    lax.fori_loop(0, mixes, first_heads, 0)
    lax.fori_loop(0, mixes, last_head, 0)
    lax.fori_loop(mixes - lag, mixes, ending, 0)

    with scope("drain"):
        sent = 2 * n_chips - 1
        arrived(gath.at[0:sent], tok_send)
        arrived(mx.at[0:sent], mix_send)
        arrived(wg.at[0], pw_send)
        w_done(w_send.at[0], 1)
        w_done(w_send.at[1], half_sp - 1)
        w_done(w_send.at[2], half_sp)
        arrived(logs.at[0:n_sp - 1], log_send)
        arrived(tots.at[0:n_sp - 1], tot_send)

        @pl.when(sp < n_sp - 1)
        def _():
            arrived(kbuf.at[0:2 * WINDOW, :], halo_send.at[0])

        @pl.when(sp > 0)
        def _():
            arrived(kbuf.at[0:2 * WINDOW, :], halo_send.at[1])


def body(n_sp, n_tp, tokens, norm_gain, w_q, w_k, w_v, w_rq, w_rk, w_rv, w_rg, att_sink,
         decay_log, init_state, out_att, out_ret):
    rows, chan = tokens.shape
    width = n_tp * chan
    ret = decay_log.shape[0]
    heads = att_sink.shape[0]
    kv_cols = w_k.shape[1]
    kv = kv_cols // HD
    chunks = rows // CHUNK
    n_chips = n_tp // 2
    weights = (w_q, w_k, w_v, w_rq, w_rk, w_rv, w_rg)
    names = ("q", "k", "v", "rq", "rk", "rv", "g")
    cols = [w.shape[1] for w in weights]
    joined = all(count % 128 == 0 for count in cols)
    places, dots = [], []
    if joined:
        buffers = [sum(cols)]
        at = 0
        for count in cols:
            places.append((0, at, count))
            at += count
        for group in ((3, 4), (5,), (1, 2), (0,), (6,)):
            dots.append((0, places[group[0]][1], sum(cols[i] for i in group),
                         tuple((names[i], cols[i]) for i in group)))
    else:
        buffers = cols
        for i, count in enumerate(cols):
            places.append((i, 0, count))
            dots.append((i, 0, count, ((names[i], count),)))
    att_w, ret_w = heads * HD, ret * RV
    paired = kv == 2 and 2 * HD == 128
    assert kv == 1 or HD % ((att_w + ret_w) // n_sp) == 0
    cfg = dict(paired=paired, n_sp=n_sp, n_tp=n_tp, n_chips=n_chips, chunks=chunks, chan=chan, heads=heads,
               ret=ret, kv=kv, buffers=buffers, places=places, dots=dots, joined=joined)
    tables = rope_tables(n_sp * chunks, CHUNK, ret) + rope_tables(CHUNK, 1, ret)
    small = [norm_gain.reshape(1, width), att_sink.reshape(1, heads), decay_log]
    small += [jnp.asarray(t) for t in tables]
    anyw = pl.BlockSpec(memory_space=pl.ANY)
    dma = pltpu.SemaphoreType.DMA
    mixes = rows // MIX
    scratch = [pltpu.VMEM((width, count), BF16) for count in buffers] + [
        pltpu.VMEM(a.shape, F32) for a in small] + [
        pltpu.VMEM((rows, group[2]), F32) for group in dots] + [
        pltpu.VMEM((n_tp, att_w + ret_w, chan), BF16),
        pltpu.VMEM((n_tp, rows, chan), BF16),
        pltpu.VMEM((max(n_chips - 1, 1), CHUNK, 2 * chan), BF16),
        pltpu.VMEM((rows, att_w * (2 if paired else 1)), BF16),
        pltpu.VMEM((rows + 2 * WINDOW, kv_cols), BF16),
        pltpu.VMEM((kv_cols, rows + 2 * WINDOW), BF16),
        pltpu.VMEM((n_tp, rows, att_w + ret_w), BF16),
        pltpu.VMEM((ret, rows, 2 * RK), BF16),
        pltpu.VMEM((ret, rows, RV), F32),
        pltpu.VMEM((rows, ret_w), BF16),
        pltpu.VMEM((ret, chunks, RK, RV), F32),
        pltpu.VMEM((ret, chunks, RK, RV), F32),
        pltpu.VMEM((ret, chunks, 8, 128), F32),
        pltpu.VMEM((ret, chunks, 2 * RK, RV), BF16),
        pltpu.VMEM((rows, 1), F32),
        pltpu.VMEM((ret, chunks, CHUNK, CHUNK), F32),
        pltpu.VMEM((ret, rows, 2 * RK), F32),
        pltpu.VMEM((ret, rows, 2 * RK), F32),
        pltpu.VMEM((3, MIX + 2 * WINDOW, MIX), F32),
        pltpu.VMEM((rows, chan), F32),
        pltpu.VMEM((ret, RK, RV), BF16),
        pltpu.VMEM((ret, RK, RV), BF16),
        pltpu.VMEM((n_sp, ret, RK, RV), BF16),
        pltpu.VMEM((n_sp, ret, 8, 128), F32),
        pltpu.VMEM((2, ret, RK, RV), F32),
        pltpu.SemaphoreType.REGULAR,
        dma((len(buffers),)), dma, dma, dma((len(small) + 1,)),
        dma, dma((n_chips - 1, chunks)), dma((chunks,)), dma((chunks,)),
        dma, dma((n_chips - 1, mixes)), dma((ret, n_chips - 1, mixes)), dma((mixes,)), dma((mixes,)),
        dma, dma, dma((3,)), dma((n_sp // 2 + 1,)),
        dma((2,)), dma((2,)),
        dma, dma((ret,)), dma, dma,
    ]
    return pl.pallas_call(
        functools.partial(kernel, cfg),
        out_shape=pltpu.VMEM((rows, chan), BF16),
        in_specs=[anyw] * (11 + len(small)),
        out_specs=pl.BlockSpec(memory_space=pltpu.VMEM),
        scratch_shapes=scratch,
        compiler_params=pltpu.CompilerParams(
            collective_id=0, has_side_effects=True, vmem_limit_bytes=60 * 1024 * 1024),
    )(tokens, *weights, init_state, out_att, out_ret, *small)


def solution(mesh):
    n_sp, n_tp = mesh.shape["sp"], mesh.shape["tp"]
    in_specs = (
        P("sp", "tp"),
        P(),
        P(None, "tp"),
        P(None, "tp"),
        P(None, "tp"),
        P(None, "tp"),
        P(None, "tp"),
        P(None, "tp"),
        P(None, "tp"),
        P("tp"),
        P("tp", "sp"),
        P(None, "tp", None, None),
        P("tp", None),
        P("tp", None),
    )
    return jax.shard_map(functools.partial(body, n_sp, n_tp), mesh=mesh, in_specs=in_specs,
                         out_specs=P("sp", "tp"), check_vma=False)
```

```python
import contextlib
import functools

import jax
import jax.numpy as jnp
import numpy as np
from jax import lax
from jax.experimental import pallas as pl
from jax.experimental.pallas import tpu as pltpu
from jax.sharding import PartitionSpec as P

HD = 64
RK = 64
RV = 128
WINDOW = 128
CHUNK = 256
MIX = 128
NORM_EPS = 1e-06
ROPE_BASE = 10000.0
F32 = jnp.float32
BF16 = jnp.bfloat16
MESH = pl.DeviceIdType.MESH


def scope(name):
    return contextlib.nullcontext()


def rope_tables(count, step, heads):
    half = RK // 2
    inverse = ROPE_BASE ** (-2.0 * np.arange(half, dtype=np.float64) / RK)
    angles = (np.arange(count, dtype=np.float64) * step)[:, None] * inverse[None, :]
    wide = np.tile(np.concatenate([angles, angles], axis=1), (1, heads))
    return np.cos(wide).astype(np.float32), np.sin(wide).astype(np.float32)


def remote(src, dst, send, recv, **where):
    return pltpu.make_async_remote_copy(
        src_ref=src, dst_ref=dst, send_sem=send, recv_sem=recv,
        device_id=where, device_id_type=MESH,
    )


def rows_of(index, size):
    return pl.ds(pl.multiple_of(index * size, size), size)


def mm(a, b):
    return jnp.dot(a, b, preferred_element_type=F32)


def mm_t(a, b):
    return lax.dot_general(a, b, (((1,), (1,)), ((), ())), preferred_element_type=F32)


def tm_m(a, b):
    return lax.dot_general(a, b, (((0,), (0,)), ((), ())), preferred_element_type=F32)


class Spread:
    def __init__(self, place, buf, columns, size, send, cross, near, settled, src=None):
        self.place, self.buf, self.columns, self.size = place, buf, columns, size
        self.send, self.cross, self.near, self.settled, self.src = send, cross, near, settled, src

    def block(self, slot, c):
        return self.buf.at[slot, rows_of(c, self.size), self.columns]

    def start(self, c):
        tp, partner, across, n_chips = self.place
        src = self.block(tp, c) if self.src is None else self.src.at[rows_of(c, self.size), :]
        for k in range(1, n_chips):
            remote(src, self.block(tp, c), self.send, self.cross.at[n_chips - k - 1, c], tp=across(k)).start()
        remote(src, self.block(tp, c), self.send, self.near.at[c], tp=partner).start()

    def relay(self, c):
        _, partner, across, n_chips = self.place
        for k in range(1, n_chips):
            block = self.block(across(k), c)
            remote(block, block, self.send, self.cross.at[k - 1, c], tp=partner).wait_recv()
            remote(block, block, self.send, self.settled.at[c], tp=partner).start()


def kernel(cfg, *refs):
    n_buf, n_small = len(cfg["buffers"]), 8
    (tokens, w_q, w_k, w_v, w_rq, w_rk, w_rv, w_rg, init, o_att, o_ret) = refs[:11]
    small_hbm = refs[11:11 + n_small - 1]
    out = refs[10 + n_small]
    rest = refs[11 + n_small:]
    w_bufs = rest[:n_buf]
    small = rest[n_buf:n_buf + n_small - 1]
    parts = rest[n_buf + n_small - 1:n_buf + n_small - 1 + len(cfg["dots"])]
    gain, sink, decay, outer_cos, outer_sin, inner_cos, inner_sin = small
    (wg, gath, xbuf, qs, kbuf, vt, mx, qfb, rloc, gs, fterm, bterm, blog, both_in,
     sqs, dm, kfac, qfac, bias, base,
     tot_f, tot_b, tots, logs, states,
     ready, w_sem, wo_sem, tok_sem, small_sem,
     tok_send, tok_cross, tok_near, tok_settled, half_cross, half_settled, mix_send, att_cross, ret_cross, most_settled, last_settled,
     pw_send, pw_recv, w_send, w_recv,
     halo_send, halo_recv, tot_send, tot_recv, log_send, log_recv) = rest[n_buf + n_small - 1 + len(parts):]
    n_tp, n_sp, n_chips, chunks = cfg["n_tp"], cfg["n_sp"], cfg["n_chips"], cfg["chunks"]
    chan, heads, ret, kv = cfg["chan"], cfg["heads"], cfg["ret"], cfg["kv"]
    rows = chunks * CHUNK
    width = n_tp * chan
    groups = heads // kv
    seq_len = rows * n_sp
    att_w, ret_w = heads * HD, ret * RV
    piece = (att_w + ret_w) // n_sp
    per = CHUNK // MIX
    mixes = rows // MIX
    sp = lax.axis_index("sp")
    tp = lax.axis_index("tp")
    core = lax.rem(tp, 2)
    chip = lax.div(tp, 2)
    partner = chip * 2 + 1 - core

    def across(k):
        return lax.rem(chip + k, n_chips) * 2 + core

    place = (tp, partner, across, n_chips)
    tok = Spread(place, gath, slice(None), CHUNK, tok_send, tok_cross, tok_near, tok_settled, src=tokens)
    atd = Spread(place, mx, pl.ds(0, att_w), MIX, mix_send, att_cross, most_settled, most_settled)
    most = att_w + ret_w - RV
    rtd = []
    for h in range(ret):
        settled = most_settled if h < ret - 1 else last_settled
        rtd.append(Spread(place, mx, pl.ds(att_w + h * RV, RV), MIX, mix_send, ret_cross.at[h], settled, settled))

    def arrived(ref, sem):
        pltpu.make_async_copy(ref, ref, sem).wait()

    barrier = pltpu.get_barrier_semaphore()
    for k in range(1, n_tp):
        pl.semaphore_signal(barrier, inc=1, device_id={"tp": lax.rem(tp + k, n_tp)}, device_id_type=MESH)

    @pl.when(sp == 0)
    def _():
        for k in range(1, n_sp):
            pl.semaphore_signal(barrier, inc=1, device_id={"sp": k}, device_id_type=MESH)

    token_copy = pltpu.make_async_copy(tokens, gath.at[tp], tok_sem)
    token_copy.start()
    local = [pltpu.make_async_copy(a, b, small_sem.at[i]) for i, (a, b) in enumerate(zip(small_hbm, small))]
    local.append(pltpu.make_async_copy(init, states, small_sem.at[n_small - 1]))
    weights = (w_q, w_k, w_v, w_rq, w_rk, w_rv, w_rg)
    for w_ref, (b, off, cols) in zip(weights, cfg["places"]):
        dst = w_bufs[b].at[:, pl.ds(off, cols)] if cfg["joined"] else w_bufs[b]
        pltpu.make_async_copy(w_ref, dst, w_sem.at[b]).start()
    paired = cfg["paired"]

    def att_row(row):
        if kv == 1:
            return row
        spot, within = row // HD, row % HD
        return (spot % kv * groups + spot // kv) * HD + within

    runs = [(o_att, att_row(b * HD), b * HD, HD) for b in range(heads)]
    runs.append((o_ret, 0, att_w, ret_w))

    def columns(t):
        return pl.ds(pl.multiple_of(t * chan, chan), chan)

    for src, row, first, count in runs:
        pltpu.make_async_copy(src.at[pl.ds(row, count), columns(tp)], wg.at[tp, pl.ds(first, count), :], wo_sem).start()
    for copy in local:
        copy.start()

    with scope("barrier"):
        @pl.when(sp == 0)
        def _():
            pl.semaphore_wait(barrier, n_tp - 1)

        @pl.when(sp > 0)
        def _():
            pl.semaphore_wait(barrier, n_tp)
            pl.semaphore_signal(ready, inc=1, device_id={"sp": 0}, device_id_type=MESH)

    others = [lax.rem(chip + k, n_chips) * 2 + p for k in range(1, n_chips) for p in range(2)]

    def w_copy(t, e, send, recv, **where):
        block = wg.at[t, rows_of(e, piece), :]
        return remote(block, block, w_send.at[send], w_recv.at[recv], **where)

    def w_done(sem, pieces):
        left, full = pieces * len(others) * piece, att_w + ret_w
        while left > 0:
            arrived(wg.at[0, 0:min(left, full), :], sem)
            left -= full

    def w_first(src, row):
        for t in others:
            remote(src.at[pl.ds(pl.multiple_of(row, piece), piece), columns(t)], wg.at[tp, rows_of(sp, piece), :],
                   w_send.at[0], w_recv.at[0], tp=t).start()

    @pl.when(sp * piece < att_w)
    def _():
        w_first(o_att, att_row(sp * piece))

    @pl.when(sp * piece >= att_w)
    def _():
        w_first(o_ret, sp * piece - att_w)

    def order(i):
        return lax.rem(i + chunks - 1, chunks)

    def first_sends(i, carry):
        tok.start(order(i))
        return carry

    final = chunks - 2

    def half_rows(part):
        return pl.ds(final * CHUNK + part * MIX, MIX)

    def half_start(part):
        mine = half_rows(part)
        for k in range(1, n_chips):
            remote(tokens.at[mine, :], gath.at[tp, mine, :], tok_send, half_cross.at[n_chips - k - 1, part],
                   tp=across(k)).start()
        remote(tokens.at[mine, :], gath.at[tp, mine, :], tok_send, tok_near.at[final], tp=partner).start()

    def half_relay(part):
        for k in range(1, n_chips):
            block = gath.at[across(k), half_rows(part), :]
            remote(block, block, tok_send, half_cross.at[k - 1, part], tp=partner).wait_recv()
            remote(block, block, tok_send, half_settled.at[part], tp=partner).start()

    lax.fori_loop(0, chunks - 1, first_sends, 0)
    for part in range(per):
        half_start(part)

    for src, row, first, count in runs:
        remote(src.at[pl.ds(row, count), columns(partner)], wg.at[tp, pl.ds(first, count), :],
               pw_send, pw_recv, tp=partner).start()

    with scope("lwait"):
        for copy in local:
            copy.wait()
        token_copy.wait()
        for i, buf in enumerate(w_bufs):
            arrived(buf, w_sem.at[i])
        arrived(wg.at[tp], wo_sem)

    for h in range(ret):
        total = jnp.sum(decay[h:h + 1, :], axis=1, keepdims=True)
        logs[sp, h] = jnp.broadcast_to(total, (8, 128))

    @pl.when(sp == 0)
    def _():
        kbuf[0:WINDOW, :] = jnp.zeros((WINDOW, kbuf.shape[1]), BF16)
        vt[:, 0:WINDOW] = jnp.zeros((vt.shape[0], WINDOW), BF16)

    @pl.when(sp == n_sp - 1)
    def _():
        kbuf[rows + WINDOW:, :] = jnp.zeros((WINDOW, kbuf.shape[1]), BF16)
        vt[:, rows + WINDOW:] = jnp.zeros((vt.shape[0], WINDOW), BF16)

    row_i = lax.broadcasted_iota(jnp.int32, (CHUNK, CHUNK), 0)
    col_i = lax.broadcasted_iota(jnp.int32, (CHUNK, CHUNK), 1)
    low = lax.broadcasted_iota(jnp.int32, (CHUNK, 2 * RK), 1) < RK

    def decays(c, carry):
        here = rows_of(c, CHUNK)
        for h in range(ret):
            log_row = decay[h:h + 1, here]
            wide = jnp.broadcast_to(log_row, (CHUNK, CHUNK))
            log_col = jnp.sum(jnp.where(row_i == col_i, wide, 0.0), axis=1, keepdims=True)
            cum_col = jnp.sum(jnp.where(col_i <= row_i, wide, 0.0), axis=1, keepdims=True)
            cum_row = jnp.sum(jnp.where(row_i <= col_i, log_col, 0.0), axis=0, keepdims=True)
            total = jnp.sum(log_row, axis=1, keepdims=True)
            dm[h, c] = jnp.exp(-jnp.abs(cum_col - cum_row))
            up = jnp.exp(cum_col)
            down = jnp.exp(jnp.minimum(total - cum_col, 0.0))
            kfac[h, here, :] = jnp.where(low, down, up)
            qfac[h, here, :] = jnp.where(low, up, down)
            blog[h, c] = jnp.broadcast_to(total, (8, 128))
        return carry

    with scope("decays"):
        lax.fori_loop(0, chunks, decays, 0)

    shape = (MIX + 2 * WINDOW, MIX)
    q_i = lax.broadcasted_iota(jnp.int32, shape, 1)
    k_i = lax.broadcasted_iota(jnp.int32, shape, 0)
    band = (k_i >= q_i) & (k_i <= q_i + 2 * WINDOW)
    bias[0] = jnp.where(band, 0.0, -jnp.inf)
    bias[1] = jnp.where(band & (k_i >= WINDOW), 0.0, -jnp.inf)
    bias[2] = jnp.where(band & (k_i < MIX + WINDOW), 0.0, -jnp.inf)

    def normed(here, which, dst, first=0, size=CHUNK):
        squares = jnp.zeros((size, 1), F32)
        for p in range(2):
            slot = which * 2 + p
            x = gath[slot, here, :].astype(F32)
            squares = squares + jnp.sum(x * x, axis=1, keepdims=True)
            xbuf[dst, first:first + size, p * chan:(p + 1) * chan] = (x * gain[0:1, columns(slot)]).astype(BF16)
        return squares

    def product(which, src, b, off, cols, first=0, size=CHUNK):
        span = pl.ds(pl.multiple_of(which * (2 * chan), 2 * chan), 2 * chan)
        return mm(xbuf[src, first:first + size, :], w_bufs[b][span, off:off + cols])

    def near(i, carry):
        c = order(i)
        here = rows_of(c, CHUNK)
        arrived(gath.at[0, here, :], tok_near.at[c])
        sqs[here, :] = normed(here, chip, 0)
        for part, (b, off, cols, _) in zip(parts, cfg["dots"]):
            part[here, :] = product(chip, 0, b, off, cols)
        return carry

    with scope("near"):
        lax.fori_loop(0, chunks // 2, near, 0)

    with scope("ready"):
        @pl.when(sp == 0)
        def _():
            pl.semaphore_wait(ready, n_sp - 1)
            for k in range(1, n_sp):
                pl.semaphore_signal(ready, inc=1, device_id={"sp": k}, device_id_type=MESH)

        @pl.when(sp > 0)
        def _():
            pl.semaphore_wait(ready, 1)

    for k in range(1, n_sp):
        remote(logs.at[sp], logs.at[sp], log_send, log_recv, sp=lax.rem(sp + k, n_sp)).start()

    beside = sp + 1 - 2 * lax.rem(sp, 2)
    half_sp = n_sp // 2
    with scope("wfwd"):
        w_done(w_recv.at[0], 1)

        def w_pass(k, carry):
            for t in others:
                w_copy(t, sp, 1, k + 1, sp=lax.rem(sp + 2 * k, n_sp)).start()
            return carry

        lax.fori_loop(1, half_sp, w_pass, 0)
        for t in others:
            w_copy(t, sp, 2, 1, sp=beside).start()

    def w_aside(first, end):
        def w_over(k, carry):
            w_done(w_recv.at[k + 1], 1)
            for t in others:
                w_copy(t, lax.rem(sp + n_sp - 2 * k, n_sp), 2, 1, sp=beside).start()
            return carry

        lax.fori_loop(first, end, w_over, 0)

    with scope("near"):
        lax.fori_loop(chunks // 2, chunks, near, 0)

    rw = ret * RK
    p_row = lax.broadcasted_iota(jnp.int32, (rw, rw), 0)
    p_col = lax.broadcasted_iota(jnp.int32, (rw, rw), 1)
    first_half = lax.rem(p_col, RK) < RK // 2
    swap = jnp.where(
        first_half & (p_row == p_col + RK // 2), -1.0,
        jnp.where(jnp.logical_not(first_half) & (p_row == p_col - RK // 2), 1.0, 0.0),
    ).astype(BF16)
    ones = jnp.ones((HD, MIX + 2 * WINDOW), BF16)

    def attend(i):
        here = rows_of(i, MIX)
        span = pl.ds(pl.multiple_of(i * MIX, MIX), MIX + 2 * WINDOW)
        edge = lax.select((sp == 0) & (i == 0), 1, lax.select((sp == n_sp - 1) & (i == mixes - 1), 2, 0))
        block = bias[edge]
        block = jnp.concatenate([block] * groups, axis=1)
        done = []
        for g in range(kv):
            if paired:
                spots = [(j * kv + g) * 2 * HD for j in range(groups)]
                query = jnp.concatenate([qs[here, at:at + 2 * HD] for at in spots], axis=0)
                key = kbuf[span, :]
            else:
                spots = [(g * groups + j) * HD for j in range(groups)]
                query = jnp.concatenate([qs[here, at:at + HD] for at in spots], axis=0)
                key = kbuf[span, g * HD:(g + 1) * HD]
            value = jnp.concatenate([vt[g * HD:(g + 1) * HD, span], ones], axis=0)
            scores = mm_t(key, query) + block
            sink_row = jnp.concatenate(
                [jnp.broadcast_to(sink[0:1, g * groups + j:g * groups + j + 1], (1, MIX)) for j in range(groups)],
                axis=1)
            top = jnp.maximum(jnp.max(scores, axis=0, keepdims=True), sink_row)
            result = mm(value, jnp.exp(scores - top).astype(BF16))
            scale = 1.0 / (result[HD:HD + 1, :] + jnp.exp(sink_row - top))
            done.append(result[0:HD, :] * scale)
        both = jnp.concatenate(done, axis=0) if kv > 1 else done[0]
        turned = [jnp.transpose(both[:, j * MIX:(j + 1) * MIX]).astype(BF16) for j in range(groups)]
        if kv * HD % 128 == 0:
            for j in range(groups):
                mx[tp, here, j * kv * HD:(j + 1) * kv * HD] = turned[j]
        else:
            mx[tp, here, 0:att_w] = jnp.concatenate(turned, axis=1)
        atd.start(i)

    left, right = sp - 1, sp + 1

    def halo(side, i, where):
        def part(at):
            return kbuf.at[pl.ds(at, WINDOW), :] if i == 0 else vt.at[:, pl.ds(at, WINDOW)]

        src, dst = ((rows, 0), (WINDOW, rows + WINDOW))[side]
        return remote(part(src), part(dst), halo_send.at[side], halo_recv.at[side], sp=where)

    far = [(k - 1, lax.rem(chip + k, n_chips)) for k in range(1, n_chips)]

    def finish(found, here, inv_rms, first, size, *wanted):
        for part, (b, off, cols, names) in zip(parts, cfg["dots"]):
            if names[0][0] not in wanted:
                continue
            total = part[here, :]
            for at, which in far:
                total = total + product(which, at, b, off, cols, first, size)
            block = (total * inv_rms).astype(BF16)
            at = 0
            for name, count in names:
                found[name] = block[:, at:at + count]
                at += count

    def inverse(squares):
        return lax.rsqrt(squares / width + NORM_EPS)

    def attention_inputs(here, shifted, inv_rms, first, size):
        found = {}
        finish(found, here, inv_rms, first, size, "q", "k", "v")
        scaled = found["q"] * jnp.asarray(HD ** -0.5, BF16)
        if paired:
            wide = scaled.astype(F32)
            head = [wide[:, at:at + 2 * HD] for at in range(0, att_w, 2 * HD)]
            turned = [pltpu.roll(x, HD, 1) for x in head]
            lowest = lax.broadcasted_iota(jnp.int32, (size, 2 * HD), 1) < HD
            for j in range(groups):
                for g in range(kv):
                    at = (g * groups + j) * HD
                    x = (head if at % (2 * HD) == g * HD else turned)[at // (2 * HD)]
                    keep = lowest if g == 0 else jnp.logical_not(lowest)
                    to = (j * kv + g) * 2 * HD
                    qs[here, to:to + 2 * HD] = jnp.where(keep, x, 0.0).astype(BF16)
        else:
            qs[here, :] = scaled
        kbuf[shifted, :] = found["k"]
        vt[:, shifted] = jnp.transpose(found["v"].astype(F32)).astype(BF16)

    def far_squares(here, first, size):
        squares = sqs[here, :]
        for at, which in far:
            squares = squares + normed(here, which, at, first, size)
        return squares

    def half(part, between):
        mine = half_rows(part)
        half_relay(part)
        between()
        with scope("x2"):
            arrived(gath.at[0:n_chips - 1, mine, :], half_settled.at[part])
        return far_squares(mine, part * MIX, MIX)

    def half_inputs(part, squares):
        with scope("phaseB"):
            attention_inputs(half_rows(part), pl.ds(final * CHUNK + part * MIX + WINDOW, MIX), inverse(squares),
                             part * MIX, MIX)

    def chunk(c, last, between, squares=None, while_waiting=None):
        here = rows_of(c, CHUNK)
        if not last:
            with scope("x1"):
                tok.relay(c)
            between()
            with scope("x2"):
                arrived(gath.at[0:n_chips - 1, here, :], tok_settled.at[c])
        ctx = scope("phaseA")
        ctx.__enter__()
        if not last:
            squares = far_squares(here, 0, CHUNK)
        inv_rms = inverse(squares)
        found = {}
        finish(found, here, inv_rms, 0, CHUNK, "rq", "rk", "rv")
        spot = sp * chunks + c
        oc, os_ = outer_cos[pl.ds(spot, 1), :], outer_sin[pl.ds(spot, 1), :]
        ic, is_ = inner_cos[...], inner_sin[...]
        cosine = oc * ic - os_ * is_
        sine = os_ * ic + oc * is_
        query_rot = found["rq"].astype(F32) * cosine + mm(found["rq"], swap) * sine
        key_rot = (found["rk"].astype(F32) * cosine + mm(found["rk"], swap) * sine) * RK ** -0.5

        def doubled(x):
            if ret == 2:
                turned = pltpu.roll(x, RK, 1)
                return jnp.where(low, x, turned), jnp.where(low, turned, x)
            return [jnp.concatenate([x[:, h * RK:(h + 1) * RK]] * 2, axis=1) for h in range(ret)]

        keys = doubled(key_rot)
        for h in range(ret):
            both = (keys[h] * kfac[h, here, :]).astype(BF16)
            terms = tm_m(both, found["rv"][:, h * RV:(h + 1) * RV])
            fterm[h, c] = terms[:RK]
            bterm[h, c] = terms[RK:]
        ctx.__exit__(None, None, None)
        if last:
            with scope("totals"):
                send_totals()
        if last:
            while_waiting()
        else:
            with scope("phaseB"):
                attention_inputs(here, pl.ds(pl.multiple_of(c * CHUNK + WINDOW, 128), CHUNK), inv_rms, 0, CHUNK)
        ctx = scope("phaseC")
        ctx.__enter__()
        finish(found, here, inv_rms, 0, CHUNK, "g")
        gs[here, :] = found["g"]
        queries = doubled(query_rot)
        key_bf = key_rot.astype(BF16)
        for h in range(ret):
            if ret == 2:
                keep = low if h == 0 else jnp.logical_not(low)
                inner = mm_t(jnp.where(keep, query_rot, 0.0).astype(BF16), key_bf)
            else:
                inner = mm_t(query_rot[:, h * RK:(h + 1) * RK].astype(BF16), key_bf[:, h * RK:(h + 1) * RK])
            rloc[h, here, :] = mm((inner * dm[h, c]).astype(BF16), found["rv"][:, h * RV:(h + 1) * RV])
            qfb[h, here, :] = (queries[h] * qfac[h, here, :]).astype(BF16)
        ctx.__exit__(None, None, None)

    def send_totals():
        for h in range(ret):
            state = jnp.zeros((RK, RV), F32)
            back = jnp.zeros((RK, RV), F32)
            for c in range(chunks):
                state = jnp.exp(blog[h, c, 0:1, :]) * state + fterm[h, c]
                back = jnp.exp(blog[h, chunks - 1 - c, 0:1, :]) * back + bterm[h, chunks - 1 - c]
            tot_f[h] = state.astype(BF16)
            tot_b[h] = back.astype(BF16)

            def send_f(i, carry):
                remote(tot_f.at[h], tots.at[sp, h], tot_send, tot_recv.at[h], sp=n_sp - 1 - i).start()
                return carry

            def send_b(d, carry):
                remote(tot_b.at[h], tots.at[sp, h], tot_send, tot_recv.at[h], sp=d).start()
                return carry

            lax.fori_loop(0, n_sp - 1 - sp, send_f, 0)
            lax.fori_loop(0, sp, send_b, 0)

    early = per * (chunks - 3) + 1

    def block_of(j):
        turn = early - per + 1
        return lax.select(j < turn, j, lax.select(j == turn, mixes - 1, j - 1))

    def halo_wait(side):
        arrived(kbuf.at[0:2 * WINDOW, :], halo_recv.at[side])

    def one(j):
        with scope("attend"):
            attend(j)

    def chunk_body(i, carry):
        c = order(i)

        if chunks > 4:
            @pl.when(i > 2)
            def _():
                one(per * (i - 3) + 1)

        def between():
            @pl.when(i == chunks - 2)
            def _():
                with scope("aside"):
                    w_aside(chunks - 1, half_sp)

            @pl.when((i == 2) & (sp > 0))
            def _():
                with scope("halo0"):
                    halo_wait(0)

            @pl.when(i == 2)
            def _():
                one(0)

            if chunks > 4:
                @pl.when(i > 2)
                def _():
                    one(per * (i - 3) + 2)

        chunk(c, False, between)

        @pl.when((i == 0) & (sp < n_sp - 1))
        def _():
            for b in range(2):
                halo(0, b, right).start()

        @pl.when((i == 1) & (sp > 0))
        def _():
            for b in range(2):
                halo(1, b, left).start()

        @pl.when(i < min(chunks - 2, half_sp - 1))
        def _():
            with scope("aside"):
                w_aside(i + 1, i + 2)

        return carry

    lax.fori_loop(0, chunks - 1, chunk_body, 0)

    def late(j, carry):
        with scope("late"):
            attend(j)
        with scope("lrelay"):
            atd.relay(block_of(j - early))
        return carry

    first_squares = half(0, lambda: one(early - per))
    half_inputs(0, first_squares)

    @pl.when(sp < n_sp - 1)
    def _():
        with scope("halo1"):
            halo_wait(1)

    one(mixes - 1)
    last_squares = half(1, lambda: one(early - per + 1))

    def rest():
        late(early, 0)
        half_inputs(1, last_squares)
        lax.fori_loop(early + 1, mixes - 1, late, 0)

    chunk(final, True, None, jnp.concatenate([first_squares, last_squares], axis=0), rest)

    def states_of(h):
        arrived(tots.at[0:n_sp - 1, 0], tot_recv.at[h])

        def from_low(e, state):
            return jnp.exp(logs[e, h, 0:1, :]) * state + tots[e, h].astype(F32)

        def from_high(i, back):
            e = n_sp - 1 - i
            return jnp.exp(logs[e, h, 0:1, :]) * back + tots[e, h].astype(F32)

        state = lax.fori_loop(0, sp, from_low, states[0, h])
        back = lax.fori_loop(0, n_sp - 1 - sp, from_high, states[1, h])
        for c in range(chunks):
            both_in[h, c, 0:RK] = state.astype(BF16)
            state = jnp.exp(blog[h, c, 0:1, :]) * state + fterm[h, c]
            r = chunks - 1 - c
            both_in[h, r, RK:2 * RK] = back.astype(BF16)
            back = jnp.exp(blog[h, r, 0:1, :]) * back + bterm[h, r]

    def retain(c, h):
        here = rows_of(c, MIX)
        combined = rloc[h, here, :] + mm(qfb[h, here, :], both_in[h, lax.div(c, per)])
        centered = combined - jnp.mean(combined, axis=1, keepdims=True)
        normed_ret = centered * lax.rsqrt(jnp.mean(centered * centered, axis=1, keepdims=True) + NORM_EPS)
        gate = gs[here, h * RV:(h + 1) * RV].astype(F32)
        mx[tp, here, att_w + h * RV:att_w + (h + 1) * RV] = (gate / (1.0 + jnp.exp(-gate)) * normed_ret).astype(BF16)
        rtd[h].start(c)

    arrived(logs.at[0:n_sp - 1], log_recv)
    for h in range(ret):
        with scope("states"):
            states_of(h)

        def ret_body(c, carry):
            retain(c, h)
            return carry

        with scope("retain"):
            lax.fori_loop(0, mixes, ret_body, 0)

    def att_rest(j, carry):
        atd.relay(block_of(j))
        return carry

    with scope("attrest"):
        lax.fori_loop(mixes - 1 - early, mixes, att_rest, 0)

    with scope("wsettle"):
        arrived(wg.at[0], pw_recv)
        w_done(w_recv.at[1], half_sp)

    def mix_most(c):
        here = rows_of(c, MIX)
        with scope("bsettle"):
            arrived(mx.at[0:n_chips, here, 0:most], most_settled.at[c])
        with scope("base"):
            total = mm(mx[0, here, 0:most], wg[0, 0:most, :])
            for t in range(1, n_tp):
                total = total + mm(mx[t, here, 0:most], wg[t, 0:most, :])
            base[here, :] = total

    def mix_last(c):
        here = rows_of(c, MIX)
        with scope("msettle"):
            arrived(mx.at[0:n_chips, here, most:most + RV], last_settled.at[c])
        with scope("mix"):
            total = base[here, :]
            for t in range(n_tp):
                total = total + mm(mx[t, here, most:], wg[t, most:, :])
            out[here, :] = total.astype(BF16)

    lag = 2

    def first_heads(c, carry):
        with scope("hrelay"):
            for h in range(ret - 1):
                rtd[h].relay(c)

        @pl.when(c >= lag)
        def _():
            mix_most(c - lag)

        return carry

    def last_head(c, carry):
        with scope("rrelay"):
            rtd[ret - 1].relay(c)

        @pl.when(c < lag)
        def _():
            mix_most(mixes - lag + c)

        @pl.when(c >= lag)
        def _():
            mix_last(c - lag)

        return carry

    def ending(c, carry):
        mix_last(c)
        return carry

    lax.fori_loop(0, mixes, first_heads, 0)
    lax.fori_loop(0, mixes, last_head, 0)
    lax.fori_loop(mixes - lag, mixes, ending, 0)

    with scope("drain"):
        sent = 2 * n_chips - 1
        arrived(gath.at[0:sent], tok_send)
        arrived(mx.at[0:sent], mix_send)
        arrived(wg.at[0], pw_send)
        w_done(w_send.at[0], 1)
        w_done(w_send.at[1], half_sp - 1)
        w_done(w_send.at[2], half_sp)
        arrived(logs.at[0:n_sp - 1], log_send)
        arrived(tots.at[0:n_sp - 1], tot_send)

        @pl.when(sp < n_sp - 1)
        def _():
            arrived(kbuf.at[0:2 * WINDOW, :], halo_send.at[0])

        @pl.when(sp > 0)
        def _():
            arrived(kbuf.at[0:2 * WINDOW, :], halo_send.at[1])


def body(n_sp, n_tp, tokens, norm_gain, w_q, w_k, w_v, w_rq, w_rk, w_rv, w_rg, att_sink,
         decay_log, init_state, out_att, out_ret):
    rows, chan = tokens.shape
    width = n_tp * chan
    ret = decay_log.shape[0]
    heads = att_sink.shape[0]
    kv_cols = w_k.shape[1]
    kv = kv_cols // HD
    chunks = rows // CHUNK
    n_chips = n_tp // 2
    weights = (w_q, w_k, w_v, w_rq, w_rk, w_rv, w_rg)
    names = ("q", "k", "v", "rq", "rk", "rv", "g")
    cols = [w.shape[1] for w in weights]
    joined = all(count % 128 == 0 for count in cols)
    places, dots = [], []
    if joined:
        buffers = [sum(cols)]
        at = 0
        for count in cols:
            places.append((0, at, count))
            at += count
        for group in ((3, 4), (5,), (1, 2), (0,), (6,)):
            dots.append((0, places[group[0]][1], sum(cols[i] for i in group),
                         tuple((names[i], cols[i]) for i in group)))
    else:
        buffers = cols
        for i, count in enumerate(cols):
            places.append((i, 0, count))
            dots.append((i, 0, count, ((names[i], count),)))
    att_w, ret_w = heads * HD, ret * RV
    paired = kv == 2 and 2 * HD == 128
    assert kv == 1 or HD % ((att_w + ret_w) // n_sp) == 0
    cfg = dict(paired=paired, n_sp=n_sp, n_tp=n_tp, n_chips=n_chips, chunks=chunks, chan=chan, heads=heads,
               ret=ret, kv=kv, buffers=buffers, places=places, dots=dots, joined=joined)
    tables = rope_tables(n_sp * chunks, CHUNK, ret) + rope_tables(CHUNK, 1, ret)
    small = [norm_gain.reshape(1, width), att_sink.reshape(1, heads), decay_log]
    small += [jnp.asarray(t) for t in tables]
    anyw = pl.BlockSpec(memory_space=pl.ANY)
    dma = pltpu.SemaphoreType.DMA
    mixes = rows // MIX
    scratch = [pltpu.VMEM((width, count), BF16) for count in buffers] + [
        pltpu.VMEM(a.shape, F32) for a in small] + [
        pltpu.VMEM((rows, group[2]), F32) for group in dots] + [
        pltpu.VMEM((n_tp, att_w + ret_w, chan), BF16),
        pltpu.VMEM((n_tp, rows, chan), BF16),
        pltpu.VMEM((max(n_chips - 1, 1), CHUNK, 2 * chan), BF16),
        pltpu.VMEM((rows, att_w * (2 if paired else 1)), BF16),
        pltpu.VMEM((rows + 2 * WINDOW, kv_cols), BF16),
        pltpu.VMEM((kv_cols, rows + 2 * WINDOW), BF16),
        pltpu.VMEM((n_tp, rows, att_w + ret_w), BF16),
        pltpu.VMEM((ret, rows, 2 * RK), BF16),
        pltpu.VMEM((ret, rows, RV), F32),
        pltpu.VMEM((rows, ret_w), BF16),
        pltpu.VMEM((ret, chunks, RK, RV), F32),
        pltpu.VMEM((ret, chunks, RK, RV), F32),
        pltpu.VMEM((ret, chunks, 8, 128), F32),
        pltpu.VMEM((ret, chunks, 2 * RK, RV), BF16),
        pltpu.VMEM((rows, 1), F32),
        pltpu.VMEM((ret, chunks, CHUNK, CHUNK), F32),
        pltpu.VMEM((ret, rows, 2 * RK), F32),
        pltpu.VMEM((ret, rows, 2 * RK), F32),
        pltpu.VMEM((3, MIX + 2 * WINDOW, MIX), F32),
        pltpu.VMEM((rows, chan), F32),
        pltpu.VMEM((ret, RK, RV), BF16),
        pltpu.VMEM((ret, RK, RV), BF16),
        pltpu.VMEM((n_sp, ret, RK, RV), BF16),
        pltpu.VMEM((n_sp, ret, 8, 128), F32),
        pltpu.VMEM((2, ret, RK, RV), F32),
        pltpu.SemaphoreType.REGULAR,
        dma((len(buffers),)), dma, dma, dma((len(small) + 1,)),
        dma, dma((n_chips - 1, chunks)), dma((chunks,)), dma((chunks,)),
        dma((n_chips - 1, CHUNK // MIX)), dma((CHUNK // MIX,)),
        dma, dma((n_chips - 1, mixes)), dma((ret, n_chips - 1, mixes)), dma((mixes,)), dma((mixes,)),
        dma, dma, dma((3,)), dma((n_sp // 2 + 1,)),
        dma((2,)), dma((2,)),
        dma, dma((ret,)), dma, dma,
    ]
    return pl.pallas_call(
        functools.partial(kernel, cfg),
        out_shape=pltpu.VMEM((rows, chan), BF16),
        in_specs=[anyw] * (11 + len(small)),
        out_specs=pl.BlockSpec(memory_space=pltpu.VMEM),
        scratch_shapes=scratch,
        compiler_params=pltpu.CompilerParams(
            collective_id=0, has_side_effects=True, vmem_limit_bytes=60 * 1024 * 1024),
    )(tokens, *weights, init_state, out_att, out_ret, *small)


def solution(mesh):
    n_sp, n_tp = mesh.shape["sp"], mesh.shape["tp"]
    in_specs = (
        P("sp", "tp"),
        P(),
        P(None, "tp"),
        P(None, "tp"),
        P(None, "tp"),
        P(None, "tp"),
        P(None, "tp"),
        P(None, "tp"),
        P(None, "tp"),
        P("tp"),
        P("tp", "sp"),
        P(None, "tp", None, None),
        P("tp", None),
        P("tp", None),
    )
    return jax.shard_map(functools.partial(body, n_sp, n_tp), mesh=mesh, in_specs=in_specs,
                         out_specs=P("sp", "tp"), check_vma=False)
```

```python
import contextlib
import functools

import jax
import jax.numpy as jnp
import numpy as np
from jax import lax
from jax.experimental import pallas as pl
from jax.experimental.pallas import tpu as pltpu
from jax.sharding import PartitionSpec as P

HD = 64
RK = 64
RV = 128
WINDOW = 128
CHUNK = 256
MIX = 128
NORM_EPS = 1e-06
ROPE_BASE = 10000.0
F32 = jnp.float32
BF16 = jnp.bfloat16
MESH = pl.DeviceIdType.MESH


def scope(name):
    return contextlib.nullcontext()


def rope_tables(count, step, heads):
    half = RK // 2
    inverse = ROPE_BASE ** (-2.0 * np.arange(half, dtype=np.float64) / RK)
    angles = (np.arange(count, dtype=np.float64) * step)[:, None] * inverse[None, :]
    wide = np.tile(np.concatenate([angles, angles], axis=1), (1, heads))
    return np.cos(wide).astype(np.float32), np.sin(wide).astype(np.float32)


def remote(src, dst, send, recv, **where):
    return pltpu.make_async_remote_copy(
        src_ref=src, dst_ref=dst, send_sem=send, recv_sem=recv,
        device_id=where, device_id_type=MESH,
    )


def rows_of(index, size):
    return pl.ds(pl.multiple_of(index * size, size), size)


def mm(a, b):
    return jnp.dot(a, b, preferred_element_type=F32)


def mm_t(a, b):
    return lax.dot_general(a, b, (((1,), (1,)), ((), ())), preferred_element_type=F32)


def tm_m(a, b):
    return lax.dot_general(a, b, (((0,), (0,)), ((), ())), preferred_element_type=F32)


class Spread:
    def __init__(self, place, buf, columns, size, send, cross, near, settled, src=None, crossing=1, settling=1):
        self.place, self.buf, self.columns, self.size = place, buf, columns, size
        self.send, self.cross, self.near, self.settled, self.src = send, cross, near, settled, src
        self.crossing, self.settling = crossing, settling

    def block(self, slot, c):
        return self.buf.at[slot, rows_of(c, self.size), self.columns]

    def start(self, c):
        tp, partner, across, n_chips = self.place
        src = self.block(tp, c) if self.src is None else self.src.at[rows_of(c, self.size), :]
        for k in range(1, n_chips):
            remote(src, self.block(tp, c), self.send, self.cross.at[n_chips - k - 1, lax.div(c, self.crossing)],
                   tp=across(k)).start()
        near = self.near if self.src is not None else self.near.at[lax.div(c, self.settling)]
        remote(src, self.block(tp, c), self.send, near, tp=partner).start()

    def relay(self, c):
        _, partner, across, n_chips = self.place
        for k in range(1, n_chips):
            block = self.buf.at[across(k), rows_of(c, self.size * self.crossing), self.columns]
            remote(block, block, self.send, self.cross.at[k - 1, c], tp=partner).wait_recv()
            settled = self.settled.at[lax.div(c * self.crossing, self.settling)]
            remote(block, block, self.send, settled, tp=partner).start()


def kernel(cfg, *refs):
    n_buf, n_small = len(cfg["buffers"]), 8
    (tokens, w_q, w_k, w_v, w_rq, w_rk, w_rv, w_rg, init, o_att, o_ret) = refs[:11]
    small_hbm = refs[11:11 + n_small - 1]
    out = refs[10 + n_small]
    rest = refs[11 + n_small:]
    w_bufs = rest[:n_buf]
    small = rest[n_buf:n_buf + n_small - 1]
    parts = rest[n_buf + n_small - 1:n_buf + n_small - 1 + len(cfg["dots"])]
    gain, sink, decay, outer_cos, outer_sin, inner_cos, inner_sin = small
    (wg, gath, xbuf, qs, kbuf, vt, mx, qfb, rloc, gs, fterm, bterm, blog, both_in,
     sqs, dm, kfac, qfac, bias, base, w_last,
     tot_f, tot_b, tots, logs, states,
     ready, w_sem, wo_sem, tok_sem, small_sem,
     tok_send, tok_cross, tok_near, tok_settled, half_cross, half_settled, mix_send, att_cross, ret_cross, last_cross, most_settled,
     last_settled,
     pw_send, pw_recv, w_send, w_recv,
     halo_send, halo_recv, tot_send, tot_recv, log_send, log_recv) = rest[n_buf + n_small - 1 + len(parts):]
    n_tp, n_sp, n_chips, chunks = cfg["n_tp"], cfg["n_sp"], cfg["n_chips"], cfg["chunks"]
    chan, heads, ret, kv = cfg["chan"], cfg["heads"], cfg["ret"], cfg["kv"]
    rows = chunks * CHUNK
    width = n_tp * chan
    groups = heads // kv
    seq_len = rows * n_sp
    att_w, ret_w = heads * HD, ret * RV
    piece = (att_w + ret_w) // n_sp
    per = CHUNK // MIX
    mixes = rows // MIX
    sp = lax.axis_index("sp")
    tp = lax.axis_index("tp")
    core = lax.rem(tp, 2)
    chip = lax.div(tp, 2)
    partner = chip * 2 + 1 - core

    def across(k):
        return lax.rem(chip + k, n_chips) * 2 + core

    place = (tp, partner, across, n_chips)
    tok = Spread(place, gath, slice(None), CHUNK, tok_send, tok_cross, tok_near, tok_settled, src=tokens)
    atd = Spread(place, mx, pl.ds(0, att_w), MIX, mix_send, att_cross, most_settled, most_settled,
                 settling=per)
    most = att_w + ret_w - RV
    rtd = []
    for h in range(ret):
        settled, cross, share = (most_settled, ret_cross.at[h], per) if h < ret - 1 else (last_settled, last_cross, 1)
        rtd.append(Spread(place, mx, pl.ds(att_w + h * RV, RV), MIX, mix_send, cross, settled, settled,
                          crossing=share, settling=share))

    def arrived(ref, sem):
        pltpu.make_async_copy(ref, ref, sem).wait()

    barrier = pltpu.get_barrier_semaphore()
    for k in range(1, n_tp):
        pl.semaphore_signal(barrier, inc=1, device_id={"tp": lax.rem(tp + k, n_tp)}, device_id_type=MESH)

    @pl.when(sp == 0)
    def _():
        for k in range(1, n_sp):
            pl.semaphore_signal(barrier, inc=1, device_id={"sp": k}, device_id_type=MESH)

    token_copy = pltpu.make_async_copy(tokens, gath.at[tp], tok_sem)
    token_copy.start()
    local = [pltpu.make_async_copy(a, b, small_sem.at[i]) for i, (a, b) in enumerate(zip(small_hbm, small))]
    local.append(pltpu.make_async_copy(init, states, small_sem.at[n_small - 1]))
    weights = (w_q, w_k, w_v, w_rq, w_rk, w_rv, w_rg)
    for w_ref, (b, off, cols) in zip(weights, cfg["places"]):
        dst = w_bufs[b].at[:, pl.ds(off, cols)] if cfg["joined"] else w_bufs[b]
        pltpu.make_async_copy(w_ref, dst, w_sem.at[b]).start()
    paired = cfg["paired"]

    def att_row(row):
        if kv == 1:
            return row
        spot, within = row // HD, row % HD
        return (spot % kv * groups + spot // kv) * HD + within

    runs = [(o_att, att_row(b * HD), b * HD, HD) for b in range(heads)]
    runs.append((o_ret, 0, att_w, ret_w))

    def columns(t):
        return pl.ds(pl.multiple_of(t * chan, chan), chan)

    for src, row, first, count in runs:
        pltpu.make_async_copy(src.at[pl.ds(row, count), columns(tp)], wg.at[tp, pl.ds(first, count), :], wo_sem).start()
    for copy in local:
        copy.start()

    with scope("barrier"):
        @pl.when(sp == 0)
        def _():
            pl.semaphore_wait(barrier, n_tp - 1)

        @pl.when(sp > 0)
        def _():
            pl.semaphore_wait(barrier, n_tp)
            pl.semaphore_signal(ready, inc=1, device_id={"sp": 0}, device_id_type=MESH)

    others = [lax.rem(chip + k, n_chips) * 2 + p for k in range(1, n_chips) for p in range(2)]

    def w_copy(t, e, send, recv, **where):
        block = wg.at[t, rows_of(e, piece), :]
        return remote(block, block, w_send.at[send], w_recv.at[recv], **where)

    def w_done(sem, pieces):
        left, full = pieces * len(others) * piece, att_w + ret_w
        while left > 0:
            arrived(wg.at[0, 0:min(left, full), :], sem)
            left -= full

    def w_first(src, row):
        for t in others:
            remote(src.at[pl.ds(pl.multiple_of(row, piece), piece), columns(t)], wg.at[tp, rows_of(sp, piece), :],
                   w_send.at[0], w_recv.at[0], tp=t).start()

    @pl.when(sp * piece < att_w)
    def _():
        w_first(o_att, att_row(sp * piece))

    @pl.when(sp * piece >= att_w)
    def _():
        w_first(o_ret, sp * piece - att_w)

    def order(i):
        return lax.rem(i + chunks - 1, chunks)

    def first_sends(i, carry):
        tok.start(order(i))
        return carry

    final = chunks - 2

    def half_rows(part):
        return pl.ds(final * CHUNK + part * MIX, MIX)

    def half_start(part):
        mine = half_rows(part)
        for k in range(1, n_chips):
            remote(tokens.at[mine, :], gath.at[tp, mine, :], tok_send, half_cross.at[n_chips - k - 1, part],
                   tp=across(k)).start()
        remote(tokens.at[mine, :], gath.at[tp, mine, :], tok_send, tok_near, tp=partner).start()

    def half_relay(part):
        for k in range(1, n_chips):
            block = gath.at[across(k), half_rows(part), :]
            remote(block, block, tok_send, half_cross.at[k - 1, part], tp=partner).wait_recv()
            remote(block, block, tok_send, half_settled.at[part], tp=partner).start()

    lax.fori_loop(0, chunks - 1, first_sends, 0)
    for part in range(per):
        half_start(part)

    for src, row, first, count in runs:
        remote(src.at[pl.ds(row, count), columns(partner)], wg.at[tp, pl.ds(first, count), :],
               pw_send, pw_recv, tp=partner).start()

    with scope("lwait"):
        for copy in local:
            copy.wait()
        token_copy.wait()
        for i, buf in enumerate(w_bufs):
            arrived(buf, w_sem.at[i])
        arrived(wg.at[tp], wo_sem)

    for h in range(ret):
        total = jnp.sum(decay[h:h + 1, :], axis=1, keepdims=True)
        logs[sp, h] = jnp.broadcast_to(total, (8, 128))

    @pl.when(sp == 0)
    def _():
        kbuf[0:WINDOW, :] = jnp.zeros((WINDOW, kbuf.shape[1]), BF16)
        vt[:, 0:WINDOW] = jnp.zeros((vt.shape[0], WINDOW), BF16)

    @pl.when(sp == n_sp - 1)
    def _():
        kbuf[rows + WINDOW:, :] = jnp.zeros((WINDOW, kbuf.shape[1]), BF16)
        vt[:, rows + WINDOW:] = jnp.zeros((vt.shape[0], WINDOW), BF16)

    row_i = lax.broadcasted_iota(jnp.int32, (CHUNK, CHUNK), 0)
    col_i = lax.broadcasted_iota(jnp.int32, (CHUNK, CHUNK), 1)
    low = lax.broadcasted_iota(jnp.int32, (CHUNK, 2 * RK), 1) < RK

    def decays(c, carry):
        here = rows_of(c, CHUNK)
        for h in range(ret):
            log_row = decay[h:h + 1, here]
            wide = jnp.broadcast_to(log_row, (CHUNK, CHUNK))
            log_col = jnp.sum(jnp.where(row_i == col_i, wide, 0.0), axis=1, keepdims=True)
            cum_col = jnp.sum(jnp.where(col_i <= row_i, wide, 0.0), axis=1, keepdims=True)
            cum_row = jnp.sum(jnp.where(row_i <= col_i, log_col, 0.0), axis=0, keepdims=True)
            total = jnp.sum(log_row, axis=1, keepdims=True)
            dm[h, c] = jnp.exp(-jnp.abs(cum_col - cum_row))
            up = jnp.exp(cum_col)
            down = jnp.exp(jnp.minimum(total - cum_col, 0.0))
            kfac[h, here, :] = jnp.where(low, down, up)
            qfac[h, here, :] = jnp.where(low, up, down)
            blog[h, c] = jnp.broadcast_to(total, (8, 128))
        return carry

    with scope("decays"):
        lax.fori_loop(0, chunks, decays, 0)

    shape = (MIX + 2 * WINDOW, MIX)
    q_i = lax.broadcasted_iota(jnp.int32, shape, 1)
    k_i = lax.broadcasted_iota(jnp.int32, shape, 0)
    band = (k_i >= q_i) & (k_i <= q_i + 2 * WINDOW)
    bias[0] = jnp.where(band, 0.0, -jnp.inf)
    bias[1] = jnp.where(band & (k_i >= WINDOW), 0.0, -jnp.inf)
    bias[2] = jnp.where(band & (k_i < MIX + WINDOW), 0.0, -jnp.inf)

    def normed(here, which, dst, first=0, size=CHUNK):
        squares = jnp.zeros((size, 1), F32)
        for p in range(2):
            slot = which * 2 + p
            x = gath[slot, here, :].astype(F32)
            squares = squares + jnp.sum(x * x, axis=1, keepdims=True)
            xbuf[dst, first:first + size, p * chan:(p + 1) * chan] = (x * gain[0:1, columns(slot)]).astype(BF16)
        return squares

    def product(which, src, b, off, cols, first=0, size=CHUNK):
        span = pl.ds(pl.multiple_of(which * (2 * chan), 2 * chan), 2 * chan)
        return mm(xbuf[src, first:first + size, :], w_bufs[b][span, off:off + cols])

    def near(i, carry):
        c = order(i)
        here = rows_of(c, CHUNK)
        sqs[here, :] = normed(here, chip, 0)
        for part, (b, off, cols, _) in zip(parts, cfg["dots"]):
            part[here, :] = product(chip, 0, b, off, cols)
        return carry

    with scope("near"):
        arrived(gath.at[0], tok_near)
        lax.fori_loop(0, chunks // 2, near, 0)

    with scope("ready"):
        @pl.when(sp == 0)
        def _():
            pl.semaphore_wait(ready, n_sp - 1)
            for k in range(1, n_sp):
                pl.semaphore_signal(ready, inc=1, device_id={"sp": k}, device_id_type=MESH)

        @pl.when(sp > 0)
        def _():
            pl.semaphore_wait(ready, 1)

    for k in range(1, n_sp):
        remote(logs.at[sp], logs.at[sp], log_send, log_recv, sp=lax.rem(sp + k, n_sp)).start()

    beside = sp + 1 - 2 * lax.rem(sp, 2)
    half_sp = n_sp // 2
    with scope("wfwd"):
        w_done(w_recv.at[0], 1)

        def w_pass(k, carry):
            for t in others:
                w_copy(t, sp, 1, k + 1, sp=lax.rem(sp + 2 * k, n_sp)).start()
            return carry

        lax.fori_loop(1, half_sp, w_pass, 0)
        for t in others:
            w_copy(t, sp, 2, 1, sp=beside).start()

    def w_aside(first, end):
        def w_over(k, carry):
            w_done(w_recv.at[k + 1], 1)
            for t in others:
                w_copy(t, lax.rem(sp + n_sp - 2 * k, n_sp), 2, 1, sp=beside).start()
            return carry

        lax.fori_loop(first, end, w_over, 0)

    with scope("near"):
        lax.fori_loop(chunks // 2, chunks, near, 0)

    rw = ret * RK
    p_row = lax.broadcasted_iota(jnp.int32, (rw, rw), 0)
    p_col = lax.broadcasted_iota(jnp.int32, (rw, rw), 1)
    first_half = lax.rem(p_col, RK) < RK // 2
    swap = jnp.where(
        first_half & (p_row == p_col + RK // 2), -1.0,
        jnp.where(jnp.logical_not(first_half) & (p_row == p_col - RK // 2), 1.0, 0.0),
    ).astype(BF16)
    ones = jnp.ones((HD, MIX + 2 * WINDOW), BF16)

    def attend(i):
        here = rows_of(i, MIX)
        span = pl.ds(pl.multiple_of(i * MIX, MIX), MIX + 2 * WINDOW)
        edge = lax.select((sp == 0) & (i == 0), 1, lax.select((sp == n_sp - 1) & (i == mixes - 1), 2, 0))
        block = bias[edge]
        block = jnp.concatenate([block] * groups, axis=1)
        done = []
        for g in range(kv):
            if paired:
                spots = [(j * kv + g) * 2 * HD for j in range(groups)]
                query = jnp.concatenate([qs[here, at:at + 2 * HD] for at in spots], axis=0)
                key = kbuf[span, :]
            else:
                spots = [(g * groups + j) * HD for j in range(groups)]
                query = jnp.concatenate([qs[here, at:at + HD] for at in spots], axis=0)
                key = kbuf[span, g * HD:(g + 1) * HD]
            value = jnp.concatenate([vt[g * HD:(g + 1) * HD, span], ones], axis=0)
            scores = mm_t(key, query) + block
            sink_row = jnp.concatenate(
                [jnp.broadcast_to(sink[0:1, g * groups + j:g * groups + j + 1], (1, MIX)) for j in range(groups)],
                axis=1)
            top = jnp.maximum(jnp.max(scores, axis=0, keepdims=True), sink_row)
            result = mm(value, jnp.exp(scores - top).astype(BF16))
            scale = 1.0 / (result[HD:HD + 1, :] + jnp.exp(sink_row - top))
            done.append(result[0:HD, :] * scale)
        both = jnp.concatenate(done, axis=0) if kv > 1 else done[0]
        turned = [jnp.transpose(both[:, j * MIX:(j + 1) * MIX]).astype(BF16) for j in range(groups)]
        if kv * HD % 128 == 0:
            for j in range(groups):
                mx[tp, here, j * kv * HD:(j + 1) * kv * HD] = turned[j]
        else:
            mx[tp, here, 0:att_w] = jnp.concatenate(turned, axis=1)
        atd.start(i)

    left, right = sp - 1, sp + 1

    def halo(side, i, where):
        def part(at):
            return kbuf.at[pl.ds(at, WINDOW), :] if i == 0 else vt.at[:, pl.ds(at, WINDOW)]

        src, dst = ((rows, 0), (WINDOW, rows + WINDOW))[side]
        return remote(part(src), part(dst), halo_send.at[side], halo_recv.at[side], sp=where)

    far = [(k - 1, lax.rem(chip + k, n_chips)) for k in range(1, n_chips)]

    def finish(found, here, inv_rms, first, size, *wanted):
        for part, (b, off, cols, names) in zip(parts, cfg["dots"]):
            if names[0][0] not in wanted:
                continue
            total = part[here, :]
            for at, which in far:
                total = total + product(which, at, b, off, cols, first, size)
            block = (total * inv_rms).astype(BF16)
            at = 0
            for name, count in names:
                found[name] = block[:, at:at + count]
                at += count

    def inverse(squares):
        return lax.rsqrt(squares / width + NORM_EPS)

    def attention_inputs(here, shifted, inv_rms, first, size):
        found = {}
        finish(found, here, inv_rms, first, size, "q", "k", "v")
        scaled = found["q"] * jnp.asarray(HD ** -0.5, BF16)
        if paired:
            wide = scaled.astype(F32)
            head = [wide[:, at:at + 2 * HD] for at in range(0, att_w, 2 * HD)]
            turned = [pltpu.roll(x, HD, 1) for x in head]
            lowest = lax.broadcasted_iota(jnp.int32, (size, 2 * HD), 1) < HD
            for j in range(groups):
                for g in range(kv):
                    at = (g * groups + j) * HD
                    x = (head if at % (2 * HD) == g * HD else turned)[at // (2 * HD)]
                    keep = lowest if g == 0 else jnp.logical_not(lowest)
                    to = (j * kv + g) * 2 * HD
                    qs[here, to:to + 2 * HD] = jnp.where(keep, x, 0.0).astype(BF16)
        else:
            qs[here, :] = scaled
        kbuf[shifted, :] = found["k"]
        vt[:, shifted] = jnp.transpose(found["v"].astype(F32)).astype(BF16)

    def far_squares(here, first, size):
        squares = sqs[here, :]
        for at, which in far:
            squares = squares + normed(here, which, at, first, size)
        return squares

    def half(part, between):
        mine = half_rows(part)
        half_relay(part)
        between()
        with scope("x2"):
            arrived(gath.at[0:n_chips - 1, mine, :], half_settled.at[part])
        return far_squares(mine, part * MIX, MIX)

    def half_inputs(part, squares):
        with scope("phaseB"):
            attention_inputs(half_rows(part), pl.ds(final * CHUNK + part * MIX + WINDOW, MIX), inverse(squares),
                             part * MIX, MIX)

    def chunk(c, last, between, squares=None, while_waiting=None):
        here = rows_of(c, CHUNK)
        if not last:
            with scope("x1"):
                tok.relay(c)
            between()
            with scope("x2"):
                arrived(gath.at[0:n_chips - 1, here, :], tok_settled.at[c])
        ctx = scope("phaseA")
        ctx.__enter__()
        if not last:
            squares = far_squares(here, 0, CHUNK)
        inv_rms = inverse(squares)
        found = {}
        finish(found, here, inv_rms, 0, CHUNK, "rq", "rk", "rv")
        spot = sp * chunks + c
        oc, os_ = outer_cos[pl.ds(spot, 1), :], outer_sin[pl.ds(spot, 1), :]
        ic, is_ = inner_cos[...], inner_sin[...]
        cosine = oc * ic - os_ * is_
        sine = os_ * ic + oc * is_
        query_rot = found["rq"].astype(F32) * cosine + mm(found["rq"], swap) * sine
        key_rot = (found["rk"].astype(F32) * cosine + mm(found["rk"], swap) * sine) * RK ** -0.5

        def doubled(x):
            if ret == 2:
                turned = pltpu.roll(x, RK, 1)
                return jnp.where(low, x, turned), jnp.where(low, turned, x)
            return [jnp.concatenate([x[:, h * RK:(h + 1) * RK]] * 2, axis=1) for h in range(ret)]

        keys = doubled(key_rot)
        for h in range(ret):
            both = (keys[h] * kfac[h, here, :]).astype(BF16)
            terms = tm_m(both, found["rv"][:, h * RV:(h + 1) * RV])
            fterm[h, c] = terms[:RK]
            bterm[h, c] = terms[RK:]
        ctx.__exit__(None, None, None)
        if last:
            with scope("totals"):
                send_totals()
        if last:
            while_waiting()
        else:
            with scope("phaseB"):
                attention_inputs(here, pl.ds(pl.multiple_of(c * CHUNK + WINDOW, 128), CHUNK), inv_rms, 0, CHUNK)
        ctx = scope("phaseC")
        ctx.__enter__()
        finish(found, here, inv_rms, 0, CHUNK, "g")
        gs[here, :] = found["g"]
        queries = doubled(query_rot)
        key_bf = key_rot.astype(BF16)
        for h in range(ret):
            if ret == 2:
                keep = low if h == 0 else jnp.logical_not(low)
                inner = mm_t(jnp.where(keep, query_rot, 0.0).astype(BF16), key_bf)
            else:
                inner = mm_t(query_rot[:, h * RK:(h + 1) * RK].astype(BF16), key_bf[:, h * RK:(h + 1) * RK])
            rloc[h, here, :] = mm((inner * dm[h, c]).astype(BF16), found["rv"][:, h * RV:(h + 1) * RV])
            qfb[h, here, :] = (queries[h] * qfac[h, here, :]).astype(BF16)
        ctx.__exit__(None, None, None)

    def send_totals():
        for h in range(ret):
            state = jnp.zeros((RK, RV), F32)
            back = jnp.zeros((RK, RV), F32)
            for c in range(chunks):
                state = jnp.exp(blog[h, c, 0:1, :]) * state + fterm[h, c]
                back = jnp.exp(blog[h, chunks - 1 - c, 0:1, :]) * back + bterm[h, chunks - 1 - c]
            tot_f[h] = state.astype(BF16)
            tot_b[h] = back.astype(BF16)

            def send_f(i, carry):
                remote(tot_f.at[h], tots.at[sp, h], tot_send, tot_recv.at[h], sp=n_sp - 1 - i).start()
                return carry

            def send_b(d, carry):
                remote(tot_b.at[h], tots.at[sp, h], tot_send, tot_recv.at[h], sp=d).start()
                return carry

            lax.fori_loop(0, n_sp - 1 - sp, send_f, 0)
            lax.fori_loop(0, sp, send_b, 0)

    early = per * (chunks - 3) + 1

    def block_of(j):
        turn = early - per + 1
        return lax.select(j < turn, j, lax.select(j == turn, mixes - 1, j - 1))

    def halo_wait(side):
        arrived(kbuf.at[0:2 * WINDOW, :], halo_recv.at[side])

    def one(j):
        with scope("attend"):
            attend(j)

    def chunk_body(i, carry):
        c = order(i)

        if chunks > 4:
            @pl.when(i > 2)
            def _():
                one(per * (i - 3) + 1)

        def between():
            @pl.when(i == chunks - 2)
            def _():
                with scope("aside"):
                    w_aside(chunks - 1, half_sp)

            @pl.when((i == 2) & (sp > 0))
            def _():
                with scope("halo0"):
                    halo_wait(0)

            @pl.when(i == 2)
            def _():
                one(0)

            if chunks > 4:
                @pl.when(i > 2)
                def _():
                    one(per * (i - 3) + 2)

        chunk(c, False, between)

        @pl.when((i == 0) & (sp < n_sp - 1))
        def _():
            for b in range(2):
                halo(0, b, right).start()

        @pl.when((i == 1) & (sp > 0))
        def _():
            for b in range(2):
                halo(1, b, left).start()

        @pl.when(i < min(chunks - 2, half_sp - 1))
        def _():
            with scope("aside"):
                w_aside(i + 1, i + 2)

        return carry

    lax.fori_loop(0, chunks - 1, chunk_body, 0)

    def late(j, carry):
        with scope("late"):
            attend(j)
        with scope("lrelay"):
            atd.relay(block_of(j - early))
        return carry

    first_squares = half(0, lambda: one(early - per))
    half_inputs(0, first_squares)

    @pl.when(sp < n_sp - 1)
    def _():
        with scope("halo1"):
            halo_wait(1)

    one(mixes - 1)
    last_squares = half(1, lambda: one(early - per + 1))

    def rest():
        late(early, 0)
        half_inputs(1, last_squares)
        lax.fori_loop(early + 1, mixes - 1, late, 0)

    chunk(final, True, None, jnp.concatenate([first_squares, last_squares], axis=0), rest)

    def states_of(h):
        arrived(tots.at[0:n_sp - 1, 0], tot_recv.at[h])

        def from_low(e, state):
            return jnp.exp(logs[e, h, 0:1, :]) * state + tots[e, h].astype(F32)

        def from_high(i, back):
            e = n_sp - 1 - i
            return jnp.exp(logs[e, h, 0:1, :]) * back + tots[e, h].astype(F32)

        state = lax.fori_loop(0, sp, from_low, states[0, h])
        back = lax.fori_loop(0, n_sp - 1 - sp, from_high, states[1, h])
        for c in range(chunks):
            both_in[h, c, 0:RK] = state.astype(BF16)
            state = jnp.exp(blog[h, c, 0:1, :]) * state + fterm[h, c]
            r = chunks - 1 - c
            both_in[h, r, RK:2 * RK] = back.astype(BF16)
            back = jnp.exp(blog[h, r, 0:1, :]) * back + bterm[h, r]

    def retain(c, h):
        here = rows_of(c, MIX)
        combined = rloc[h, here, :] + mm(qfb[h, here, :], both_in[h, lax.div(c, per)])
        centered = combined - jnp.mean(combined, axis=1, keepdims=True)
        normed_ret = centered * lax.rsqrt(jnp.mean(centered * centered, axis=1, keepdims=True) + NORM_EPS)
        gate = gs[here, h * RV:(h + 1) * RV].astype(F32)
        mx[tp, here, att_w + h * RV:att_w + (h + 1) * RV] = (gate / (1.0 + jnp.exp(-gate)) * normed_ret).astype(BF16)
        rtd[h].start(c)

    arrived(logs.at[0:n_sp - 1], log_recv)
    for h in range(ret):
        with scope("states"):
            states_of(h)

        def ret_body(c, carry):
            retain(c, h)
            return carry

        with scope("retain"):
            lax.fori_loop(0, mixes, ret_body, 0)

    def att_rest(j, carry):
        atd.relay(block_of(j))
        return carry

    with scope("attrest"):
        lax.fori_loop(mixes - 1 - early, mixes, att_rest, 0)

    with scope("wsettle"):
        arrived(wg.at[0], pw_recv)
        w_done(w_recv.at[1], half_sp)
        for t in range(n_tp):
            w_last[t * RV:(t + 1) * RV, :] = wg[t, most:most + RV, :]

    def mix_most(c):
        here = rows_of(c, CHUNK)
        with scope("bsettle"):
            arrived(mx.at[0:n_chips, here, 0:most], most_settled.at[c])
        with scope("base"):
            total = mm(mx[0, here, 0:most], wg[0, 0:most, :])
            for t in range(1, n_tp):
                total = total + mm(mx[t, here, 0:most], wg[t, 0:most, :])
            base[here, :] = total

    def mix_last(c):
        here = rows_of(c, MIX)
        with scope("msettle"):
            arrived(mx.at[0:n_chips, here, most:most + RV], last_settled.at[c])
        with scope("mix"):
            wide = jnp.concatenate([mx[t, here, most:] for t in range(n_tp)], axis=1)
            out[here, :] = (base[here, :] + mm(wide, w_last[...])).astype(BF16)

    lag = 2

    def first_heads(c, carry):
        with scope("hrelay"):
            for h in range(ret - 1):
                rtd[h].relay(c)

        @pl.when(c >= 1)
        def _():
            mix_most(c - 1)

        return carry

    def last_head(c, carry):
        with scope("rrelay"):
            rtd[ret - 1].relay(c)

        @pl.when(c == lag - 1)
        def _():
            mix_most(chunks - 1)

        @pl.when(c >= lag)
        def _():
            mix_last(c - lag)

        return carry

    def ending(c, carry):
        mix_last(c)
        return carry

    lax.fori_loop(0, chunks, first_heads, 0)
    lax.fori_loop(0, mixes, last_head, 0)
    lax.fori_loop(mixes - lag, mixes, ending, 0)

    with scope("drain"):
        sent = 2 * n_chips - 1
        arrived(gath.at[0:sent], tok_send)
        arrived(mx.at[0:sent], mix_send)
        arrived(wg.at[0], pw_send)
        w_done(w_send.at[0], 1)
        w_done(w_send.at[1], half_sp - 1)
        w_done(w_send.at[2], half_sp)
        arrived(logs.at[0:n_sp - 1], log_send)
        arrived(tots.at[0:n_sp - 1], tot_send)

        @pl.when(sp < n_sp - 1)
        def _():
            arrived(kbuf.at[0:2 * WINDOW, :], halo_send.at[0])

        @pl.when(sp > 0)
        def _():
            arrived(kbuf.at[0:2 * WINDOW, :], halo_send.at[1])


def body(n_sp, n_tp, tokens, norm_gain, w_q, w_k, w_v, w_rq, w_rk, w_rv, w_rg, att_sink,
         decay_log, init_state, out_att, out_ret):
    rows, chan = tokens.shape
    width = n_tp * chan
    ret = decay_log.shape[0]
    heads = att_sink.shape[0]
    kv_cols = w_k.shape[1]
    kv = kv_cols // HD
    chunks = rows // CHUNK
    n_chips = n_tp // 2
    weights = (w_q, w_k, w_v, w_rq, w_rk, w_rv, w_rg)
    names = ("q", "k", "v", "rq", "rk", "rv", "g")
    cols = [w.shape[1] for w in weights]
    joined = all(count % 128 == 0 for count in cols)
    places, dots = [], []
    if joined:
        buffers = [sum(cols)]
        at = 0
        for count in cols:
            places.append((0, at, count))
            at += count
        for group in ((3, 4), (5,), (1, 2), (0,), (6,)):
            dots.append((0, places[group[0]][1], sum(cols[i] for i in group),
                         tuple((names[i], cols[i]) for i in group)))
    else:
        buffers = cols
        for i, count in enumerate(cols):
            places.append((i, 0, count))
            dots.append((i, 0, count, ((names[i], count),)))
    att_w, ret_w = heads * HD, ret * RV
    paired = kv == 2 and 2 * HD == 128
    assert kv == 1 or HD % ((att_w + ret_w) // n_sp) == 0
    cfg = dict(paired=paired, n_sp=n_sp, n_tp=n_tp, n_chips=n_chips, chunks=chunks, chan=chan, heads=heads,
               ret=ret, kv=kv, buffers=buffers, places=places, dots=dots, joined=joined)
    tables = rope_tables(n_sp * chunks, CHUNK, ret) + rope_tables(CHUNK, 1, ret)
    small = [norm_gain.reshape(1, width), att_sink.reshape(1, heads), decay_log]
    small += [jnp.asarray(t) for t in tables]
    anyw = pl.BlockSpec(memory_space=pl.ANY)
    dma = pltpu.SemaphoreType.DMA
    mixes = rows // MIX
    scratch = [pltpu.VMEM((width, count), BF16) for count in buffers] + [
        pltpu.VMEM(a.shape, F32) for a in small] + [
        pltpu.VMEM((rows, group[2]), F32) for group in dots] + [
        pltpu.VMEM((n_tp, att_w + ret_w, chan), BF16),
        pltpu.VMEM((n_tp, rows, chan), BF16),
        pltpu.VMEM((max(n_chips - 1, 1), CHUNK, 2 * chan), BF16),
        pltpu.VMEM((rows, att_w * (2 if paired else 1)), BF16),
        pltpu.VMEM((rows + 2 * WINDOW, kv_cols), BF16),
        pltpu.VMEM((kv_cols, rows + 2 * WINDOW), BF16),
        pltpu.VMEM((n_tp, rows, att_w + ret_w), BF16),
        pltpu.VMEM((ret, rows, 2 * RK), BF16),
        pltpu.VMEM((ret, rows, RV), F32),
        pltpu.VMEM((rows, ret_w), BF16),
        pltpu.VMEM((ret, chunks, RK, RV), F32),
        pltpu.VMEM((ret, chunks, RK, RV), F32),
        pltpu.VMEM((ret, chunks, 8, 128), F32),
        pltpu.VMEM((ret, chunks, 2 * RK, RV), BF16),
        pltpu.VMEM((rows, 1), F32),
        pltpu.VMEM((ret, chunks, CHUNK, CHUNK), F32),
        pltpu.VMEM((ret, rows, 2 * RK), F32),
        pltpu.VMEM((ret, rows, 2 * RK), F32),
        pltpu.VMEM((3, MIX + 2 * WINDOW, MIX), F32),
        pltpu.VMEM((rows, chan), F32),
        pltpu.VMEM((n_tp * RV, chan), BF16),
        pltpu.VMEM((ret, RK, RV), BF16),
        pltpu.VMEM((ret, RK, RV), BF16),
        pltpu.VMEM((n_sp, ret, RK, RV), BF16),
        pltpu.VMEM((n_sp, ret, 8, 128), F32),
        pltpu.VMEM((2, ret, RK, RV), F32),
        pltpu.SemaphoreType.REGULAR,
        dma((len(buffers),)), dma, dma, dma((len(small) + 1,)),
        dma, dma((n_chips - 1, chunks)), dma, dma((chunks,)),
        dma((n_chips - 1, CHUNK // MIX)), dma((CHUNK // MIX,)),
        dma, dma((n_chips - 1, mixes)), dma((max(ret - 1, 1), n_chips - 1, chunks)),
        dma((n_chips - 1, mixes)), dma((chunks,)), dma((mixes,)),
        dma, dma, dma((3,)), dma((n_sp // 2 + 1,)),
        dma((2,)), dma((2,)),
        dma, dma((ret,)), dma, dma,
    ]
    return pl.pallas_call(
        functools.partial(kernel, cfg),
        out_shape=pltpu.VMEM((rows, chan), BF16),
        in_specs=[anyw] * (11 + len(small)),
        out_specs=pl.BlockSpec(memory_space=pltpu.VMEM),
        scratch_shapes=scratch,
        compiler_params=pltpu.CompilerParams(
            collective_id=0, has_side_effects=True, vmem_limit_bytes=60 * 1024 * 1024),
    )(tokens, *weights, init_state, out_att, out_ret, *small)


def solution(mesh):
    n_sp, n_tp = mesh.shape["sp"], mesh.shape["tp"]
    in_specs = (
        P("sp", "tp"),
        P(),
        P(None, "tp"),
        P(None, "tp"),
        P(None, "tp"),
        P(None, "tp"),
        P(None, "tp"),
        P(None, "tp"),
        P(None, "tp"),
        P("tp"),
        P("tp", "sp"),
        P(None, "tp", None, None),
        P("tp", None),
        P("tp", None),
    )
    return jax.shard_map(functools.partial(body, n_sp, n_tp), mesh=mesh, in_specs=in_specs,
                         out_specs=P("sp", "tp"), check_vma=False)
```
